128 devices in a mesh: kv: 16 (over z, x), tp: 8 (over y, core).
Axes of the slice: x: 4, y: 4, z: 4, core: 2. Of those that a mesh axis runs over, the one named last changes fastest.
Arguments:
- tokens: bfloat16 [96, 4096], P(None, 'kv'), may hold values from -210 to 210
- norm_gain: float32 [4096], P('kv'), may hold values from 0.1 to 1.9
- w_query: bfloat16 [4096, 4096], P('kv', 'tp'), may hold values from -1 to 1
- w_key: bfloat16 [4096, 4096], P('kv', 'tp'), may hold values from -2 to 2
- w_value: bfloat16 [4096, 4096], P('kv', 'tp'), may hold values from -0.09375 to 0.09375
- w_output: bfloat16 [4096, 4096], P('tp', 'kv'), may hold values from -0.09375 to 0.09375
- cache_keys: bfloat16 [4, 8192, 4096], P(None, 'kv', 'tp'), may hold values from -820 to 820
- cache_values: bfloat16 [4, 8192, 4096], P(None, 'kv', 'tp'), may hold values from -6 to 6
- map_lambda: float32 [64], P('tp'), may hold values from 0.3 to 0.8
- out_gain: float32 [4096], P('tp'), may hold values from 0.1 to 1.9
- parents: int32 [4, 24], replicated, may hold values from -1 to 22, as said below
- lengths: int32 [4], replicated, may hold values from 4096 to 8144, as said below
- accepted: int32 [4], replicated, may hold values from 0 to 24
Outputs:
- mixed: bfloat16 [96, 4096], P(None, 'kv')
- new_keys: bfloat16 [4, 8192, 4096], P(None, 'kv', 'tp')
- new_values: bfloat16 [4, 8192, 4096], P(None, 'kv', 'tp')
The draws below stay inside these ranges and needn't reach their ends.
Inputs may be any that keep to these rules, and one draw needn't show every extreme that they name: parents[b, j] lies between -1 and j - 1. `lengths`: some sequence has exactly the largest value.
All inputs are finite; a program needn't handle non-finite values.
Results may differ from the reference program's by a relative error of at most 0.029.
Values may be sent and summed in bfloat16 or wider, within the bound.
A program may use at most 128 MiB of HBM per device.

```python
import math
import jax
import jax.numpy as jnp
from jax import lax

D = 4096
HEADS = 64
HEAD = 64
QK = 32
SEQS = 4
POS_DEV = 512
PROP = 24
CACHE = 8192
ROWS = 96
N_KV = 16
N_TP = 8


def draw_tokens(key, part):
    column_rise = jnp.arange(D, dtype=jnp.float32) / (D - 1)
    shared_part = 0.8 ** 0.5
    own_part = 0.2 ** 0.5
    common = jax.random.normal(jax.random.fold_in(key, 11), (SEQS, 1, D), jnp.float32)
    own = jax.random.normal(key, (SEQS, PROP, D), jnp.float32)
    mixture = jnp.clip(shared_part * common + own_part * own, -6.0, 6.0).reshape(ROWS, D)
    values = mixture * jnp.exp(column_rise * 1.1)
    return values.astype(jnp.bfloat16)


def query_matrix(key):
    base = jnp.clip(jax.random.normal(jax.random.fold_in(key, 21), (D, HEADS * HEAD), jnp.float32), -6.0, 6.0)
    return base * D ** (-0.5)


def draw_w_query(key, part):
    return query_matrix(key).astype(jnp.bfloat16)


def draw_w_key(key, part):
    coupling = math.log(1.6 * CACHE) / math.sqrt(QK)
    noise = jnp.clip(jax.random.normal(jax.random.fold_in(key, 22), (D, HEADS * HEAD), jnp.float32), -6.0, 6.0)
    values = coupling * query_matrix(key) + noise * D ** (-0.5)
    return values.astype(jnp.bfloat16)


def draw_cache_keys(key, part):
    values = 1.7 * jnp.clip(jax.random.normal(key, (SEQS, CACHE, HEADS * HEAD), jnp.float32), -6.0, 6.0)
    return values.astype(jnp.bfloat16)


def draw_parents(key, part):
    limits = jnp.arange(PROP, dtype=jnp.int32)
    return jax.random.randint(key, (SEQS, PROP), -1, limits[None, :]).astype(jnp.int32)


def draw_lengths(key, part):
    drawn = jax.random.randint(key, (SEQS,), CACHE // 2, CACHE - 2 * PROP + 1)
    chosen = jax.random.randint(jax.random.fold_in(key, 1), (), 0, SEQS)
    return drawn.at[chosen].set(CACHE - 2 * PROP).astype(jnp.int32)


def with_ends(array, stream_key, least, high):
    longest = array.shape.index(max(array.shape))
    spots = []
    for shift in (0, 1):
        where = [jax.random.randint(jax.random.fold_in(stream_key, axis), (), 0, length) for axis, length in enumerate(array.shape)]
        where[longest] = (where[longest] + shift) % array.shape[longest]
        spots.append(tuple(where))
    return array.at[spots[0]].set(least).at[spots[1]].set(high)


def block_levels(own_key, extent, shards, smallest, largest):
    factor_of = 1.0
    for position, shards_of in shards:
        heights = jax.random.uniform(jax.random.fold_in(jax.random.fold_in(own_key, 6), position), (shards_of,), jnp.float32, smallest / len(shards), largest / len(shards))
        factor_of = factor_of * jnp.repeat(jnp.exp(heights), extent[position] // shards_of).reshape((-1,) + (1,) * (len(extent) - 1 - position))
    return factor_of


def bell_draw(own_key, shape, scale, reach, split=(), kind=jnp.bfloat16):
    values = scale * jax.random.normal(own_key, shape, jnp.float32)
    if split:
        values = values * block_levels(own_key, shape, split, -0.22, 0.18)
    return jnp.clip(values, -reach, reach).astype(kind)


def setup_inputs(seed: int = 0) -> dict:
    keys = jax.random.split(jax.random.key(seed), 14)
    tokens = draw_tokens(jax.random.fold_in(keys[13], 71), 0)
    norm_gain = jnp.clip(1.0 + 0.18 * jax.random.normal(keys[1], (D,), jnp.float32), 0.1, 1.9)
    w_query = draw_w_query(jax.random.fold_in(keys[13], 71), 0)
    w_key = draw_w_key(jax.random.fold_in(keys[13], 71), 0)
    w_value = bell_draw(keys[4], (D, HEADS * HEAD), D ** -0.5, 0.09375, ((0, 16), (1, 8)))
    w_output = bell_draw(keys[5], (HEADS * HEAD, D), (HEADS * HEAD) ** -0.5, 0.09375, ((0, 8), (1, 16)))
    cache_keys = draw_cache_keys(jax.random.fold_in(keys[13], 71), 0)
    cache_values = bell_draw(keys[7], (SEQS, CACHE, HEADS * HEAD), 1.0, 6.0, ((1, 16), (2, 8)))
    map_lambda = jnp.clip(0.3 + 0.5 * jax.random.uniform(keys[8], (HEADS,), jnp.float32) ** block_levels(keys[8], (HEADS,), ((0, 8),), -0.2, 0.2), 0.3, 0.8)
    out_gain = jnp.clip(1.0 + 0.18 * jax.random.normal(keys[9], (HEADS * HEAD,), jnp.float32), 0.1, 1.9)
    parents = draw_parents(jax.random.fold_in(keys[13], 71), 0)
    lengths = draw_lengths(jax.random.fold_in(keys[13], 71), 0)
    accepted = with_ends(jax.random.randint(keys[12], (SEQS,), 0, PROP + 1), jax.random.fold_in(keys[12], 1), 0, PROP).astype(jnp.int32)
    return dict(tokens=tokens, norm_gain=norm_gain, w_query=w_query, w_key=w_key, w_value=w_value, w_output=w_output, cache_keys=cache_keys, cache_values=cache_values, map_lambda=map_lambda, out_gain=out_gain, parents=parents, lengths=lengths, accepted=accepted)


epsilon = 1e-05
masked_low = -1e+30

def ancestry(parents):
    count = parents.shape[1]
    places = jnp.arange(count, dtype=jnp.int32)
    parent_links = (parents[:, :, None] == places[None, None, :]).astype(jnp.float32)
    identity = jnp.eye(count, dtype=jnp.float32)[None]

    def extend(turn_index, reached):
        return jnp.minimum(1.0, identity + jnp.einsum('bji,bik->bjk', parent_links, reached))
    reached = lax.fori_loop(0, count, extend, jnp.broadcast_to(identity, parent_links.shape))
    return reached > 0.5

def reference(tokens, norm_gain, w_query, w_key, w_value, w_output, cache_keys, cache_values, map_lambda, out_gain, parents, lengths, accepted):
    f32 = jnp.float32
    bf16 = jnp.bfloat16
    tokens_wide = tokens.astype(f32)
    norm_factor = lax.rsqrt(lax.optimization_barrier(jnp.mean(tokens_wide * tokens_wide, axis=1, keepdims=True)) + epsilon)
    gained = (tokens_wide * norm_gain).astype(bf16)

    def projection(weight_matrix):
        return (jnp.dot(gained, weight_matrix, preferred_element_type=f32) * norm_factor).astype(bf16)
    queries = projection(w_query)
    keys_flat = projection(w_key)
    values_flat = projection(w_value)
    query_heads = queries.astype(f32).reshape(SEQS, PROP, HEADS, 2, QK)
    key_heads = keys_flat.astype(f32).reshape(SEQS, PROP, HEADS, 2, QK)
    value_heads = values_flat.reshape(SEQS, PROP, HEADS, HEAD)
    start = lengths + accepted
    score_scale = QK ** (-0.5)

    def cache_block(block_index):
        begin = (block_index * POS_DEV).astype(jnp.int32)
        block_keys = lax.dynamic_slice_in_dim(cache_keys, begin, POS_DEV, 1).astype(f32)
        block_keys = block_keys.reshape(SEQS, POS_DEV, HEADS, 2, QK)
        block_vals = lax.dynamic_slice_in_dim(cache_values, begin, POS_DEV, 1).astype(f32)
        block_vals = block_vals.reshape(SEQS, POS_DEV, HEADS, HEAD)
        positions = begin + jnp.arange(POS_DEV, dtype=jnp.int32)
        visible = (positions[None, :] < start[:, None])[:, None, None, None, :]
        scores = jnp.einsum('bqhmd,bkhmd->bmhqk', query_heads, block_keys) * score_scale
        block_max = lax.optimization_barrier(jnp.max(jnp.where(visible, scores, masked_low), axis=-1))
        block_weight = jnp.where(visible, jnp.exp(scores - block_max[..., None]), 0.0)
        block_total = lax.optimization_barrier(jnp.sum(block_weight, axis=-1))
        rounded = block_weight.astype(bf16).astype(f32)
        block_values = jnp.einsum('bmhqk,bkhd->bmhqd', rounded, block_vals).astype(bf16)
        return (block_max, block_total, block_values)
    maxima, totals, values = lax.map(cache_block, jnp.arange(N_KV, dtype=jnp.int32))
    cache_max = lax.optimization_barrier(jnp.max(maxima, axis=0))
    factors = jnp.exp(maxima - cache_max[None])
    cache_total = lax.optimization_barrier(jnp.sum(totals * factors, axis=0))
    cache_sum = lax.optimization_barrier(jnp.sum(values.astype(f32) * factors[..., None], axis=0))
    lineage = ancestry(parents)[:, None, None, :, :]
    self_scores = jnp.einsum('bqhmd,bjhmd->bmhqj', query_heads, key_heads) * score_scale
    self_max = lax.optimization_barrier(jnp.max(jnp.where(lineage, self_scores, masked_low), axis=-1))
    top = jnp.maximum(cache_max, self_max)
    self_weight = jnp.where(lineage, jnp.exp(self_scores - top[..., None]), 0.0)
    carried = jnp.exp(cache_max - top)
    denominator = cache_total * carried + lax.optimization_barrier(jnp.sum(self_weight, axis=-1))
    self_values = jnp.einsum('bmhqj,bjhd->bmhqd', self_weight.astype(bf16).astype(f32), value_heads.astype(f32))
    attended = (cache_sum * carried[..., None] + self_values) / denominator[..., None]
    difference = attended[:, 0] - map_lambda[None, :, None, None] * attended[:, 1]
    gains = out_gain.reshape(HEADS, HEAD)[None, :, None, :]
    normed = difference * lax.rsqrt(lax.optimization_barrier(jnp.mean(difference * difference, axis=-1, keepdims=True)) + epsilon) * gains
    normed = jnp.transpose(normed, (0, 2, 1, 3)).reshape(ROWS, HEADS * HEAD).astype(bf16)
    group = HEADS // N_TP
    pieces = normed.reshape(ROWS, N_TP, group * HEAD).astype(f32)
    weight_groups = w_output.reshape(N_TP, group * HEAD, D).astype(f32)
    partials = jnp.einsum('rgc,gcd->grd', pieces, weight_groups).astype(bf16)
    partials = lax.optimization_barrier(partials).astype(f32)
    mixed = lax.optimization_barrier(jnp.sum(partials, axis=0)).astype(bf16)

    def place(cache_row, new_rows, begin):
        return lax.dynamic_update_slice(cache_row, new_rows, (begin, jnp.int32(0)))
    new_keys = jax.vmap(place)(cache_keys, keys_flat.reshape(SEQS, PROP, HEADS * HEAD), start)
    new_values = jax.vmap(place)(cache_values, values_flat.reshape(SEQS, PROP, HEADS * HEAD), start)
    return (mixed, new_keys, new_values)
```

```python
import functools

import jax
import jax.numpy as jnp
from jax import lax
from jax.experimental import pallas as pl
from jax.experimental.pallas import tpu as pltpu
from jax.sharding import PartitionSpec as P

D = 4096
HEAD = 64
QK = 32
SEQS = 4
PROP = 24
KV = 16
TP = 8
BLOCK = 128
PAD = 32
POS = 512
ROWS = 96
EPS = 1e-05
LOW = -1e30
LOG2E = 1.4426950408889634
SCALE2 = QK ** (-0.5) * LOG2E
F32 = jnp.float32
BF16 = jnp.bfloat16
NT = (((1,), (1,)), ((), ()))


def _distance(step):
    ring = (0, 1, 2, 1)
    return ring[step >> 2] + ring[step & 3]


PARTNERS = sorted(range(1, KV), key=lambda step: -_distance(step))


def _dot(a, b):
    return jnp.dot(a, b, preferred_element_type=F32)


def _dot_nt(a, b):
    return lax.dot_general(a, b, NT, preferred_element_type=F32)


def _lane_head_map(rows):
    lane = lax.broadcasted_iota(jnp.int32, (rows, BLOCK), 1)
    return lane


def _expanded(chunk):
    lane = lax.broadcasted_iota(jnp.int32, (PROP, BLOCK), 1)
    parts = []
    for which in range(2):
        for head in range(2):
            low = head * HEAD + which * QK
            inside = (lane >= low) & (lane < low + QK)
            parts.append(jnp.where(inside, chunk, 0.0))
    parts.append(jnp.zeros((BLOCK - 4 * PROP, BLOCK), F32))
    return jnp.concatenate(parts, axis=0).astype(BF16)


def _main_kernel(
    tok_hbm,
    gain_ref,
    wq_hbm,
    wk_hbm,
    wv_hbm,
    wo_hbm,
    ck_hbm,
    cv_hbm,
    lam_ref,
    og_ref,
    par_ref,
    len_ref,
    acc_ref,
    mixed_ref,
    kvn_ref,
    tok,
    wqkv,
    wo,
    kbuf,
    vbuf,
    vt,
    pq,
    rq,
    pkv,
    rkv,
    qg,
    kvg,
    dv,
    rdv,
    ds,
    rds,
    ng,
    part,
    rpart,
    par_pad,
    qe,
    load_sem,
    q_send,
    q_recv,
    kv_send,
    kv_recv,
    qg_send,
    qg_recv,
    kvg_send,
    kvg_recv,
    dv_send,
    dv_recv,
    ds_send,
    ds_recv,
    ng_send,
    ng_recv,
    mx_send,
    mx_recv,
):
    me = lax.axis_index("kv")
    tp = lax.axis_index("tp")
    z = me // 4
    x = lax.rem(me, 4)

    loads = {}

    def load(name, src, dst, index):
        copy = pltpu.make_async_copy(src, dst, load_sem.at[index])
        copy.start()
        loads[name] = copy

    load("tok", tok_hbm, tok, 0)
    load("wq", wq_hbm, wqkv.at[0], 1)
    load("wk", wk_hbm, wqkv.at[1], 2)
    load("wv", wv_hbm, wqkv.at[2], 3)
    for b in range(SEQS):
        load(("v", b), cv_hbm.at[b], vbuf.at[b], 4 + b)
    for b in range(SEQS):
        load(("k", b), ck_hbm.at[b], kbuf.at[b], 8 + b)
    load("wo", wo_hbm, wo, 12)

    barrier = pltpu.get_barrier_semaphore()
    for step in PARTNERS:
        pl.semaphore_signal(barrier, inc=1, device_id={"kv": me ^ step}, device_id_type=pl.DeviceIdType.MESH)
    for step in range(1, TP):
        pl.semaphore_signal(barrier, inc=1, device_id={"tp": tp ^ step}, device_id_type=pl.DeviceIdType.MESH)

    def to_kv(step, src, dst, send, recv):
        return pltpu.make_async_remote_copy(
            src_ref=src,
            dst_ref=dst,
            send_sem=send.at[step],
            recv_sem=recv.at[step],
            device_id={"kv": me ^ step},
            device_id_type=pl.DeviceIdType.MESH,
        )

    def q_copy(step):
        return to_kv(step, pq.at[me ^ step], rq.at[step], q_send, q_recv)

    def kv_copy(step):
        return to_kv(step, pkv.at[me ^ step], rkv.at[step], kv_send, kv_recv)

    def qg_copy(step):
        return to_kv(step, qg.at[me], qg.at[me], qg_send, qg_recv)

    def kvg_copy(step):
        return to_kv(step, kvg.at[me], kvg.at[me], kvg_send, kvg_recv)

    def dv_copy(step):
        return to_kv(step, dv.at[me ^ step], rdv.at[step], dv_send, dv_recv)

    def ds_copy(step):
        return to_kv(step, ds.at[me ^ step], rds.at[step], ds_send, ds_recv)

    def ng_slot():
        return ng.at[x, pl.ds(pl.multiple_of(z * PAD, PAD), PAD), :]

    def ng_copy(step):
        return to_kv(step, ng_slot(), ng_slot(), ng_send, ng_recv)

    def mx_copy(step):
        return pltpu.make_async_remote_copy(
            src_ref=part,
            dst_ref=rpart.at[step],
            send_sem=mx_send.at[step],
            recv_sem=mx_recv.at[step],
            device_id={"tp": tp ^ step},
            device_id_type=pl.DeviceIdType.MESH,
        )

    loads["tok"].wait()
    wide = tok[...].astype(F32)
    gained = (wide * gain_ref[...]).astype(BF16)
    square = jnp.sum(wide * wide, axis=1, keepdims=True)
    eye = lax.broadcasted_iota(jnp.int32, (PROP, BLOCK), 0) == lax.broadcasted_iota(jnp.int32, (PROP, BLOCK), 1)
    loads["wq"].wait()
    partial_q = _dot(gained, wqkv[0])
    for b in range(SEQS):
        column = square[b * PROP : (b + 1) * PROP]
        row = jnp.sum(jnp.where(eye, column, 0.0), axis=0, keepdims=True)
        tail = jnp.broadcast_to(row, (PAD - PROP, BLOCK))
        for block in range(4):
            pq[b * 4 + block, 0:PROP] = partial_q[b * PROP : (b + 1) * PROP, block * BLOCK : (block + 1) * BLOCK]
            pq[b * 4 + block, PROP:PAD] = tail
    pl.semaphore_wait(barrier, KV - 1 + TP - 1)
    for step in PARTNERS:
        q_copy(step).start()
    for which in range(2):
        loads["wk" if which == 0 else "wv"].wait()
        partial_kv = _dot(gained, wqkv[1 + which])
        for b in range(SEQS):
            for block in range(4):
                pkv[b * 4 + block, which] = partial_kv[
                    b * PROP : (b + 1) * PROP, block * BLOCK : (block + 1) * BLOCK
                ]
    for step in PARTNERS:
        kv_copy(step).start()

    def transpose_values(b):
        loads[("v", b)].wait()
        for block in range(4):
            vt[b, block * BLOCK : (block + 1) * BLOCK, :] = jnp.transpose(
                vbuf[b, :, block * BLOCK : (block + 1) * BLOCK]
            )

    transpose_values(0)
    transpose_values(1)

    for step in PARTNERS:
        q_copy(step).wait_recv()
    total = pq[me]
    for step in range(1, KV):
        total = total + rq[step]
    square_row = total[PROP : PROP + 1]
    square_column = jnp.sum(jnp.where(eye, square_row, 0.0), axis=1, keepdims=True)
    factor = lax.rsqrt(square_column / D + EPS)
    own_q = total[0:PROP] * factor
    zero_tail = jnp.zeros((PAD - PROP, BLOCK), F32)
    qg[me] = jnp.concatenate([own_q, zero_tail], axis=0).astype(BF16)
    for step in PARTNERS:
        qg_copy(step).start()

    for step in PARTNERS:
        kv_copy(step).wait_recv()
    for which in range(2):
        summed = pkv[me, which]
        for step in range(1, KV):
            summed = summed + rkv[step, which]
        kvg[me, which] = jnp.concatenate([summed * factor, zero_tail], axis=0).astype(BF16)
    for step in PARTNERS:
        kvg_copy(step).start()

    transpose_values(2)
    transpose_values(3)
    for b in range(SEQS):
        loads[("k", b)].wait()

    lane = lax.broadcasted_iota(jnp.int32, (HEAD, BLOCK), 1)
    second_head = ((lane >= PROP) & (lane < 2 * PROP)) | (lane >= 3 * PROP)
    for step in PARTNERS:
        qg_copy(step).wait_recv()
    for z_step in (2, 1, 3, 0):
        b = z ^ z_step
        begin = len_ref[b] + acc_ref[b] - me * POS
        position = lax.broadcasted_iota(jnp.int32, (POS, 2 * BLOCK), 0)
        visible = position < begin
        for half in range(2):
            for side in range(2):
                chunk = qg[b * 4 + half * 2 + side, 0:PAD].astype(F32)[0:PROP]
                qe[side * BLOCK : (side + 1) * BLOCK, side * BLOCK : (side + 1) * BLOCK] = _expanded(chunk)
                qe[side * BLOCK : (side + 1) * BLOCK, (1 - side) * BLOCK : (2 - side) * BLOCK] = jnp.zeros(
                    (BLOCK, BLOCK), BF16
                )
            keys = kbuf[b, :, half * 2 * BLOCK : (half + 1) * 2 * BLOCK]
            scores = _dot_nt(keys, qe[...]) * SCALE2
            scores = jnp.where(visible, scores, LOW)
            largest = jnp.max(scores, axis=0, keepdims=True)
            weight = jnp.exp2(scores - largest)
            weight_sum = jnp.sum(weight, axis=0, keepdims=True)
            weight = weight.astype(BF16)
            for side in range(2):
                block = half * 2 + side
                lanes = slice(side * BLOCK, (side + 1) * BLOCK)
                out = _dot(vt[b, block * BLOCK : (block + 1) * BLOCK, :], weight[:, lanes])
                owner = b * 4 + block
                dv[owner] = jnp.where(second_head, out[HEAD:], out[:HEAD]).astype(BF16)
                ds[owner, 0:1] = largest[:, lanes]
                ds[owner, 1:2] = weight_sum[:, lanes]
                ds[owner, 2:8] = jnp.zeros((6, BLOCK), F32)

                def send(block=block):
                    step = (z_step << 2) | (x ^ block)
                    dv_copy(step).start()
                    ds_copy(step).start()

                if z_step == 0:
                    pl.when(x != block)(send)
                else:
                    send()

    par_pad[...] = jnp.full((8, BLOCK), -1, jnp.int32)
    par_pad[0:SEQS, 0:PROP] = par_ref[...]
    parent_row = par_pad[pl.ds(z, 1), :]
    row_index = lax.broadcasted_iota(jnp.int32, (BLOCK, BLOCK), 0)
    lane_index = lax.broadcasted_iota(jnp.int32, (BLOCK, BLOCK), 1)
    reach = ((parent_row == row_index) & (lane_index < PROP)) | (row_index == lane_index)
    reach = jnp.where(reach, 1.0, 0.0).astype(BF16)
    for _ in range(5):
        reach = jnp.minimum(_dot(reach, reach), 1.0).astype(BF16)
    spread = (lax.rem(lane_index, PROP) == row_index) & (lane_index < 4 * PROP) & (row_index < PROP)
    lineage = _dot(reach, jnp.where(spread, 1.0, 0.0).astype(BF16))[0:PAD]
    linked = (lineage > 0.5) & (lax.broadcasted_iota(jnp.int32, (PAD, BLOCK), 0) < PROP)
    own_expanded = _expanded(qg[me].astype(F32)[0:PROP])
    self_scores = _dot_nt(kvg[me, 0], own_expanded) * SCALE2
    self_scores = jnp.where(linked, self_scores, LOW)
    self_max = jnp.max(self_scores, axis=0, keepdims=True)
    self_weight = jnp.where(linked, jnp.exp2(self_scores - self_max), 0.0)
    self_total = jnp.sum(self_weight, axis=0, keepdims=True)
    values_t = jnp.transpose(kvg[me, 1].astype(F32)).astype(BF16)
    self_out = _dot(values_t, self_weight.astype(BF16))
    self_sum = jnp.where(second_head, self_out[HEAD:], self_out[:HEAD])

    for step in PARTNERS:
        ds_copy(step).wait_recv()
    maxima = [ds[me, 0:1]] + [rds[step, 0:1] for step in range(1, KV)]
    totals = [ds[me, 1:2]] + [rds[step, 1:2] for step in range(1, KV)]
    top = functools.reduce(jnp.maximum, maxima, self_max)
    self_factor = jnp.exp2(self_max - top)
    denominator = self_total * self_factor
    factors = []
    for largest, weight_sum in zip(maxima, totals):
        factors.append(jnp.exp2(largest - top))
        denominator = denominator + weight_sum * factors[-1]
    for step in PARTNERS:
        dv_copy(step).wait_recv()
    merged = self_sum * self_factor + dv[me].astype(F32) * factors[0]
    for step in range(1, KV):
        merged = merged + rdv[step].astype(F32) * factors[step]
    attended = merged / denominator
    lane_row = lax.broadcasted_iota(jnp.int32, (1, BLOCK), 1)
    lam = jnp.where(lane_row < PROP, lam_ref[x * 2], lam_ref[x * 2 + 1])
    difference = attended - lam * pltpu.roll(attended, BLOCK - 2 * PROP, 1)
    power = jnp.mean(difference * difference, axis=0, keepdims=True)
    normed = difference * lax.rsqrt(power + EPS)
    stacked = jnp.concatenate([normed, pltpu.roll(normed, BLOCK - PROP, 1)], axis=0)
    turned = jnp.transpose(stacked)[0:PROP]
    turned = turned * og_ref[pl.ds(x, 1), :]
    ng[x, pl.ds(pl.multiple_of(z * PAD, PAD), PAD), :] = jnp.concatenate([turned, zero_tail], axis=0).astype(BF16)
    for step in PARTNERS:
        ng_copy(step).start()

    loads["wo"].wait()
    for step in PARTNERS:
        ng_copy(step).wait_recv()
    rows = jnp.concatenate([ng[block] for block in range(4)], axis=1)
    projected = _dot(rows, wo[...])
    projected = jnp.concatenate([projected[b * PAD : b * PAD + PROP] for b in range(SEQS)], axis=0)
    part[...] = projected.astype(BF16)
    for step in range(1, TP):
        mx_copy(step).start()
    for step in range(1, TP):
        mx_copy(step).wait_recv()
    mixed = part[...].astype(F32)
    for step in range(1, TP):
        mixed = mixed + rpart[step].astype(F32)
    mixed_ref[...] = mixed.astype(BF16)

    for step in PARTNERS:
        kvg_copy(step).wait_recv()
    kvn_ref[...] = kvg[...]
    for step in PARTNERS:
        for copy in (q_copy, kv_copy, qg_copy, kvg_copy, dv_copy, ds_copy, ng_copy):
            copy(step).wait_send()
    for step in range(1, TP):
        mx_copy(step).wait_send()


def _main(tokens, gain, w_query, w_key, w_value, w_output, cache_keys, cache_values, lam, out_gain, parents, lengths, accepted):
    hbm = pl.BlockSpec(memory_space=pl.ANY)
    vmem = pl.BlockSpec(memory_space=pltpu.VMEM)
    smem = pl.BlockSpec(memory_space=pltpu.SMEM)
    dma = pltpu.SemaphoreType.DMA
    return pl.pallas_call(
        _main_kernel,
        out_shape=(
            jax.ShapeDtypeStruct((ROWS, 256), BF16),
            jax.ShapeDtypeStruct((KV, 2, PAD, BLOCK), BF16),
        ),
        in_specs=[hbm, vmem, hbm, hbm, hbm, hbm, hbm, hbm, smem, vmem, vmem, smem, smem],
        out_specs=(vmem, vmem),
        scratch_shapes=[
            pltpu.VMEM((ROWS, 256), BF16),
            pltpu.VMEM((3, 256, 512), BF16),
            pltpu.VMEM((512, 256), BF16),
            pltpu.VMEM((SEQS, POS, 512), BF16),
            pltpu.VMEM((SEQS, POS, 512), BF16),
            pltpu.VMEM((SEQS, 512, POS), BF16),
            pltpu.VMEM((KV, PAD, BLOCK), F32),
            pltpu.VMEM((KV, PAD, BLOCK), F32),
            pltpu.VMEM((KV, 2, PROP, BLOCK), F32),
            pltpu.VMEM((KV, 2, PROP, BLOCK), F32),
            pltpu.VMEM((KV, PAD, BLOCK), BF16),
            pltpu.VMEM((KV, 2, PAD, BLOCK), BF16),
            pltpu.VMEM((KV, HEAD, BLOCK), BF16),
            pltpu.VMEM((KV, HEAD, BLOCK), BF16),
            pltpu.VMEM((KV, 8, BLOCK), F32),
            pltpu.VMEM((KV, 8, BLOCK), F32),
            pltpu.VMEM((4, SEQS * PAD, BLOCK), BF16),
            pltpu.VMEM((ROWS, 256), BF16),
            pltpu.VMEM((TP, ROWS, 256), BF16),
            pltpu.VMEM((8, BLOCK), jnp.int32),
            pltpu.VMEM((2 * BLOCK, 2 * BLOCK), BF16),
            dma((13,)),
        ]
        + [dma((KV,))] * 14
        + [dma((TP,))] * 2,
        compiler_params=pltpu.CompilerParams(
            collective_id=0, has_side_effects=True, vmem_limit_bytes=48 * 1024 * 1024
        ),
        name="attention",
    )(tokens, gain, w_query, w_key, w_value, w_output, cache_keys, cache_values, lam, out_gain, parents, lengths, accepted)


def _cache_kernel(ck_hbm, cv_hbm, kvn_ref, len_ref, acc_ref, nk_hbm, nv_hbm, kbuf, vbuf, in_sem, out_sem):
    me = lax.axis_index("kv")
    pairs = ((ck_hbm, nk_hbm, kbuf), (cv_hbm, nv_hbm, vbuf))

    def fetch(which, b):
        src, _, buf = pairs[which]
        return pltpu.make_async_copy(src.at[b], buf.at[b], in_sem.at[which, b])

    def put(which, b):
        _, dst, buf = pairs[which]
        return pltpu.make_async_copy(buf.at[b], dst.at[b], out_sem.at[which, b])

    for b in range(SEQS):
        for which in range(2):
            fetch(which, b).start()
    for b in range(SEQS):
        begin = len_ref[b] + acc_ref[b] - me * POS
        window = jnp.clip((begin + 8 * PAD) // 16 * 16 - 8 * PAD, 0, POS - 48)
        window = pl.multiple_of(window, 16)
        offset = lax.broadcasted_iota(jnp.int32, (48, PAD), 0) + window - begin
        slot = lax.broadcasted_iota(jnp.int32, (48, PAD), 1)
        placing = jnp.where((offset == slot) & (slot < PROP), 1.0, 0.0).astype(BF16)
        row = lax.broadcasted_iota(jnp.int32, (48, 512), 0) + window - begin
        written = (row >= 0) & (row < PROP)
        for which in range(2):
            fresh = jnp.concatenate([kvn_ref[b * 4 + block, which] for block in range(4)], axis=1)
            moved = _dot(placing, fresh)
            fetch(which, b).wait()
            buf = pairs[which][2]
            old = buf[b, pl.ds(window, 48), :].astype(F32)
            buf[b, pl.ds(window, 48), :] = jnp.where(written, moved, old).astype(BF16)
            put(which, b).start()
    for b in range(SEQS):
        for which in range(2):
            put(which, b).wait()


def _caches(cache_keys, cache_values, fresh, lengths, accepted):
    hbm = pl.BlockSpec(memory_space=pl.ANY)
    smem = pl.BlockSpec(memory_space=pltpu.SMEM)
    return pl.pallas_call(
        _cache_kernel,
        out_shape=(
            jax.ShapeDtypeStruct(cache_keys.shape, BF16),
            jax.ShapeDtypeStruct(cache_values.shape, BF16),
        ),
        in_specs=[hbm, hbm, pl.BlockSpec(memory_space=pltpu.VMEM), smem, smem],
        out_specs=(hbm, hbm),
        scratch_shapes=[
            pltpu.VMEM((SEQS, POS, 512), BF16),
            pltpu.VMEM((SEQS, POS, 512), BF16),
            pltpu.SemaphoreType.DMA((2, SEQS)),
            pltpu.SemaphoreType.DMA((2, SEQS)),
        ],
        name="caches",
    )(cache_keys, cache_values, fresh, lengths, accepted)


def _local(
    tokens,
    norm_gain,
    w_query,
    w_key,
    w_value,
    w_output,
    cache_keys,
    cache_values,
    map_lambda,
    out_gain,
    parents,
    lengths,
    accepted,
):
    mixed, fresh = _main(
        tokens,
        norm_gain.reshape(1, 256),
        w_query,
        w_key,
        w_value,
        w_output,
        cache_keys,
        cache_values,
        map_lambda,
        out_gain.reshape(4, BLOCK),
        parents,
        lengths,
        accepted,
    )
    new_keys, new_values = _caches(cache_keys, cache_values, fresh, lengths, accepted)
    return mixed, new_keys, new_values


def solution(mesh):
    return jax.shard_map(
        _local,
        mesh=mesh,
        in_specs=(
            P(None, "kv"),
            P("kv"),
            P("kv", "tp"),
            P("kv", "tp"),
            P("kv", "tp"),
            P("tp", "kv"),
            P(None, "kv", "tp"),
            P(None, "kv", "tp"),
            P("tp"),
            P("tp"),
            P(),
            P(),
            P(),
        ),
        out_specs=(P(None, "kv"), P(None, "kv", "tp"), P(None, "kv", "tp")),
        check_vma=False,
    )
```

```python
import functools

import jax
import jax.numpy as jnp
from jax import lax
from jax.experimental import pallas as pl
from jax.experimental.pallas import tpu as pltpu
from jax.sharding import PartitionSpec as P

D = 4096
HEAD = 64
QK = 32
SEQS = 4
PROP = 24
KV = 16
TP = 8
BLOCK = 128
PAD = 32
POS = 512
ROWS = 96
EPS = 1e-05
LOW = -1e30
LOG2E = 1.4426950408889634
WRITE_VMEM = 16 * 1024 * 1024
MAIN_VMEM = 40 * 1024 * 1024
SCALE2 = QK ** (-0.5) * LOG2E
F32 = jnp.float32
BF16 = jnp.bfloat16
NT = (((1,), (1,)), ((), ()))


def _distance(step):
    ring = (0, 1, 2, 1)
    return ring[step >> 2] + ring[step & 3]


Z_ORDER = (0, 2, 1, 3)
PARTNERS = sorted(range(1, KV), key=lambda step: -_distance(step))


def _dot(a, b):
    return jnp.dot(a, b, preferred_element_type=F32)


def _dot_nt(a, b):
    return lax.dot_general(a, b, NT, preferred_element_type=F32)


def _split_rows(row):
    high = row.astype(BF16).astype(F32)
    middle = (row - high).astype(BF16).astype(F32)
    low = row - high - middle
    index = lax.broadcasted_iota(jnp.int32, (PAD - PROP, BLOCK), 0)
    return jnp.where(index == 0, high, jnp.where(index == 1, middle, jnp.where(index == 2, low, 0.0)))


def _expanded(chunk):
    lane = lax.broadcasted_iota(jnp.int32, (PROP, BLOCK), 1)
    parts = []
    for which in range(2):
        for head in range(2):
            low = head * HEAD + which * QK
            inside = (lane >= low) & (lane < low + QK)
            parts.append(jnp.where(inside, chunk, 0.0))
    parts.append(jnp.zeros((BLOCK - 4 * PROP, BLOCK), F32))
    return jnp.concatenate(parts, axis=0).astype(BF16)


def _main_kernel(
    tok_hbm,
    gain_hbm,
    wq_hbm,
    wk_hbm,
    wv_hbm,
    wo_hbm,
    ck_hbm,
    cv_hbm,
    lam_hbm,
    og_hbm,
    par_hbm,
    len_hbm,
    acc_hbm,
    mixed_ref,
    kbuf,
    vbuf,
    tok,
    gain_ref,
    og_ref,
    par_ref,
    lam_ref,
    len_ref,
    acc_ref,
    wqkv,
    wo,
    vt,
    pq,
    rq,
    pkv,
    rkv,
    qg,
    kvg,
    dv,
    rdv,
    ds,
    rds,
    ng,
    part,
    rpart,
    par_pad,
    qe,
    load_sem,
    q_send,
    q_recv,
    kv_send,
    kv_recv,
    qg_send,
    qg_recv,
    kvg_send,
    kvg_recv,
    dv_send,
    dv_recv,
    ds_send,
    ds_recv,
    ng_send,
    ng_recv,
    mx_send,
    mx_recv,
):
    me = lax.axis_index("kv")
    tp = lax.axis_index("tp")
    z = me // 4
    x = lax.rem(me, 4)

    barrier = pltpu.get_barrier_semaphore()
    for step in PARTNERS:
        pl.semaphore_signal(barrier, inc=1, device_id={"kv": me ^ step}, device_id_type=pl.DeviceIdType.MESH)
    for step in range(1, TP):
        pl.semaphore_signal(barrier, inc=1, device_id={"tp": tp ^ step}, device_id_type=pl.DeviceIdType.MESH)

    loads = {}

    def load(name, src, dst, index):
        copy = pltpu.make_async_copy(src, dst, load_sem.at[index])
        copy.start()
        loads[name] = copy

    load("tok", tok_hbm, tok, 0)
    load("gain", gain_hbm, gain_ref, 13)
    load("wq", wq_hbm, wqkv.at[0], 1)
    load("wk", wk_hbm, wqkv.at[1], 2)
    load("wv", wv_hbm, wqkv.at[2], 3)
    for b in range(SEQS):
        load(("v", b), cv_hbm.at[b], vbuf.at[b], 4 + b)
    for b in range(SEQS):
        load(("k", b), ck_hbm.at[b], kbuf.at[b], 8 + b)
    load("wo", wo_hbm, wo, 12)
    load("og", og_hbm, og_ref, 14)
    load("par", par_hbm, par_ref, 15)
    load("lam", lam_hbm, lam_ref, 16)
    load("len", len_hbm, len_ref, 17)
    load("acc", acc_hbm, acc_ref, 18)

    def to_kv(step, src, dst, send, recv):
        return pltpu.make_async_remote_copy(
            src_ref=src,
            dst_ref=dst,
            send_sem=send.at[step],
            recv_sem=recv.at[step],
            device_id={"kv": me ^ step},
            device_id_type=pl.DeviceIdType.MESH,
        )

    def q_copy(step):
        return to_kv(step, pq.at[me ^ step], rq.at[step], q_send, q_recv)

    def kv_copy(step):
        return to_kv(step, pkv.at[me ^ step], rkv.at[step], kv_send, kv_recv)

    def qg_copy(step):
        return to_kv(step, qg.at[me], qg.at[me], qg_send, qg_recv)

    def kvg_copy(step):
        return to_kv(step, kvg.at[me], kvg.at[me], kvg_send, kvg_recv)

    def dv_copy(step):
        return to_kv(step, dv.at[me ^ step], rdv.at[step], dv_send, dv_recv)

    def ds_copy(step):
        return to_kv(step, ds.at[me ^ step], rds.at[step], ds_send, ds_recv)

    def ng_slot():
        return ng.at[x, pl.ds(pl.multiple_of(z * PAD, PAD), PAD), :]

    def ng_copy(step):
        return to_kv(step, ng_slot(), ng_slot(), ng_send, ng_recv)

    def mx_copy(far, step):
        return pltpu.make_async_remote_copy(
            src_ref=part.at[z // 2 ^ far],
            dst_ref=rpart.at[far, step],
            send_sem=mx_send.at[far, step],
            recv_sem=mx_recv.at[far, step],
            device_id={"tp": tp ^ step},
            device_id_type=pl.DeviceIdType.MESH,
        )

    loads["tok"].wait()
    loads["gain"].wait()
    wide = tok[...].astype(F32)
    gained = (wide * gain_ref[...]).astype(BF16)
    square = jnp.sum(wide * wide, axis=1, keepdims=True)
    eye = lax.broadcasted_iota(jnp.int32, (PROP, BLOCK), 0) == lax.broadcasted_iota(jnp.int32, (PROP, BLOCK), 1)
    loads["wq"].wait()
    partial_q = _dot(gained, wqkv[0])
    for b in range(SEQS):
        column = square[b * PROP : (b + 1) * PROP]
        row = jnp.sum(jnp.where(eye, column, 0.0), axis=0, keepdims=True)
        tail = _split_rows(row)
        for block in range(4):
            chunk = partial_q[b * PROP : (b + 1) * PROP, block * BLOCK : (block + 1) * BLOCK]
            pq[b * 4 + block] = jnp.concatenate([chunk, tail], axis=0).astype(BF16)
    pl.semaphore_wait(barrier, KV - 1 + TP - 1)
    for step in PARTNERS:
        q_copy(step).start()
    projected = []
    for which in range(2):
        loads["wk" if which == 0 else "wv"].wait()
        projected.append(_dot(gained, wqkv[1 + which]))
    for b in range(SEQS):
        for block in range(4):
            pkv[b * 4 + block] = jnp.concatenate(
                [
                    part_kv[b * PROP : (b + 1) * PROP, block * BLOCK : (block + 1) * BLOCK]
                    for part_kv in projected
                ],
                axis=0,
            ).astype(BF16)
    def transpose_values(b):
        loads[("v", b)].wait()
        for block in range(4):
            vt[b, block * BLOCK : (block + 1) * BLOCK, :] = jnp.transpose(
                vbuf[b, :, block * BLOCK : (block + 1) * BLOCK]
            )

    for order in range(SEQS):
        for half in range(2):
            for side in range(2):
                qe[order, half, side * BLOCK : (side + 1) * BLOCK, (1 - side) * BLOCK : (2 - side) * BLOCK] = (
                    jnp.zeros((BLOCK, BLOCK), BF16)
                )
    transpose_values(0)
    transpose_values(1)

    for step in PARTNERS:
        q_copy(step).wait_recv()
    total = pq[me].astype(F32)
    for step in range(1, KV):
        total = total + rq[step].astype(F32)
    square_row = jnp.sum(total[PROP:PAD], axis=0, keepdims=True)
    square_column = jnp.sum(jnp.where(eye, square_row, 0.0), axis=1, keepdims=True)
    factor = lax.rsqrt(square_column / D + EPS)
    own_q = total[0:PROP] * factor
    zero_tail = jnp.zeros((PAD - PROP, BLOCK), F32)
    qg[me] = jnp.concatenate([own_q, zero_tail], axis=0).astype(BF16)
    for step in PARTNERS:
        qg_copy(step).start()

    for step in PARTNERS:
        kv_copy(step).start()
    transpose_values(2)
    transpose_values(3)
    for b in range(SEQS):
        loads[("k", b)].wait()
    for name in ("og", "par", "lam", "len", "acc"):
        loads[name].wait()

    lane = lax.broadcasted_iota(jnp.int32, (HEAD, BLOCK), 1)
    second_head = ((lane >= PROP) & (lane < 2 * PROP)) | (lane >= 3 * PROP)
    for order, z_step in enumerate(Z_ORDER):
        for step in PARTNERS:
            if step >> 2 == z_step:
                qg_copy(step).wait_recv()
        b = z ^ z_step
        begin = len_ref[b] + acc_ref[b] - me * POS
        visible = lax.broadcasted_iota(jnp.int32, (POS, BLOCK), 0) < begin
        visible = jnp.concatenate([visible, visible], axis=1)
        for half in range(2):
            for side in range(2):
                chunk = qg[b * 4 + half * 2 + side].astype(F32)[0:PROP]
                lanes = slice(side * BLOCK, (side + 1) * BLOCK)
                qe[order, half, lanes, lanes] = _expanded(chunk)
        for half in range(2):
            keys = kbuf[b, :, half * 2 * BLOCK : (half + 1) * 2 * BLOCK]
            scores = _dot_nt(keys, qe[order, half]) * SCALE2
            scores = jnp.where(visible, scores, LOW)
            largest = jnp.max(scores, axis=0, keepdims=True)
            weight = jnp.exp2(scores - largest)
            weight_sum = jnp.sum(weight, axis=0, keepdims=True)
            weight = weight.astype(BF16)
            for side in range(2):
                block = half * 2 + side
                lanes = slice(side * BLOCK, (side + 1) * BLOCK)
                out = _dot(vt[b, block * BLOCK : (block + 1) * BLOCK, :], weight[:, lanes])
                owner = b * 4 + block
                dv[owner] = jnp.where(second_head, out[HEAD:], out[:HEAD]).astype(BF16)
                ds[owner] = jnp.concatenate(
                    [jnp.broadcast_to(largest[:, lanes], (4, BLOCK)), jnp.broadcast_to(weight_sum[:, lanes], (4, BLOCK))],
                    axis=0,
                )
        for x_step in (2, 1, 3, 0):
            step = z_step << 2 | x_step
            if step:
                dv_copy(step).start()
                ds_copy(step).start()

    for step in PARTNERS:
        kv_copy(step).wait_recv()
    summed = pkv[me].astype(F32)
    for step in range(1, KV):
        summed = summed + rkv[step].astype(F32)
    own_k = jnp.concatenate([summed[0:PROP] * factor, zero_tail], axis=0).astype(BF16)
    own_v = jnp.concatenate([summed[PROP:] * factor, zero_tail], axis=0)
    kvg[me] = jnp.concatenate([summed[0:PROP] * factor, summed[PROP:] * factor], axis=0).astype(BF16)
    for step in PARTNERS:
        kvg_copy(step).start()
    par_pad[...] = jnp.full((8, BLOCK), -1, jnp.int32)
    par_pad[0:SEQS, 0:PROP] = par_ref[...]
    parent_row = par_pad[pl.ds(z, 1), :]
    row_index = lax.broadcasted_iota(jnp.int32, (BLOCK, BLOCK), 0)
    lane_index = lax.broadcasted_iota(jnp.int32, (BLOCK, BLOCK), 1)
    reach = ((parent_row == row_index) & (lane_index < PROP)) | (row_index == lane_index)
    reach = jnp.where(reach, 1.0, 0.0).astype(BF16)
    for _ in range(5):
        reach = jnp.minimum(_dot(reach, reach), 1.0).astype(BF16)
    spread = (lax.rem(lane_index, PROP) == row_index) & (lane_index < 4 * PROP) & (row_index < PROP)
    lineage = _dot(reach, jnp.where(spread, 1.0, 0.0).astype(BF16))[0:PAD]
    linked = (lineage > 0.5) & (lax.broadcasted_iota(jnp.int32, (PAD, BLOCK), 0) < PROP)
    own_expanded = _expanded(qg[me].astype(F32)[0:PROP])
    self_scores = _dot_nt(own_k, own_expanded) * SCALE2
    self_scores = jnp.where(linked, self_scores, LOW)
    self_max = jnp.max(self_scores, axis=0, keepdims=True)
    self_weight = jnp.where(linked, jnp.exp2(self_scores - self_max), 0.0)
    self_total = jnp.sum(self_weight, axis=0, keepdims=True)
    values_t = jnp.transpose(own_v).astype(BF16)
    self_out = _dot(values_t, self_weight.astype(BF16))
    self_sum = jnp.where(second_head, self_out[HEAD:], self_out[:HEAD])

    for step in PARTNERS:
        ds_copy(step).wait_recv()
    maxima = [ds[me, 0:1]] + [rds[step, 0:1] for step in range(1, KV)]
    totals = [ds[me, 4:5]] + [rds[step, 4:5] for step in range(1, KV)]
    top = functools.reduce(jnp.maximum, maxima, self_max)
    self_factor = jnp.exp2(self_max - top)
    denominator = self_total * self_factor
    factors = []
    for largest, weight_sum in zip(maxima, totals):
        factors.append(jnp.exp2(largest - top))
        denominator = denominator + weight_sum * factors[-1]
    for step in PARTNERS:
        dv_copy(step).wait_recv()
    merged = self_sum * self_factor + dv[me].astype(F32) * factors[0]
    for step in range(1, KV):
        merged = merged + rdv[step].astype(F32) * factors[step]
    attended = merged / denominator
    lane_row = lax.broadcasted_iota(jnp.int32, (1, BLOCK), 1)
    lam = jnp.where(lane_row < PROP, lam_ref[x * 2], lam_ref[x * 2 + 1])
    difference = attended - lam * pltpu.roll(attended, BLOCK - 2 * PROP, 1)
    power = jnp.mean(difference * difference, axis=0, keepdims=True)
    normed = difference * lax.rsqrt(power + EPS)
    stacked = jnp.concatenate([normed, pltpu.roll(normed, BLOCK - PROP, 1)], axis=0)
    turned = jnp.transpose(stacked)[0:PROP]
    turned = turned * og_ref[pl.ds(x, 1), :]
    ng[x, pl.ds(pl.multiple_of(z * PAD, PAD), PAD), :] = jnp.concatenate([turned, zero_tail], axis=0).astype(BF16)
    for step in PARTNERS:
        ng_copy(step).start()

    loads["wo"].wait()
    for far in range(2):
        for step in PARTNERS:
            if step >> 3 == far:
                ng_copy(step).wait_recv()
        pair = z // 2 ^ far
        first = pl.multiple_of(pair * 2 * PAD, 2 * PAD)
        rows = jnp.concatenate([ng[block, pl.ds(first, 2 * PAD), :] for block in range(4)], axis=1)
        projected = _dot(rows, wo[...])
        projected = jnp.concatenate([projected[0:PROP], projected[PAD : PAD + PROP]], axis=0)
        part[pair] = projected.astype(BF16)
        for step in range(1, TP):
            mx_copy(far, step).start()

    for step in PARTNERS:
        kvg_copy(step).wait_recv()
    for b in range(SEQS):
        begin = len_ref[b] + acc_ref[b] - me * POS
        position = lax.broadcasted_iota(jnp.int32, (POS, BLOCK), 0) - begin
        written = (position >= 0) & (position < PROP)
        slot = lax.broadcasted_iota(jnp.int32, (POS, BLOCK), 1)
        for which, buf in enumerate((kbuf, vbuf)):
            offset = which * PROP
            placing = jnp.where(written & (position + offset == slot), 1.0, 0.0).astype(BF16)[:, 0 : 2 * PROP]
            for block in range(4):
                lanes = slice(block * BLOCK, (block + 1) * BLOCK)
                moved = _dot(placing, kvg[b * 4 + block])
                buf[b, :, lanes] = jnp.where(written, moved, buf[b, :, lanes].astype(F32)).astype(BF16)

    for far in range(2):
        for step in range(1, TP):
            mx_copy(far, step).wait_recv()
        pair = z // 2 ^ far
        mixed = part[pair].astype(F32)
        for step in range(1, TP):
            mixed = mixed + rpart[far, step].astype(F32)
        mixed_ref[pair] = mixed.astype(BF16)

    for step in PARTNERS:
        for copy in (q_copy, kv_copy, qg_copy, kvg_copy, dv_copy, ds_copy, ng_copy):
            copy(step).wait_send()
    for far in range(2):
        for step in range(1, TP):
            mx_copy(far, step).wait_send()


def _main(*arrays):
    hbm = pl.BlockSpec(memory_space=pltpu.HBM)
    vmem = pl.BlockSpec(memory_space=pltpu.VMEM)
    dma = pltpu.SemaphoreType.DMA
    return pl.pallas_call(
        _main_kernel,
        out_shape=(
            jax.ShapeDtypeStruct((2, 2 * PROP, 256), BF16),
            jax.ShapeDtypeStruct((SEQS, POS, 512), BF16),
            jax.ShapeDtypeStruct((SEQS, POS, 512), BF16),
        ),
        in_specs=[hbm] * 13,
        out_specs=(vmem,) * 3,
        scratch_shapes=[
            pltpu.VMEM((ROWS, 256), BF16),
            pltpu.VMEM((1, 256), F32),
            pltpu.VMEM((4, BLOCK), F32),
            pltpu.VMEM((SEQS, PROP), jnp.int32),
            pltpu.SMEM((TP,), F32),
            pltpu.SMEM((SEQS,), jnp.int32),
            pltpu.SMEM((SEQS,), jnp.int32),
            pltpu.VMEM((3, 256, 512), BF16),
            pltpu.VMEM((512, 256), BF16),
            pltpu.VMEM((SEQS, 512, POS), BF16),
            pltpu.VMEM((KV, PAD, BLOCK), BF16),
            pltpu.VMEM((KV, PAD, BLOCK), BF16),
            pltpu.VMEM((KV, 2 * PROP, BLOCK), BF16),
            pltpu.VMEM((KV, 2 * PROP, BLOCK), BF16),
            pltpu.VMEM((KV, PAD, BLOCK), BF16),
            pltpu.VMEM((KV, 2 * PROP, BLOCK), BF16),
            pltpu.VMEM((KV, HEAD, BLOCK), BF16),
            pltpu.VMEM((KV, HEAD, BLOCK), BF16),
            pltpu.VMEM((KV, 8, BLOCK), F32),
            pltpu.VMEM((KV, 8, BLOCK), F32),
            pltpu.VMEM((4, SEQS * PAD, BLOCK), BF16),
            pltpu.VMEM((2, 2 * PROP, 256), BF16),
            pltpu.VMEM((2, TP, 2 * PROP, 256), BF16),
            pltpu.VMEM((8, BLOCK), jnp.int32),
            pltpu.VMEM((SEQS, 2, 2 * BLOCK, 2 * BLOCK), BF16),
            dma((19,)),
        ]
        + [dma((KV,))] * 14
        + [dma((2, TP))] * 2,
        compiler_params=pltpu.CompilerParams(
            collective_id=0, has_side_effects=True, vmem_limit_bytes=MAIN_VMEM
        ),
        name="attention",
    )(*(pltpu.with_memory_space_constraint(array, pltpu.HBM) for array in arrays))


def _write_kernel(mixed_ref, keys_ref, values_ref, mixed_hbm, keys_hbm, values_hbm, sem):
    copies = [pltpu.make_async_copy(mixed_ref, mixed_hbm, sem.at[0])]
    for b in range(SEQS):
        copies.append(pltpu.make_async_copy(keys_ref.at[b], keys_hbm.at[b], sem.at[1 + b]))
        copies.append(pltpu.make_async_copy(values_ref.at[b], values_hbm.at[b], sem.at[1 + SEQS + b]))
    for copy in copies:
        copy.start()
    for copy in copies:
        copy.wait()


def _write(*arrays):
    hbm = pl.BlockSpec(memory_space=pltpu.HBM)
    vmem = pl.BlockSpec(memory_space=pltpu.VMEM)
    return pl.pallas_call(
        _write_kernel,
        out_shape=tuple(jax.ShapeDtypeStruct(array.shape, array.dtype) for array in arrays),
        in_specs=[vmem] * 3,
        out_specs=(hbm,) * 3,
        scratch_shapes=[pltpu.SemaphoreType.DMA((1 + 2 * SEQS,))],
        compiler_params=pltpu.CompilerParams(vmem_limit_bytes=WRITE_VMEM),
        name="write",
    )(*arrays)


def _local(
    tokens,
    norm_gain,
    w_query,
    w_key,
    w_value,
    w_output,
    cache_keys,
    cache_values,
    map_lambda,
    out_gain,
    parents,
    lengths,
    accepted,
):
    mixed, keys, values = _main(
        tokens,
        norm_gain.reshape(1, 256),
        w_query,
        w_key,
        w_value,
        w_output,
        cache_keys,
        cache_values,
        map_lambda,
        out_gain.reshape(4, BLOCK),
        parents,
        lengths,
        accepted,
    )
    mixed, new_keys, new_values = _write(mixed, keys, values)
    return mixed.reshape(ROWS, 256), new_keys, new_values


def solution(mesh):
    return jax.shard_map(
        _local,
        mesh=mesh,
        in_specs=(
            P(None, "kv"),
            P("kv"),
            P("kv", "tp"),
            P("kv", "tp"),
            P("kv", "tp"),
            P("tp", "kv"),
            P(None, "kv", "tp"),
            P(None, "kv", "tp"),
            P("tp"),
            P("tp"),
            P(),
            P(),
            P(),
        ),
        out_specs=(P(None, "kv"), P(None, "kv", "tp"), P(None, "kv", "tp")),
        check_vma=False,
    )
```

```python
import functools

import jax
import jax.numpy as jnp
from jax import lax
from jax.experimental import pallas as pl
from jax.experimental.pallas import tpu as pltpu
from jax.sharding import PartitionSpec as P

D = 4096
HEAD = 64
QK = 32
SEQS = 4
PROP = 24
KV = 16
TP = 8
BLOCK = 128
PAD = 32
POS = 512
ROWS = 96
EPS = 1e-05
LOW = -1e30
LOG2E = 1.4426950408889634
WRITE_VMEM = 16 * 1024 * 1024
MAIN_VMEM = 40 * 1024 * 1024
SCALE2 = QK ** (-0.5) * LOG2E
F32 = jnp.float32
BF16 = jnp.bfloat16
NT = (((1,), (1,)), ((), ()))


def _distance(step):
    ring = (0, 1, 2, 1)
    return ring[step >> 2] + ring[step & 3]


Q_SEND = 0
KV_SEND = 1
QG_SEND = 2
KVG_SEND = 3
DV_SEND = 4
DS_SEND = 5
NG_SEND = 6
MX_SEND = 7
Q_RECV = 8
KV_RECV = 9
KVG_RECV = 10
DV_RECV = 11
DS_RECV = 12
QG_RECV = 13
NG_RECV = 17
MX_RECV = 21
SEMAPHORES = 25
Z_ORDER = (0, 2, 1, 3)
Z_OUT = (0, 1, 3, 2)
TP_ORDER = (4, 5, 2, 3, 6, 7, 1)
PARTNERS = sorted(range(1, KV), key=lambda step: -_distance(step))


def _dot(a, b):
    return jnp.dot(a, b, preferred_element_type=F32)


def _dot_nt(a, b):
    return lax.dot_general(a, b, NT, preferred_element_type=F32)


def _split_rows(row):
    high = row.astype(BF16).astype(F32)
    middle = (row - high).astype(BF16).astype(F32)
    low = row - high - middle
    index = lax.broadcasted_iota(jnp.int32, (PAD - PROP, BLOCK), 0)
    return jnp.where(index == 0, high, jnp.where(index == 1, middle, jnp.where(index == 2, low, 0.0)))


def _packed(block):
    rest = block[48:]
    moved = jnp.concatenate([pltpu.roll(rest, 96 - 32 * part, 1) for part in range(3)], axis=0)
    return jnp.where(lax.broadcasted_iota(jnp.int32, (48, BLOCK), 1) < 96, block[:48], moved)


def _unpacked(packed):
    lane = lax.broadcasted_iota(jnp.int32, (16, BLOCK), 1)
    parts = [pltpu.roll(packed[16 * part : 16 * part + 16], 32 * part + 32, 1) for part in range(3)]
    rest = jnp.where(lane < 32, parts[0], jnp.where(lane < 64, parts[1], parts[2]))
    return jnp.concatenate([packed, rest], axis=0)


def _expanded(chunk):
    lane = lax.broadcasted_iota(jnp.int32, (PROP, BLOCK), 1)
    parts = []
    for which in range(2):
        for head in range(2):
            low = head * HEAD + which * QK
            inside = (lane >= low) & (lane < low + QK)
            parts.append(jnp.where(inside, chunk, 0.0))
    parts.append(jnp.zeros((BLOCK - 4 * PROP, BLOCK), F32))
    return jnp.concatenate(parts, axis=0).astype(BF16)


def _main_kernel(
    tok_hbm,
    gain_hbm,
    wq_hbm,
    wk_hbm,
    wv_hbm,
    wo_hbm,
    ck_hbm,
    cv_hbm,
    lam_hbm,
    og_hbm,
    par_hbm,
    len_hbm,
    acc_hbm,
    mixed_ref,
    keys_out,
    values_out,
    kbuf,
    vbuf,
    tok,
    gain_ref,
    og_ref,
    par_ref,
    lam_ref,
    len_ref,
    acc_ref,
    wqkv,
    wo,
    vt,
    pq,
    rq,
    pkv,
    rkv,
    qg,
    kvg,
    dv,
    rdv,
    ds,
    rds,
    ng,
    part,
    rpart,
    par_pad,
    qe,
    load_sem,
    sems,
    out_sem,
):
    me = lax.axis_index("kv")
    tp = lax.axis_index("tp")
    z = me // 4
    x = lax.rem(me, 4)

    barrier = pltpu.get_barrier_semaphore()
    for step in PARTNERS:
        pl.semaphore_signal(barrier, inc=1, device_id={"kv": me ^ step}, device_id_type=pl.DeviceIdType.MESH)
    for step in range(1, TP):
        pl.semaphore_signal(barrier, inc=1, device_id={"tp": tp ^ step}, device_id_type=pl.DeviceIdType.MESH)

    loads = [
        (tok_hbm, tok),
        (gain_hbm, gain_ref),
        (wq_hbm, wqkv.at[0]),
        (wk_hbm, wqkv.at[1]),
        (wv_hbm, wqkv.at[2]),
        (cv_hbm, vbuf),
        (ck_hbm, kbuf),
        (wo_hbm, wo),
        (og_hbm, og_ref),
        (par_hbm, par_ref),
        (lam_hbm, lam_ref),
        (len_hbm, len_ref),
        (acc_hbm, acc_ref),
    ]
    loads = [pltpu.make_async_copy(src, dst, load_sem.at[index]) for index, (src, dst) in enumerate(loads)]
    for copy in loads:
        copy.start()

    def arrived(ref, sem):
        pltpu.make_async_copy(ref, ref, sem).wait()

    def to_kv(step, src, dst, send, recv):
        return pltpu.make_async_remote_copy(
            src_ref=src,
            dst_ref=dst,
            send_sem=send,
            recv_sem=recv,
            device_id={"kv": me ^ step},
            device_id_type=pl.DeviceIdType.MESH,
        )

    def q_copy(step):
        return to_kv(step, pq.at[me ^ step], rq.at[step], sems.at[Q_SEND], sems.at[Q_RECV])

    def kv_copy(step):
        return to_kv(step, pkv.at[me ^ step], rkv.at[step], sems.at[KV_SEND], sems.at[KV_RECV])

    def qg_copy(step):
        return to_kv(step, qg.at[me], qg.at[me], sems.at[QG_SEND], sems.at[QG_RECV + (step >> 2)])

    def kvg_copy(step):
        return to_kv(step, kvg.at[me], kvg.at[me], sems.at[KVG_SEND], sems.at[KVG_RECV])

    def dv_copy(step):
        return to_kv(step, dv.at[me ^ step], rdv.at[step], sems.at[DV_SEND], sems.at[DV_RECV])

    def ds_copy(step):
        return to_kv(step, ds.at[me ^ step], rds.at[step], sems.at[DS_SEND], sems.at[DS_RECV])

    def ng_copy(step):
        return to_kv(step, ng.at[me], ng.at[me], sems.at[NG_SEND], sems.at[NG_RECV + (step >> 2)])

    def mx_copy(z_step, step):
        return pltpu.make_async_remote_copy(
            src_ref=part.at[z ^ z_step],
            dst_ref=rpart.at[z_step, step],
            send_sem=sems.at[MX_SEND],
            recv_sem=sems.at[MX_RECV + z_step],
            device_id={"tp": tp ^ step},
            device_id_type=pl.DeviceIdType.MESH,
        )

    def out_copy(which, b):
        buf, out = ((kbuf, keys_out), (vbuf, values_out))[which]
        return pltpu.make_async_copy(buf.at[b], out.at[b], out_sem.at[which])

    loads[0].wait()
    loads[1].wait()
    wide = tok[...].astype(F32)
    gained = (wide * gain_ref[...]).astype(BF16)
    square = jnp.sum(wide * wide, axis=1, keepdims=True)
    eye = lax.broadcasted_iota(jnp.int32, (PROP, BLOCK), 0) == lax.broadcasted_iota(jnp.int32, (PROP, BLOCK), 1)
    loads[2].wait()
    partial_q = _dot(gained, wqkv[0])
    for b in range(SEQS):
        column = square[b * PROP : (b + 1) * PROP]
        row = jnp.sum(jnp.where(eye, column, 0.0), axis=0, keepdims=True)
        tail = _split_rows(row)
        for block in range(4):
            chunk = partial_q[b * PROP : (b + 1) * PROP, block * BLOCK : (block + 1) * BLOCK]
            pq[b * 4 + block] = jnp.concatenate([chunk, tail], axis=0).astype(BF16)
    pl.semaphore_wait(barrier, KV - 1 + TP - 1)
    for step in PARTNERS:
        q_copy(step).start()
    projected = []
    for which in range(2):
        loads[3 + which].wait()
        projected.append(_dot(gained, wqkv[1 + which]))
    for b in range(SEQS):
        for block in range(4):
            pkv[b * 4 + block] = jnp.concatenate(
                [
                    part_kv[b * PROP : (b + 1) * PROP, block * BLOCK : (block + 1) * BLOCK]
                    for part_kv in projected
                ],
                axis=0,
            ).astype(BF16)
    loads[5].wait()

    def transpose_values(b):
        for block in range(4):
            vt[b, block * BLOCK : (block + 1) * BLOCK, :] = jnp.transpose(
                vbuf[b, :, block * BLOCK : (block + 1) * BLOCK]
            )

    for order in range(SEQS):
        for half in range(2):
            for side in range(2):
                qe[order, half, side * BLOCK : (side + 1) * BLOCK, (1 - side) * BLOCK : (2 - side) * BLOCK] = (
                    jnp.zeros((BLOCK, BLOCK), BF16)
                )
    transpose_values(0)
    transpose_values(1)

    arrived(rq.at[1:], sems.at[Q_RECV])
    total = pq[me].astype(F32)
    for step in range(1, KV):
        total = total + rq[step].astype(F32)
    square_row = jnp.sum(total[PROP:PAD], axis=0, keepdims=True)
    square_column = jnp.sum(jnp.where(eye, square_row, 0.0), axis=1, keepdims=True)
    factor = lax.rsqrt(square_column / D + EPS)
    own_q = total[0:PROP] * factor
    zero_tail = jnp.zeros((PAD - PROP, BLOCK), F32)
    qg[me] = own_q.astype(BF16)
    for z_step in Z_ORDER:
        for step in PARTNERS:
            if step >> 2 == z_step:
                qg_copy(step).start()

    for step in PARTNERS:
        kv_copy(step).start()
    transpose_values(2)
    transpose_values(3)
    for copy in [loads[6]] + loads[8:]:
        copy.wait()

    lane = lax.broadcasted_iota(jnp.int32, (HEAD, BLOCK), 1)
    second_head = ((lane >= PROP) & (lane < 2 * PROP)) | (lane >= 3 * PROP)
    for order, z_step in enumerate(Z_ORDER):
        arrived(qg.at[pl.ds((z ^ z_step) * 4, 4 if z_step else 3)], sems.at[QG_RECV + z_step])
        b = z ^ z_step
        begin = len_ref[b] + acc_ref[b] - me * POS
        visible = lax.broadcasted_iota(jnp.int32, (POS, BLOCK), 0) < begin
        visible = jnp.concatenate([visible, visible], axis=1)
        for half in range(2):
            for side in range(2):
                chunk = qg[b * 4 + half * 2 + side].astype(F32)
                lanes = slice(side * BLOCK, (side + 1) * BLOCK)
                qe[order, half, lanes, lanes] = _expanded(chunk)
        for half in range(2):
            keys = kbuf[b, :, half * 2 * BLOCK : (half + 1) * 2 * BLOCK]
            scores = _dot_nt(keys, qe[order, half]) * SCALE2
            scores = jnp.where(visible, scores, LOW)
            largest = jnp.max(scores, axis=0, keepdims=True)
            weight = jnp.exp2(scores - largest)
            weight_sum = jnp.sum(weight, axis=0, keepdims=True)
            weight = weight.astype(BF16)
            for side in range(2):
                block = half * 2 + side
                lanes = slice(side * BLOCK, (side + 1) * BLOCK)
                out = _dot(vt[b, block * BLOCK : (block + 1) * BLOCK, :], weight[:, lanes])
                owner = b * 4 + block
                dv[owner] = _packed(jnp.where(second_head, out[HEAD:], out[:HEAD])).astype(BF16)
                ds[owner] = jnp.concatenate([largest[:, lanes], weight_sum[:, lanes]], axis=0)
        for x_step in (2, 1, 3, 0):
            step = z_step << 2 | x_step
            if step:
                dv_copy(step).start()
                ds_copy(step).start()

    arrived(rkv.at[1:], sems.at[KV_RECV])
    summed = pkv[me].astype(F32)
    for step in range(1, KV):
        summed = summed + rkv[step].astype(F32)
    own_k = jnp.concatenate([summed[0:PROP] * factor, zero_tail], axis=0).astype(BF16)
    own_v = jnp.concatenate([summed[PROP:] * factor, zero_tail], axis=0)
    kvg[me] = jnp.concatenate([summed[0:PROP] * factor, summed[PROP:] * factor], axis=0).astype(BF16)
    par_pad[...] = jnp.full((8, BLOCK), -1, jnp.int32)
    par_pad[0:SEQS, 0:PROP] = par_ref[...]
    parent_row = par_pad[pl.ds(z, 1), :]
    row_index = lax.broadcasted_iota(jnp.int32, (BLOCK, BLOCK), 0)
    lane_index = lax.broadcasted_iota(jnp.int32, (BLOCK, BLOCK), 1)
    reach = ((parent_row == row_index) & (lane_index < PROP)) | (row_index == lane_index)
    reach = jnp.where(reach, 1.0, 0.0).astype(BF16)
    for _ in range(5):
        reach = jnp.minimum(_dot(reach, reach), 1.0).astype(BF16)
    spread = (lax.rem(lane_index, PROP) == row_index) & (lane_index < 4 * PROP) & (row_index < PROP)
    lineage = _dot(reach, jnp.where(spread, 1.0, 0.0).astype(BF16))[0:PAD]
    linked = (lineage > 0.5) & (lax.broadcasted_iota(jnp.int32, (PAD, BLOCK), 0) < PROP)
    own_expanded = _expanded(qg[me].astype(F32))
    self_scores = _dot_nt(own_k, own_expanded) * SCALE2
    self_scores = jnp.where(linked, self_scores, LOW)
    self_max = jnp.max(self_scores, axis=0, keepdims=True)
    self_weight = jnp.where(linked, jnp.exp2(self_scores - self_max), 0.0)
    self_total = jnp.sum(self_weight, axis=0, keepdims=True)
    values_t = jnp.transpose(own_v).astype(BF16)
    self_out = _dot(values_t, self_weight.astype(BF16))
    self_sum = jnp.where(second_head, self_out[HEAD:], self_out[:HEAD])

    arrived(rds.at[1:], sems.at[DS_RECV])
    maxima = jnp.concatenate([ds[me, 0:1]] + [rds[step, 0:1] for step in range(1, KV)], axis=0)
    totals = jnp.concatenate([ds[me, 1:2]] + [rds[step, 1:2] for step in range(1, KV)], axis=0)
    top = jnp.maximum(jnp.max(maxima, axis=0, keepdims=True), self_max)
    self_factor = jnp.exp2(self_max - top)
    factors = jnp.exp2(maxima - top)
    denominator = self_total * self_factor + jnp.sum(totals * factors, axis=0, keepdims=True)
    used = lax.broadcasted_iota(jnp.int32, (KV, BLOCK), 1) < 96
    factors = [jnp.where(used, factors, pltpu.roll(factors, 96 - 32 * third, 1)) for third in range(3)]
    arrived(rdv.at[1:], sems.at[DV_RECV])
    merged = [dv[me, 16 * third : 16 * third + 16].astype(F32) * factors[third][0:1] for third in range(3)]
    for step in range(1, KV):
        for third in range(3):
            block = rdv[step, 16 * third : 16 * third + 16].astype(F32)
            merged[third] = merged[third] + block * factors[third][step : step + 1]
    merged = _unpacked(jnp.concatenate(merged, axis=0)) + self_sum * self_factor
    attended = merged / denominator
    lane_row = lax.broadcasted_iota(jnp.int32, (1, BLOCK), 1)
    lam = jnp.where(lane_row < PROP, lam_ref[x * 2], lam_ref[x * 2 + 1])
    difference = attended - lam * pltpu.roll(attended, BLOCK - 2 * PROP, 1)
    power = jnp.mean(difference * difference, axis=0, keepdims=True)
    normed = difference * lax.rsqrt(power + EPS)
    stacked = jnp.concatenate([normed, pltpu.roll(normed, BLOCK - PROP, 1)], axis=0)
    turned = jnp.transpose(stacked)[0:PROP]
    turned = turned * og_ref[pl.ds(x, 1), :]
    ng[me] = turned.astype(BF16)
    for step in PARTNERS:
        ng_copy(step).start()
    for step in PARTNERS:
        kvg_copy(step).start()

    loads[7].wait()
    for z_step in Z_OUT:
        arrived(ng.at[pl.ds((z ^ z_step) * 4, 4 if z_step else 3)], sems.at[NG_RECV + z_step])
        b = z ^ z_step
        rows = jnp.concatenate([ng[b * 4 + block] for block in range(4)], axis=1)
        part[b] = _dot(rows, wo[...]).astype(BF16)
        for step in TP_ORDER:
            mx_copy(z_step, step).start()

    arrived(kvg.at[1:], sems.at[KVG_RECV])
    for b in range(SEQS):
        begin = len_ref[b] + acc_ref[b] - me * POS
        position = lax.broadcasted_iota(jnp.int32, (POS, BLOCK), 0) - begin
        written = (position >= 0) & (position < PROP)
        slot = lax.broadcasted_iota(jnp.int32, (POS, BLOCK), 1)
        for which, buf in enumerate((kbuf, vbuf)):
            offset = which * PROP
            placing = jnp.where(written & (position + offset == slot), 1.0, 0.0).astype(BF16)[:, 0 : 2 * PROP]
            for block in range(4):
                lanes = slice(block * BLOCK, (block + 1) * BLOCK)
                moved = _dot(placing, kvg[b * 4 + block])
                buf[b, :, lanes] = jnp.where(written, moved, buf[b, :, lanes].astype(F32)).astype(BF16)
            out_copy(which, b).start()

    for z_step in Z_OUT:
        arrived(rpart.at[z_step, 1:], sems.at[MX_RECV + z_step])
        b = z ^ z_step
        mixed = part[b].astype(F32)
        for step in range(1, TP):
            mixed = mixed + rpart[z_step, step].astype(F32)
        mixed_ref[b] = mixed.astype(BF16)

    arrived(kbuf, out_sem.at[0])
    arrived(vbuf, out_sem.at[1])
    for ref, index in (
        (pq, Q_SEND),
        (pkv, KV_SEND),
        (qg, QG_SEND),
        (kvg, KVG_SEND),
        (dv, DV_SEND),
        (ds, DS_SEND),
        (ng, NG_SEND),
    ):
        arrived(ref.at[1:], sems.at[index])
    arrived(rpart.at[:, 1:], sems.at[MX_SEND])


def _main(*arrays):
    hbm = pl.BlockSpec(memory_space=pltpu.HBM)
    vmem = pl.BlockSpec(memory_space=pltpu.VMEM)
    dma = pltpu.SemaphoreType.DMA
    return pl.pallas_call(
        _main_kernel,
        out_shape=(
            jax.ShapeDtypeStruct((SEQS, PROP, 256), BF16),
            jax.ShapeDtypeStruct((SEQS, POS, 512), BF16),
            jax.ShapeDtypeStruct((SEQS, POS, 512), BF16),
        ),
        in_specs=[hbm] * 13,
        out_specs=(vmem, pl.BlockSpec(memory_space=pl.ANY), pl.BlockSpec(memory_space=pl.ANY)),
        scratch_shapes=[
            pltpu.VMEM((SEQS, POS, 512), BF16),
            pltpu.VMEM((SEQS, POS, 512), BF16),
            pltpu.VMEM((ROWS, 256), BF16),
            pltpu.VMEM((1, 256), F32),
            pltpu.VMEM((4, BLOCK), F32),
            pltpu.VMEM((SEQS, PROP), jnp.int32),
            pltpu.SMEM((TP,), F32),
            pltpu.SMEM((SEQS,), jnp.int32),
            pltpu.SMEM((SEQS,), jnp.int32),
            pltpu.VMEM((3, 256, 512), BF16),
            pltpu.VMEM((512, 256), BF16),
            pltpu.VMEM((SEQS, 512, POS), BF16),
            pltpu.VMEM((KV, PAD, BLOCK), BF16),
            pltpu.VMEM((KV, PAD, BLOCK), BF16),
            pltpu.VMEM((KV, 2 * PROP, BLOCK), BF16),
            pltpu.VMEM((KV, 2 * PROP, BLOCK), BF16),
            pltpu.VMEM((KV, PROP, BLOCK), BF16),
            pltpu.VMEM((KV, 2 * PROP, BLOCK), BF16),
            pltpu.VMEM((KV, 48, BLOCK), BF16),
            pltpu.VMEM((KV, 48, BLOCK), BF16),
            pltpu.VMEM((KV, 2, BLOCK), F32),
            pltpu.VMEM((KV, 2, BLOCK), F32),
            pltpu.VMEM((KV, PROP, BLOCK), BF16),
            pltpu.VMEM((SEQS, PROP, 256), BF16),
            pltpu.VMEM((SEQS, TP, PROP, 256), BF16),
            pltpu.VMEM((8, BLOCK), jnp.int32),
            pltpu.VMEM((SEQS, 2, 2 * BLOCK, 2 * BLOCK), BF16),
            dma((13,)),
            dma((SEMAPHORES,)),
            dma((2,)),
        ],
        compiler_params=pltpu.CompilerParams(
            collective_id=0, has_side_effects=True, vmem_limit_bytes=MAIN_VMEM
        ),
        name="attention",
    )(*(pltpu.with_memory_space_constraint(array, pltpu.HBM) for array in arrays))


def _write_kernel(mixed_ref, keys_ref, values_ref, mixed_hbm, keys_hbm, values_hbm, sem):
    copies = [
        pltpu.make_async_copy(keys_ref, keys_hbm, sem.at[0]),
        pltpu.make_async_copy(values_ref, values_hbm, sem.at[1]),
        pltpu.make_async_copy(mixed_ref, mixed_hbm, sem.at[2]),
    ]
    for copy in copies:
        copy.start()
    for copy in copies:
        copy.wait()


def _write(*arrays):
    hbm = pl.BlockSpec(memory_space=pltpu.HBM)
    return pl.pallas_call(
        _write_kernel,
        out_shape=tuple(jax.ShapeDtypeStruct(array.shape, array.dtype) for array in arrays),
        in_specs=[pl.BlockSpec(memory_space=pl.ANY)] * 3,
        out_specs=(hbm,) * 3,
        scratch_shapes=[pltpu.SemaphoreType.DMA((3,))],
        compiler_params=pltpu.CompilerParams(vmem_limit_bytes=WRITE_VMEM),
        name="write",
    )(*arrays)


def _local(
    tokens,
    norm_gain,
    w_query,
    w_key,
    w_value,
    w_output,
    cache_keys,
    cache_values,
    map_lambda,
    out_gain,
    parents,
    lengths,
    accepted,
):
    mixed, keys, values = _main(
        tokens,
        norm_gain.reshape(1, 256),
        w_query,
        w_key,
        w_value,
        w_output,
        cache_keys,
        cache_values,
        map_lambda,
        out_gain.reshape(4, BLOCK),
        parents,
        lengths,
        accepted,
    )
    mixed, new_keys, new_values = _write(mixed, keys, values)
    return mixed.reshape(ROWS, 256), new_keys, new_values


def solution(mesh):
    return jax.shard_map(
        _local,
        mesh=mesh,
        in_specs=(
            P(None, "kv"),
            P("kv"),
            P("kv", "tp"),
            P("kv", "tp"),
            P("kv", "tp"),
            P("tp", "kv"),
            P(None, "kv", "tp"),
            P(None, "kv", "tp"),
            P("tp"),
            P("tp"),
            P(),
            P(),
            P(),
        ),
        out_specs=(P(None, "kv"), P(None, "kv", "tp"), P(None, "kv", "tp")),
        check_vma=False,
    )
```

```python
import functools

import jax
import jax.numpy as jnp
from jax import lax
from jax.experimental import pallas as pl
from jax.experimental.pallas import tpu as pltpu
from jax.sharding import PartitionSpec as P

D = 4096
HEAD = 64
QK = 32
SEQS = 4
PROP = 24
KV = 16
TP = 8
BLOCK = 128
PAD = 32
POS = 512
ROWS = 96
EPS = 1e-05
LOW = -1e30
LOG2E = 1.4426950408889634
WRITE_VMEM = 16 * 1024 * 1024
MAIN_VMEM = 40 * 1024 * 1024
SCALE2 = QK ** (-0.5) * LOG2E
F32 = jnp.float32
BF16 = jnp.bfloat16
NT = (((1,), (1,)), ((), ()))


def _distance(step):
    ring = (0, 1, 2, 1)
    return ring[step >> 2] + ring[step & 3]


LOADS = 13
Q_SEND = 0
KV_SEND = 1
QG_SEND = 2
KVG_SEND = 4
DV_SEND = 6
DS_SEND = 7
NG_SEND = 8
MX_SEND = 9
GIVE_SEND = 10
Q_RECV = 13
KV_RECV = 15
DV_RECV = 17
DS_RECV = 19
QG_RECV = 21
KVG_RECV = 25
NG_RECV = 26
MX_RECV = 30
GIVE_RECV = 34
SEMAPHORES = 37
OUT = Q_RECV
Z_ORDER = (0, 1, 2, 3)
Z_OUT = (0, 1, 3, 2)
Z_SEND = (0, 2, 1, 3)
Z_GROUPS = ((0,), (1,), (2, 3))
Y_STEPS = (2, 1, 3)
PARTNERS = sorted(range(1, KV), key=lambda step: -_distance(step))


def _dot(a, b):
    return jnp.dot(a, b, preferred_element_type=F32)


def _dot_nt(a, b):
    return lax.dot_general(a, b, NT, preferred_element_type=F32)


def _split_rows(row):
    high = row.astype(BF16).astype(F32)
    middle = (row - high).astype(BF16).astype(F32)
    low = row - high - middle
    index = lax.broadcasted_iota(jnp.int32, (PAD - PROP, BLOCK), 0)
    return jnp.where(index == 0, high, jnp.where(index == 1, middle, jnp.where(index == 2, low, 0.0)))


def _packed(block):
    rest = block[48:]
    moved = jnp.concatenate([pltpu.roll(rest, 96 - 32 * part, 1) for part in range(3)], axis=0)
    return jnp.where(lax.broadcasted_iota(jnp.int32, (48, BLOCK), 1) < 96, block[:48], moved)


def _unpacked(packed):
    lane = lax.broadcasted_iota(jnp.int32, (16, BLOCK), 1)
    parts = [pltpu.roll(packed[16 * part : 16 * part + 16], 32 * part + 32, 1) for part in range(3)]
    rest = jnp.where(lane < 32, parts[0], jnp.where(lane < 64, parts[1], parts[2]))
    return jnp.concatenate([packed, rest], axis=0)


def _expanded(chunk):
    lane = lax.broadcasted_iota(jnp.int32, (PROP, BLOCK), 1)
    parts = []
    for which in range(2):
        for head in range(2):
            low = head * HEAD + which * QK
            inside = (lane >= low) & (lane < low + QK)
            parts.append(jnp.where(inside, chunk, 0.0))
    parts.append(jnp.zeros((BLOCK - 4 * PROP, BLOCK), F32))
    return jnp.concatenate(parts, axis=0).astype(BF16)


def _main_kernel(
    tok_hbm,
    gain_hbm,
    wq_hbm,
    wk_hbm,
    wv_hbm,
    wo_hbm,
    ck_hbm,
    cv_hbm,
    lam_hbm,
    og_hbm,
    par_hbm,
    len_hbm,
    acc_hbm,
    mixed_ref,
    keys_out,
    values_out,
    kbuf,
    vbuf,
    tok,
    gain_ref,
    og,
    par_ref,
    lam,
    len_ref,
    acc_ref,
    wqkv,
    wo,
    vt,
    pq,
    rq,
    pkv,
    rkv,
    oq,
    okv,
    qg,
    kvg,
    dv,
    rdv,
    ds,
    rds,
    ng,
    rpart,
    par_pad,
    qe,
    sc,
    sm,
    sems,
    ready,
    self_stats,
    self_sum,
):
    me = lax.axis_index("kv")
    tp = lax.axis_index("tp")
    z = me // 4
    x = lax.rem(me, 4)
    core = lax.rem(tp, 2)
    first = tp - core
    is_owner = core == 1
    is_other = core == 0

    def spot(kv_step, y_step, to):
        return {"kv": me ^ kv_step, "tp": (first ^ (2 * y_step)) + to}

    barrier = pltpu.get_barrier_semaphore()

    def greet(kv_step, y_step, to):
        pl.semaphore_signal(
            barrier, inc=1, device_id=spot(kv_step, y_step, to), device_id_type=pl.DeviceIdType.MESH
        )

    @pl.when(is_owner)
    def _():
        for step in PARTNERS:
            greet(step, 0, 1)
        for step in PARTNERS + [0]:
            greet(step, 0, 0)
        for step in Y_STEPS:
            greet(0, step, 1)
            greet(0, step, 0)


    loads = [
        (tok_hbm, tok),
        (gain_hbm, gain_ref),
        (wq_hbm, wqkv.at[0]),
        (wk_hbm, wqkv.at[1]),
        (wv_hbm, wqkv.at[2]),
        (cv_hbm, vbuf),
        (ck_hbm, kbuf),
        (wo_hbm, wo.at[core]),
        (og_hbm, og.at[core]),
        (lam_hbm, lam.at[core]),
        (par_hbm, par_ref),
        (len_hbm, len_ref),
        (acc_hbm, acc_ref),
    ]
    loads = [pltpu.make_async_copy(src, dst, sems.at[index]) for index, (src, dst) in enumerate(loads)]
    for copy in loads:
        copy.start()

    def arrived(ref, index):
        pltpu.make_async_copy(ref, ref, sems.at[index]).wait()

    def remote(src, dst, send, recv, where):
        return pltpu.make_async_remote_copy(
            src_ref=src,
            dst_ref=dst,
            send_sem=sems.at[send],
            recv_sem=sems.at[recv],
            device_id=where,
            device_id_type=pl.DeviceIdType.MESH,
        )

    def send_q(step):
        remote(pq.at[me ^ step], rq.at[core, step], Q_SEND, Q_RECV + core, spot(step, 0, 1)).start()

    def send_kv(step):
        remote(pkv.at[me ^ step], rkv.at[core, step], KV_SEND, KV_RECV + core, spot(step, 0, 1)).start()

    def send_d(step):
        remote(ds.at[me ^ step], rds.at[core, step], DS_SEND, DS_RECV + core, spot(step, 0, 1)).start()
        remote(dv.at[me ^ step], rdv.at[core, step], DV_SEND, DV_RECV + core, spot(step, 0, 1)).start()

    def send_qg(step, to):
        src = qg.at[me] if to else oq
        remote(src, qg.at[me], QG_SEND + to, QG_RECV + (step >> 2), spot(step, 0, to)).start()

    def send_kvg(step, to):
        src = kvg.at[me] if to else okv
        remote(src, kvg.at[me], KVG_SEND + to, KVG_RECV, spot(step, 0, to)).start()

    def send_ng(step):
        remote(ng.at[me], ng.at[me], NG_SEND, NG_RECV + (step >> 2), spot(step, 0, 1)).start()

    def send_mx(z_step, y_step, to):
        src = rpart.at[z_step, 0]
        dst = rpart.at[z_step, y_step]
        remote(src, dst, MX_SEND, MX_RECV + z_step, spot(0, y_step, to)).start()

    def out_copy(which, b):
        buf, out = ((kbuf, keys_out), (vbuf, values_out))[which]
        return pltpu.make_async_copy(buf.at[b], out.at[b], sems.at[OUT + which])

    loads[0].wait()
    loads[1].wait()
    wide = tok[...].astype(F32)
    gained = (wide * gain_ref[...]).astype(BF16)
    square = jnp.sum(wide * wide, axis=1, keepdims=True)
    eye = lax.broadcasted_iota(jnp.int32, (PROP, BLOCK), 0) == lax.broadcasted_iota(jnp.int32, (PROP, BLOCK), 1)
    loads[2].wait()
    partial_q = _dot(gained, wqkv[0])
    for b in range(SEQS):
        column = square[b * PROP : (b + 1) * PROP]
        row = jnp.sum(jnp.where(eye, column, 0.0), axis=0, keepdims=True)
        tail = _split_rows(row)
        for block in range(4):
            chunk = partial_q[b * PROP : (b + 1) * PROP, block * BLOCK : (block + 1) * BLOCK]
            pq[b * 4 + block] = jnp.concatenate([chunk, tail], axis=0).astype(BF16)

    @pl.when(is_owner)
    def _():
        pl.semaphore_wait(barrier, KV - 1 + 3)

    @pl.when(is_other)
    def _():
        pl.semaphore_wait(barrier, KV + 3)

    for step in PARTNERS:
        send_q(step)

    @pl.when(is_other)
    def _():
        send_q(0)

        def tell(kv_step, y_step):
            pl.semaphore_signal(
                ready, inc=1, device_id=spot(kv_step, y_step, 1), device_id_type=pl.DeviceIdType.MESH
            )

        for step in PARTNERS + [0]:
            tell(step, 0)
        for step in Y_STEPS:
            tell(0, step)

    projected = []
    for which in range(2):
        loads[3 + which].wait()
        projected.append(_dot(gained, wqkv[1 + which]))
    for b in range(SEQS):
        for block in range(4):
            pkv[b * 4 + block] = jnp.concatenate(
                [
                    part_kv[b * PROP : (b + 1) * PROP, block * BLOCK : (block + 1) * BLOCK]
                    for part_kv in projected
                ],
                axis=0,
            ).astype(BF16)
    loads[5].wait()

    def transpose_values(b):
        for block in range(4):
            vt[b, block * BLOCK : (block + 1) * BLOCK, :] = jnp.transpose(
                vbuf[b, :, block * BLOCK : (block + 1) * BLOCK]
            )

    for order in range(SEQS):
        for half in range(2):
            for side in range(2):
                qe[order, half, side * BLOCK : (side + 1) * BLOCK, (1 - side) * BLOCK : (2 - side) * BLOCK] = (
                    jnp.zeros((BLOCK, BLOCK), BF16)
                )
    for b in range(SEQS):
        transpose_values(b)
    for step in PARTNERS:
        send_kv(step)

    @pl.when(is_other)
    def _():
        send_kv(0)

    for index in (6, 7, 8, 9, 10, 11, 12):
        loads[index].wait()

    zero_tail = jnp.zeros((PAD - PROP, BLOCK), F32)
    lane = lax.broadcasted_iota(jnp.int32, (HEAD, BLOCK), 1)
    second_head = ((lane >= PROP) & (lane < 2 * PROP)) | (lane >= 3 * PROP)

    @pl.when(is_owner)
    def _():
        arrived(rq.at[1, 1:], Q_RECV + 1)
        arrived(rq.at[0], Q_RECV)
        factors = []
        for group in range(2):
            total = (pq[me] if group else rq[0, 0]).astype(F32)
            for step in range(1, KV):
                total = total + rq[group, step].astype(F32)
            square_row = jnp.sum(total[PROP:PAD], axis=0, keepdims=True)
            square_column = jnp.sum(jnp.where(eye, square_row, 0.0), axis=1, keepdims=True)
            factors.append(lax.rsqrt(square_column / D + EPS))
            own_q = (total[0:PROP] * factors[group]).astype(BF16)
            if group:
                qg[me] = own_q
            else:
                oq[...] = own_q
        pl.semaphore_wait(ready, KV + 3)
        for z_step in Z_SEND:
            for step in PARTNERS + [0]:
                if step >> 2 == z_step:
                    send_qg(step, 0)
                    if step:
                        send_qg(step, 1)
        arrived(rkv.at[1, 1:], KV_RECV + 1)
        arrived(rkv.at[0], KV_RECV)
        for group in range(2):
            summed = (pkv[me] if group else rkv[0, 0]).astype(F32)
            for step in range(1, KV):
                summed = summed + rkv[group, step].astype(F32)
            rows = [summed[0:PROP] * factors[group], summed[PROP:] * factors[group]]
            rows = jnp.concatenate(rows, axis=0).astype(BF16)
            if group:
                kvg[me] = rows
            else:
                okv[...] = rows
        for step in PARTNERS + [0]:
            send_kvg(step, 0)
        for step in PARTNERS:
            send_kvg(step, 1)
        par_pad[...] = jnp.full((8, BLOCK), -1, jnp.int32)
        par_pad[0:SEQS, 0:PROP] = par_ref[...]
        parent_row = par_pad[pl.ds(z, 1), :]
        row_index = lax.broadcasted_iota(jnp.int32, (BLOCK, BLOCK), 0)
        lane_index = lax.broadcasted_iota(jnp.int32, (BLOCK, BLOCK), 1)
        reach = ((parent_row == row_index) & (lane_index < PROP)) | (row_index == lane_index)
        reach = jnp.where(reach, 1.0, 0.0).astype(BF16)
        for _ in range(5):
            reach = jnp.minimum(_dot(reach, reach), 1.0).astype(BF16)
        spread = (lax.rem(lane_index, PROP) == row_index) & (lane_index < 4 * PROP) & (row_index < PROP)
        lineage = _dot(reach, jnp.where(spread, 1.0, 0.0).astype(BF16))[0:PAD]
        linked = (lineage > 0.5) & (lax.broadcasted_iota(jnp.int32, (PAD, BLOCK), 0) < PROP)
        for group in range(2):
            own_expanded = _expanded((qg[me] if group else oq[...]).astype(F32))
            own_kv = (kvg[me] if group else okv[...]).astype(F32)
            own_k = jnp.concatenate([own_kv[0:PROP], zero_tail], axis=0).astype(BF16)
            own_v = jnp.concatenate([own_kv[PROP:], zero_tail], axis=0)
            self_scores = _dot_nt(own_k, own_expanded) * SCALE2
            self_scores = jnp.where(linked, self_scores, LOW)
            largest = jnp.max(self_scores, axis=0, keepdims=True)
            self_weight = jnp.where(linked, jnp.exp2(self_scores - largest), 0.0)
            self_stats[group, 0:1] = largest
            self_stats[group, 1:2] = jnp.sum(self_weight, axis=0, keepdims=True)
            self_out = _dot(jnp.transpose(own_v).astype(BF16), self_weight.astype(BF16))
            self_sum[group] = jnp.where(second_head, self_out[HEAD:], self_out[:HEAD])

    @pl.when(is_other)
    def _():
        remote(wo.at[0], wo.at[0], GIVE_SEND, GIVE_RECV, spot(0, 0, 1)).start()
        remote(og.at[0], og.at[0], GIVE_SEND + 1, GIVE_RECV + 1, spot(0, 0, 1)).start()
        remote(lam.at[0], lam.at[0], GIVE_SEND + 2, GIVE_RECV + 2, spot(0, 0, 1)).start()


    def gathered(z_step):
        if z_step:
            arrived(qg.at[pl.ds((z ^ z_step) * 4, 4)], QG_RECV + z_step)
            return

        @pl.when(is_owner)
        def _():
            arrived(qg.at[0:3], QG_RECV)

        @pl.when(is_other)
        def _():
            arrived(qg.at[0:4], QG_RECV)

    def expand(order):
        b = z ^ Z_ORDER[order]
        for half in range(2):
            for side in range(2):
                chunk = qg[b * 4 + half * 2 + side].astype(F32)
                lanes = slice(side * BLOCK, (side + 1) * BLOCK)
                qe[order, half, lanes, lanes] = _expanded(chunk)

    def score(order):
        b = z ^ Z_ORDER[order]
        begin = len_ref[b] + acc_ref[b] - me * POS
        visible = lax.broadcasted_iota(jnp.int32, (POS, BLOCK), 0) < begin
        visible = jnp.concatenate([visible, visible], axis=1)
        for half in range(2):
            keys = kbuf[b, :, half * 2 * BLOCK : (half + 1) * 2 * BLOCK]
            scores = jnp.where(visible, _dot_nt(keys, qe[order, half]) * SCALE2, LOW)
            sc[order % 2, half] = scores
            sm[order % 2, half] = jnp.max(scores, axis=0, keepdims=True)

    def weigh(order):
        b = z ^ Z_ORDER[order]
        for half in range(2):
            largest = sm[order % 2, half]
            weight = jnp.exp2(sc[order % 2, half] - largest)
            weight_sum = jnp.sum(weight, axis=0, keepdims=True)
            weight = weight.astype(BF16)
            for side in range(2):
                block = half * 2 + side
                lanes = slice(side * BLOCK, (side + 1) * BLOCK)
                out = _dot(vt[b, block * BLOCK : (block + 1) * BLOCK, :], weight[:, lanes])
                owner = b * 4 + block
                dv[owner] = _packed(jnp.where(second_head, out[HEAD:], out[:HEAD])).astype(BF16)
                ds[owner] = jnp.concatenate([largest[:, lanes], weight_sum[:, lanes]], axis=0)

    def send(order):
        for x_step in (2, 1, 3, 0):
            step = Z_ORDER[order] << 2 | x_step
            if step:
                send_d(step)
        if Z_ORDER[order] == 0:

            @pl.when(is_other)
            def _():
                send_d(0)

    for group in Z_GROUPS:
        for order in group:
            gathered(Z_ORDER[order])
        for order in group:
            expand(order)
        score(group[0])
        for order in group:
            if order + 1 in group:
                score(order + 1)
            weigh(order)
            send(order)

    @pl.when(is_owner)
    def _():
        arrived(kvg.at[1:], KVG_RECV)

    @pl.when(is_other)
    def _():
        arrived(kvg, KVG_RECV)

    for b in range(SEQS):
        begin = len_ref[b] + acc_ref[b] - me * POS
        position = lax.broadcasted_iota(jnp.int32, (POS, BLOCK), 0) - begin
        written = (position >= 0) & (position < PROP)
        slot = lax.broadcasted_iota(jnp.int32, (POS, BLOCK), 1)
        for which, buf in enumerate((kbuf, vbuf)):
            offset = which * PROP
            placing = jnp.where(written & (position + offset == slot), 1.0, 0.0).astype(BF16)[:, 0 : 2 * PROP]
            for block in range(4):
                lanes = slice(block * BLOCK, (block + 1) * BLOCK)
                moved = _dot(placing, kvg[b * 4 + block])
                buf[b, :, lanes] = jnp.where(written, moved, buf[b, :, lanes].astype(F32)).astype(BF16)
            out_copy(which, b).start()

    @pl.when(is_owner)
    def _():
        lane_row = lax.broadcasted_iota(jnp.int32, (1, BLOCK), 1)
        arrived(og.at[0], GIVE_RECV + 1)
        arrived(lam.at[0], GIVE_RECV + 2)
        arrived(wo.at[0], GIVE_RECV)
        lam_rows = []
        for group in range(2):
            index = lax.broadcasted_iota(jnp.int32, (1, TP), 1)
            pair = [
                jnp.sum(jnp.where(index == x * 2 + head, lam[group], 0.0), axis=1, keepdims=True)
                for head in range(2)
            ]
            lam_rows.append(jnp.where(lane_row < PROP, pair[0], pair[1]))

        arrived(rds.at[1, 1:], DS_RECV + 1)
        arrived(rds.at[0], DS_RECV)
        denominator = []
        self_factor = []
        factors = []
        used = lax.broadcasted_iota(jnp.int32, (KV, BLOCK), 1) < 96
        for group in range(2):
            slots = [ds.at[me] if group else rds.at[0, 0]] + [rds.at[group, step] for step in range(1, KV)]
            maxima = jnp.concatenate([slot[0:1] for slot in slots], axis=0)
            totals = jnp.concatenate([slot[1:2] for slot in slots], axis=0)
            top = jnp.maximum(jnp.max(maxima, axis=0, keepdims=True), self_stats[group, 0:1])
            self_factor.append(jnp.exp2(self_stats[group, 0:1] - top))
            factor = jnp.exp2(maxima - top)
            denominator.append(
                self_stats[group, 1:2] * self_factor[group] + jnp.sum(totals * factor, axis=0, keepdims=True)
            )
            factors.append(
                [jnp.where(used, factor, pltpu.roll(factor, 96 - 32 * third, 1)) for third in range(3)]
            )
        arrived(rdv.at[1, 1:], DV_RECV + 1)
        arrived(rdv.at[0], DV_RECV)
        for group in range(2):
            slots = [dv.at[me] if group else rdv.at[0, 0]] + [rdv.at[group, step] for step in range(1, KV)]
            merged = []
            for third in range(3):
                rows = slice(16 * third, 16 * third + 16)
                sums = [
                    slot[rows].astype(F32) * factors[group][third][step : step + 1]
                    for step, slot in enumerate(slots)
                ]
                while len(sums) > 1:
                    sums = [a + b for a, b in zip(sums[::2], sums[1::2])]
                merged.append(sums[0])
            merged = _unpacked(jnp.concatenate(merged, axis=0)) + self_sum[group] * self_factor[group]
            attended = merged / denominator[group]
            difference = attended - lam_rows[group] * pltpu.roll(attended, BLOCK - 2 * PROP, 1)
            power = jnp.mean(difference * difference, axis=0, keepdims=True)
            normed = difference * lax.rsqrt(power + EPS)
            stacked = jnp.concatenate([normed, pltpu.roll(normed, BLOCK - PROP, 1)], axis=0)
            turned = jnp.transpose(stacked)[0:PROP]
            turned = turned * og[group, pl.ds(x, 1), :]
            ng[me, group] = turned.astype(BF16)
        for step in PARTNERS:
            send_ng(step)

        for z_step in Z_OUT:
            arrived(ng.at[pl.ds((z ^ z_step) * 4, 4 if z_step else 3)], NG_RECV + z_step)
            b = z ^ z_step
            projected = 0.0
            for group in range(2):
                rows = jnp.concatenate([ng[b * 4 + block, group] for block in range(4)], axis=1)
                projected = projected + _dot(rows, wo[group])
            rpart[z_step, 0] = projected.astype(BF16)
            for step in Y_STEPS:
                send_mx(z_step, step, 0)
            for step in Y_STEPS:
                send_mx(z_step, step, 1)
            send_mx(z_step, 0, 0)

    for z_step in Z_OUT:

        @pl.when(is_owner)
        def _(z_step=z_step):
            arrived(rpart.at[z_step, 1:], MX_RECV + z_step)

        @pl.when(is_other)
        def _(z_step=z_step):
            arrived(rpart.at[z_step], MX_RECV + z_step)

        mixed = rpart[z_step, 0].astype(F32)
        for step in range(1, 4):
            mixed = mixed + rpart[z_step, step].astype(F32)
        mixed_ref[z ^ z_step] = mixed.astype(BF16)

    arrived(kbuf, OUT)
    arrived(vbuf, OUT + 1)
    sent = ((pq, Q_SEND), (pkv, KV_SEND), (dv, DV_SEND), (ds, DS_SEND))

    @pl.when(is_owner)
    def _():
        for ref, index in sent + ((qg, QG_SEND + 1), (kvg, KVG_SEND + 1), (ng, NG_SEND)):
            arrived(ref.at[1:], index)
        arrived(qg, QG_SEND)
        arrived(kvg, KVG_SEND)
        arrived(rpart.at[0:7], MX_SEND)

    @pl.when(is_other)
    def _():
        for ref, index in sent:
            arrived(ref, index)
        arrived(wo.at[0], GIVE_SEND)
        arrived(og.at[0], GIVE_SEND + 1)
        arrived(lam.at[0], GIVE_SEND + 2)


def _main(*arrays):
    hbm = pl.BlockSpec(memory_space=pltpu.HBM)
    vmem = pl.BlockSpec(memory_space=pltpu.VMEM)
    dma = pltpu.SemaphoreType.DMA
    return pl.pallas_call(
        _main_kernel,
        out_shape=(
            jax.ShapeDtypeStruct((SEQS, PROP, 256), BF16),
            jax.ShapeDtypeStruct((SEQS, POS, 512), BF16),
            jax.ShapeDtypeStruct((SEQS, POS, 512), BF16),
        ),
        in_specs=[hbm] * 13,
        out_specs=(vmem, pl.BlockSpec(memory_space=pl.ANY), pl.BlockSpec(memory_space=pl.ANY)),
        scratch_shapes=[
            pltpu.VMEM((SEQS, POS, 512), BF16),
            pltpu.VMEM((SEQS, POS, 512), BF16),
            pltpu.VMEM((ROWS, 256), BF16),
            pltpu.VMEM((1, 256), F32),
            pltpu.VMEM((2, 4, BLOCK), F32),
            pltpu.VMEM((SEQS, PROP), jnp.int32),
            pltpu.VMEM((2, 1, TP), F32),
            pltpu.SMEM((SEQS,), jnp.int32),
            pltpu.SMEM((SEQS,), jnp.int32),
            pltpu.VMEM((3, 256, 512), BF16),
            pltpu.VMEM((2, 512, 256), BF16),
            pltpu.VMEM((SEQS, 512, POS), BF16),
            pltpu.VMEM((KV, PAD, BLOCK), BF16),
            pltpu.VMEM((2, KV, PAD, BLOCK), BF16),
            pltpu.VMEM((KV, 2 * PROP, BLOCK), BF16),
            pltpu.VMEM((2, KV, 2 * PROP, BLOCK), BF16),
            pltpu.VMEM((PROP, BLOCK), BF16),
            pltpu.VMEM((2 * PROP, BLOCK), BF16),
            pltpu.VMEM((KV, PROP, BLOCK), BF16),
            pltpu.VMEM((KV, 2 * PROP, BLOCK), BF16),
            pltpu.VMEM((KV, 48, BLOCK), BF16),
            pltpu.VMEM((2, KV, 48, BLOCK), BF16),
            pltpu.VMEM((KV, 2, BLOCK), F32),
            pltpu.VMEM((2, KV, 2, BLOCK), F32),
            pltpu.VMEM((KV, 2, PROP, BLOCK), BF16),
            pltpu.VMEM((8, 4, PROP, 256), BF16),
            pltpu.VMEM((8, BLOCK), jnp.int32),
            pltpu.VMEM((SEQS, 2, 2 * BLOCK, 2 * BLOCK), BF16),
            pltpu.VMEM((2, 2, POS, 2 * BLOCK), F32),
            pltpu.VMEM((2, 2, 1, 2 * BLOCK), F32),
            dma((SEMAPHORES,)),
            pltpu.SemaphoreType.REGULAR,
            pltpu.VMEM((2, 2, BLOCK), F32),
            pltpu.VMEM((2, HEAD, BLOCK), F32),
        ],
        compiler_params=pltpu.CompilerParams(
            collective_id=0, has_side_effects=True, vmem_limit_bytes=MAIN_VMEM
        ),
        name="attention",
    )(*(pltpu.with_memory_space_constraint(array, pltpu.HBM) for array in arrays))


def _write_kernel(mixed_ref, keys_ref, values_ref, mixed_hbm, keys_hbm, values_hbm, sem):
    copies = [
        pltpu.make_async_copy(keys_ref, keys_hbm, sem.at[0]),
        pltpu.make_async_copy(values_ref, values_hbm, sem.at[1]),
        pltpu.make_async_copy(mixed_ref, mixed_hbm, sem.at[2]),
    ]
    for copy in copies:
        copy.start()
    for copy in copies:
        copy.wait()


def _write(*arrays):
    hbm = pl.BlockSpec(memory_space=pltpu.HBM)
    return pl.pallas_call(
        _write_kernel,
        out_shape=tuple(jax.ShapeDtypeStruct(array.shape, array.dtype) for array in arrays),
        in_specs=[pl.BlockSpec(memory_space=pl.ANY)] * 3,
        out_specs=(hbm,) * 3,
        scratch_shapes=[pltpu.SemaphoreType.DMA((3,))],
        compiler_params=pltpu.CompilerParams(vmem_limit_bytes=WRITE_VMEM),
        name="write",
    )(*arrays)


def _local(
    tokens,
    norm_gain,
    w_query,
    w_key,
    w_value,
    w_output,
    cache_keys,
    cache_values,
    map_lambda,
    out_gain,
    parents,
    lengths,
    accepted,
):
    mixed, keys, values = _main(
        tokens,
        norm_gain.reshape(1, 256),
        w_query,
        w_key,
        w_value,
        w_output,
        cache_keys,
        cache_values,
        map_lambda.reshape(1, TP),
        out_gain.reshape(4, BLOCK),
        parents,
        lengths,
        accepted,
    )
    mixed, new_keys, new_values = _write(mixed, keys, values)
    return mixed.reshape(ROWS, 256), new_keys, new_values


def solution(mesh):
    return jax.shard_map(
        _local,
        mesh=mesh,
        in_specs=(
            P(None, "kv"),
            P("kv"),
            P("kv", "tp"),
            P("kv", "tp"),
            P("kv", "tp"),
            P("tp", "kv"),
            P(None, "kv", "tp"),
            P(None, "kv", "tp"),
            P("tp"),
            P("tp"),
            P(),
            P(),
            P(),
        ),
        out_specs=(P(None, "kv"), P(None, "kv", "tp"), P(None, "kv", "tp")),
        check_vma=False,
    )
```

```python
import functools

import jax
import jax.numpy as jnp
from jax import lax
from jax.experimental import pallas as pl
from jax.experimental.pallas import tpu as pltpu
from jax.sharding import PartitionSpec as P

D = 4096
HEAD = 64
QK = 32
SEQS = 4
PROP = 24
KV = 16
TP = 8
BLOCK = 128
PAD = 32
POS = 512
ROWS = 96
EPS = 1e-05
LOW = -1e30
LOG2E = 1.4426950408889634
WRITE_VMEM = 16 * 1024 * 1024
MAIN_VMEM = 40 * 1024 * 1024
SCALE2 = QK ** (-0.5) * LOG2E
F32 = jnp.float32
BF16 = jnp.bfloat16
NT = (((1,), (1,)), ((), ()))


def _distance(step):
    ring = (0, 1, 2, 1)
    return ring[step >> 2] + ring[step & 3]


LOADS = 13
Q_SEND = 0
KV_SEND = 1
QG_SEND = 2
KVG_SEND = 4
DV_SEND = 6
DS_SEND = 7
NG_SEND = 8
MX_SEND = 9
GIVE_SEND = 10
Q_RECV = 13
KV_RECV = 15
DV_RECV = 17
DS_RECV = 19
QG_RECV = 21
KVG_RECV = 25
NG_RECV = 26
MX_RECV = 30
GIVE_RECV = 34
SEMAPHORES = 37
OUT = Q_RECV
Z_ORDER = (0, 1, 2, 3)
Z_OUT = (0, 1, 3, 2)
Z_SEND = (0, 2, 1, 3)
Z_GROUPS = ((0,), (1,), (2, 3))
Y_STEPS = (2, 1, 3)
PARTNERS = sorted(range(1, KV), key=lambda step: -_distance(step))


def _dot(a, b):
    return jnp.dot(a, b, preferred_element_type=F32)


def _dot_nt(a, b):
    return lax.dot_general(a, b, NT, preferred_element_type=F32)


def _split_rows(row):
    high = row.astype(BF16).astype(F32)
    middle = (row - high).astype(BF16).astype(F32)
    low = row - high - middle
    index = lax.broadcasted_iota(jnp.int32, (PAD - PROP, BLOCK), 0)
    return jnp.where(index == 0, high, jnp.where(index == 1, middle, jnp.where(index == 2, low, 0.0)))


def _packed(block):
    rest = block[48:]
    moved = jnp.concatenate([pltpu.roll(rest, 96 - 32 * part, 1) for part in range(3)], axis=0)
    return jnp.where(lax.broadcasted_iota(jnp.int32, (48, BLOCK), 1) < 96, block[:48], moved)


def _unpacked(packed):
    lane = lax.broadcasted_iota(jnp.int32, (16, BLOCK), 1)
    parts = [pltpu.roll(packed[16 * part : 16 * part + 16], 32 * part + 32, 1) for part in range(3)]
    rest = jnp.where(lane < 32, parts[0], jnp.where(lane < 64, parts[1], parts[2]))
    return jnp.concatenate([packed, rest], axis=0)


def _expanded(chunk):
    lane = lax.broadcasted_iota(jnp.int32, (PROP, BLOCK), 1)
    parts = []
    for which in range(2):
        for head in range(2):
            low = head * HEAD + which * QK
            inside = (lane >= low) & (lane < low + QK)
            parts.append(jnp.where(inside, chunk, 0.0))
    parts.append(jnp.zeros((BLOCK - 4 * PROP, BLOCK), F32))
    return jnp.concatenate(parts, axis=0).astype(BF16)


def _main_kernel(
    tok_hbm,
    gain_hbm,
    wq_hbm,
    wk_hbm,
    wv_hbm,
    wo_hbm,
    ck_hbm,
    cv_hbm,
    lam_hbm,
    og_hbm,
    par_hbm,
    len_hbm,
    acc_hbm,
    _first_keys,
    mixed_ref,
    keys_out,
    values_out,
    kbuf,
    vbuf,
    tok,
    gain_ref,
    og,
    par_ref,
    lam,
    len_ref,
    acc_ref,
    wqkv,
    wo,
    vt,
    pq,
    rq,
    pkv,
    rkv,
    oq,
    okv,
    qg,
    kvg,
    dv,
    rdv,
    ds,
    rds,
    ng,
    rpart,
    par_pad,
    qe,
    sc,
    sm,
    sems,
    ready,
    self_stats,
    self_sum,
):
    me = lax.axis_index("kv")
    tp = lax.axis_index("tp")
    z = me // 4
    x = lax.rem(me, 4)
    core = lax.rem(tp, 2)
    first = tp - core
    is_owner = core == 1
    is_other = core == 0

    def spot(kv_step, y_step, to):
        return {"kv": me ^ kv_step, "tp": (first ^ (2 * y_step)) + to}

    barrier = pltpu.get_barrier_semaphore()

    def greet(kv_step, y_step, to):
        pl.semaphore_signal(
            barrier, inc=1, device_id=spot(kv_step, y_step, to), device_id_type=pl.DeviceIdType.MESH
        )

    @pl.when(is_owner)
    def _():
        for step in PARTNERS:
            greet(step, 0, 1)
        for step in PARTNERS + [0]:
            greet(step, 0, 0)
        for step in Y_STEPS:
            greet(0, step, 1)
            greet(0, step, 0)


    loads = [
        (tok_hbm, tok),
        (gain_hbm, gain_ref),
        (wq_hbm, wqkv.at[0]),
        (wk_hbm, wqkv.at[1]),
        (wv_hbm, wqkv.at[2]),
        (cv_hbm, vbuf),
        (ck_hbm, kbuf),
        (wo_hbm, wo.at[core]),
        (og_hbm, og.at[core]),
        (lam_hbm, lam.at[core]),
        (par_hbm, par_ref),
        (len_hbm, len_ref),
        (acc_hbm, acc_ref),
    ]
    loads = [pltpu.make_async_copy(src, dst, sems.at[index]) for index, (src, dst) in enumerate(loads)]
    for copy in loads:
        copy.start()

    def arrived(ref, index):
        pltpu.make_async_copy(ref, ref, sems.at[index]).wait()

    def remote(src, dst, send, recv, where):
        return pltpu.make_async_remote_copy(
            src_ref=src,
            dst_ref=dst,
            send_sem=sems.at[send],
            recv_sem=sems.at[recv],
            device_id=where,
            device_id_type=pl.DeviceIdType.MESH,
        )

    def send_q(step):
        remote(pq.at[me ^ step], rq.at[core, step], Q_SEND, Q_RECV + core, spot(step, 0, 1)).start()

    def send_kv(step):
        remote(pkv.at[me ^ step], rkv.at[core, step], KV_SEND, KV_RECV + core, spot(step, 0, 1)).start()

    def send_d(step):
        remote(ds.at[me ^ step], rds.at[core, step], DS_SEND, DS_RECV + core, spot(step, 0, 1)).start()
        remote(dv.at[me ^ step], rdv.at[core, step], DV_SEND, DV_RECV + core, spot(step, 0, 1)).start()

    def send_qg(step, to):
        src = qg.at[me] if to else oq
        remote(src, qg.at[me], QG_SEND + to, QG_RECV + (step >> 2), spot(step, 0, to)).start()

    def send_kvg(step, to):
        src = kvg.at[me] if to else okv
        remote(src, kvg.at[me], KVG_SEND + to, KVG_RECV, spot(step, 0, to)).start()

    def send_ng(step):
        remote(ng.at[me], ng.at[me], NG_SEND, NG_RECV + (step >> 2), spot(step, 0, 1)).start()

    def send_mx(z_step, y_step, to):
        src = rpart.at[z_step, 0]
        dst = rpart.at[z_step, y_step]
        remote(src, dst, MX_SEND, MX_RECV + z_step, spot(0, y_step, to)).start()

    def out_copy(which, b):
        buf, out = ((kbuf, keys_out), (vbuf, values_out))[which]
        return pltpu.make_async_copy(buf.at[b], out.at[b], sems.at[OUT + which])

    loads[0].wait()
    loads[1].wait()
    wide = tok[...].astype(F32)
    gained = (wide * gain_ref[...]).astype(BF16)
    square = jnp.sum(wide * wide, axis=1, keepdims=True)
    eye = lax.broadcasted_iota(jnp.int32, (PROP, BLOCK), 0) == lax.broadcasted_iota(jnp.int32, (PROP, BLOCK), 1)
    loads[2].wait()
    partial_q = _dot(gained, wqkv[0])
    for b in range(SEQS):
        column = square[b * PROP : (b + 1) * PROP]
        row = jnp.sum(jnp.where(eye, column, 0.0), axis=0, keepdims=True)
        tail = _split_rows(row)
        for block in range(4):
            chunk = partial_q[b * PROP : (b + 1) * PROP, block * BLOCK : (block + 1) * BLOCK]
            pq[b * 4 + block] = jnp.concatenate([chunk, tail], axis=0).astype(BF16)

    @pl.when(is_owner)
    def _():
        pl.semaphore_wait(barrier, KV - 1 + 3)

    @pl.when(is_other)
    def _():
        pl.semaphore_wait(barrier, KV + 3)

    for step in PARTNERS:
        send_q(step)

    @pl.when(is_other)
    def _():
        send_q(0)

        def tell(kv_step, y_step):
            pl.semaphore_signal(
                ready, inc=1, device_id=spot(kv_step, y_step, 1), device_id_type=pl.DeviceIdType.MESH
            )

        for step in PARTNERS + [0]:
            tell(step, 0)
        for step in Y_STEPS:
            tell(0, step)

    projected = []
    for which in range(2):
        loads[3 + which].wait()
        projected.append(_dot(gained, wqkv[1 + which]))
    for b in range(SEQS):
        for block in range(4):
            pkv[b * 4 + block] = jnp.concatenate(
                [
                    part_kv[b * PROP : (b + 1) * PROP, block * BLOCK : (block + 1) * BLOCK]
                    for part_kv in projected
                ],
                axis=0,
            ).astype(BF16)
    loads[5].wait()

    def transpose_values(b):
        for block in range(4):
            vt[b, block * BLOCK : (block + 1) * BLOCK, :] = jnp.transpose(
                vbuf[b, :, block * BLOCK : (block + 1) * BLOCK]
            )

    for order in range(SEQS):
        for half in range(2):
            for side in range(2):
                qe[order, half, side * BLOCK : (side + 1) * BLOCK, (1 - side) * BLOCK : (2 - side) * BLOCK] = (
                    jnp.zeros((BLOCK, BLOCK), BF16)
                )
    for b in range(SEQS):
        transpose_values(b)
    for step in PARTNERS:
        send_kv(step)

    @pl.when(is_other)
    def _():
        send_kv(0)

    for index in (6, 7, 8, 9, 10, 11, 12):
        loads[index].wait()

    zero_tail = jnp.zeros((PAD - PROP, BLOCK), F32)
    lane = lax.broadcasted_iota(jnp.int32, (HEAD, BLOCK), 1)
    second_head = ((lane >= PROP) & (lane < 2 * PROP)) | (lane >= 3 * PROP)

    @pl.when(is_owner)
    def _():
        arrived(rq.at[1, 1:], Q_RECV + 1)
        arrived(rq.at[0], Q_RECV)
        factors = []
        for group in range(2):
            total = (pq[me] if group else rq[0, 0]).astype(F32)
            for step in range(1, KV):
                total = total + rq[group, step].astype(F32)
            square_row = jnp.sum(total[PROP:PAD], axis=0, keepdims=True)
            square_column = jnp.sum(jnp.where(eye, square_row, 0.0), axis=1, keepdims=True)
            factors.append(lax.rsqrt(square_column / D + EPS))
            own_q = (total[0:PROP] * factors[group]).astype(BF16)
            if group:
                qg[me] = own_q
            else:
                oq[...] = own_q
        pl.semaphore_wait(ready, KV + 3)
        for z_step in Z_SEND:
            for step in PARTNERS + [0]:
                if step >> 2 == z_step:
                    send_qg(step, 0)
                    if step:
                        send_qg(step, 1)
        arrived(rkv.at[1, 1:], KV_RECV + 1)
        arrived(rkv.at[0], KV_RECV)
        for group in range(2):
            summed = (pkv[me] if group else rkv[0, 0]).astype(F32)
            for step in range(1, KV):
                summed = summed + rkv[group, step].astype(F32)
            rows = [summed[0:PROP] * factors[group], summed[PROP:] * factors[group]]
            rows = jnp.concatenate(rows, axis=0).astype(BF16)
            if group:
                kvg[me] = rows
            else:
                okv[...] = rows
        for step in PARTNERS + [0]:
            send_kvg(step, 0)
        for step in PARTNERS:
            send_kvg(step, 1)
        par_pad[...] = jnp.full((8, BLOCK), -1, jnp.int32)
        par_pad[0:SEQS, 0:PROP] = par_ref[...]
        parent_row = par_pad[pl.ds(z, 1), :]
        row_index = lax.broadcasted_iota(jnp.int32, (BLOCK, BLOCK), 0)
        lane_index = lax.broadcasted_iota(jnp.int32, (BLOCK, BLOCK), 1)
        reach = ((parent_row == row_index) & (lane_index < PROP)) | (row_index == lane_index)
        reach = jnp.where(reach, 1.0, 0.0).astype(BF16)
        for _ in range(5):
            reach = jnp.minimum(_dot(reach, reach), 1.0).astype(BF16)
        spread = (lax.rem(lane_index, PROP) == row_index) & (lane_index < 4 * PROP) & (row_index < PROP)
        lineage = _dot(reach, jnp.where(spread, 1.0, 0.0).astype(BF16))[0:PAD]
        linked = (lineage > 0.5) & (lax.broadcasted_iota(jnp.int32, (PAD, BLOCK), 0) < PROP)
        for group in range(2):
            own_expanded = _expanded((qg[me] if group else oq[...]).astype(F32))
            own_kv = (kvg[me] if group else okv[...]).astype(F32)
            own_k = jnp.concatenate([own_kv[0:PROP], zero_tail], axis=0).astype(BF16)
            own_v = jnp.concatenate([own_kv[PROP:], zero_tail], axis=0)
            self_scores = _dot_nt(own_k, own_expanded) * SCALE2
            self_scores = jnp.where(linked, self_scores, LOW)
            largest = jnp.max(self_scores, axis=0, keepdims=True)
            self_weight = jnp.where(linked, jnp.exp2(self_scores - largest), 0.0)
            self_stats[group, 0:1] = largest
            self_stats[group, 1:2] = jnp.sum(self_weight, axis=0, keepdims=True)
            self_out = _dot(jnp.transpose(own_v).astype(BF16), self_weight.astype(BF16))
            self_sum[group] = jnp.where(second_head, self_out[HEAD:], self_out[:HEAD])

    @pl.when(is_other)
    def _():
        remote(wo.at[0], wo.at[0], GIVE_SEND, GIVE_RECV, spot(0, 0, 1)).start()
        remote(og.at[0], og.at[0], GIVE_SEND + 1, GIVE_RECV + 1, spot(0, 0, 1)).start()
        remote(lam.at[0], lam.at[0], GIVE_SEND + 2, GIVE_RECV + 2, spot(0, 0, 1)).start()


    def gathered(z_step):
        if z_step:
            arrived(qg.at[pl.ds((z ^ z_step) * 4, 4)], QG_RECV + z_step)
            return

        @pl.when(is_owner)
        def _():
            arrived(qg.at[0:3], QG_RECV)

        @pl.when(is_other)
        def _():
            arrived(qg.at[0:4], QG_RECV)

    def expand(order):
        b = z ^ Z_ORDER[order]
        for half in range(2):
            for side in range(2):
                chunk = qg[b * 4 + half * 2 + side].astype(F32)
                lanes = slice(side * BLOCK, (side + 1) * BLOCK)
                qe[order, half, lanes, lanes] = _expanded(chunk)

    def score(order):
        b = z ^ Z_ORDER[order]
        begin = len_ref[b] + acc_ref[b] - me * POS
        visible = lax.broadcasted_iota(jnp.int32, (POS, BLOCK), 0) < begin
        visible = jnp.concatenate([visible, visible], axis=1)
        for half in range(2):
            keys = kbuf[b, :, half * 2 * BLOCK : (half + 1) * 2 * BLOCK]
            scores = jnp.where(visible, _dot_nt(keys, qe[order, half]) * SCALE2, LOW)
            sc[order % 2, half] = scores
            sm[order % 2, half] = jnp.max(scores, axis=0, keepdims=True)

    def weigh(order):
        b = z ^ Z_ORDER[order]
        for half in range(2):
            largest = sm[order % 2, half]
            weight = jnp.exp2(sc[order % 2, half] - largest)
            weight_sum = jnp.sum(weight, axis=0, keepdims=True)
            weight = weight.astype(BF16)
            for side in range(2):
                block = half * 2 + side
                lanes = slice(side * BLOCK, (side + 1) * BLOCK)
                out = _dot(vt[b, block * BLOCK : (block + 1) * BLOCK, :], weight[:, lanes])
                owner = b * 4 + block
                dv[owner] = _packed(jnp.where(second_head, out[HEAD:], out[:HEAD])).astype(BF16)
                ds[owner] = jnp.concatenate([largest[:, lanes], weight_sum[:, lanes]], axis=0)

    def send(order):
        for x_step in (2, 1, 3, 0):
            step = Z_ORDER[order] << 2 | x_step
            if step:
                send_d(step)
        if Z_ORDER[order] == 0:

            @pl.when(is_other)
            def _():
                send_d(0)

    for group in Z_GROUPS:
        for order in group:
            gathered(Z_ORDER[order])
        for order in group:
            expand(order)
        score(group[0])
        for order in group:
            if order + 1 in group:
                score(order + 1)
            weigh(order)
            send(order)

    @pl.when(is_owner)
    def _():
        arrived(kvg.at[1:], KVG_RECV)

    @pl.when(is_other)
    def _():
        arrived(kvg, KVG_RECV)

    for b in range(SEQS):
        begin = len_ref[b] + acc_ref[b] - me * POS
        position = lax.broadcasted_iota(jnp.int32, (POS, BLOCK), 0) - begin
        written = (position >= 0) & (position < PROP)
        slot = lax.broadcasted_iota(jnp.int32, (POS, BLOCK), 1)
        for which, buf in enumerate((kbuf, vbuf)):
            offset = which * PROP
            placing = jnp.where(written & (position + offset == slot), 1.0, 0.0).astype(BF16)[:, 0 : 2 * PROP]
            for block in range(4):
                lanes = slice(block * BLOCK, (block + 1) * BLOCK)
                moved = _dot(placing, kvg[b * 4 + block])
                buf[b, :, lanes] = jnp.where(written, moved, buf[b, :, lanes].astype(F32)).astype(BF16)
            out_copy(which, b).start()

    @pl.when(is_owner)
    def _():
        lane_row = lax.broadcasted_iota(jnp.int32, (1, BLOCK), 1)
        arrived(og.at[0], GIVE_RECV + 1)
        arrived(lam.at[0], GIVE_RECV + 2)
        arrived(wo.at[0], GIVE_RECV)
        lam_rows = []
        for group in range(2):
            index = lax.broadcasted_iota(jnp.int32, (1, TP), 1)
            pair = [
                jnp.sum(jnp.where(index == x * 2 + head, lam[group], 0.0), axis=1, keepdims=True)
                for head in range(2)
            ]
            lam_rows.append(jnp.where(lane_row < PROP, pair[0], pair[1]))

        arrived(rds.at[1, 1:], DS_RECV + 1)
        arrived(rds.at[0], DS_RECV)
        denominator = []
        self_factor = []
        factors = []
        used = lax.broadcasted_iota(jnp.int32, (KV, BLOCK), 1) < 96
        for group in range(2):
            slots = [ds.at[me] if group else rds.at[0, 0]] + [rds.at[group, step] for step in range(1, KV)]
            maxima = jnp.concatenate([slot[0:1] for slot in slots], axis=0)
            totals = jnp.concatenate([slot[1:2] for slot in slots], axis=0)
            top = jnp.maximum(jnp.max(maxima, axis=0, keepdims=True), self_stats[group, 0:1])
            self_factor.append(jnp.exp2(self_stats[group, 0:1] - top))
            factor = jnp.exp2(maxima - top)
            denominator.append(
                self_stats[group, 1:2] * self_factor[group] + jnp.sum(totals * factor, axis=0, keepdims=True)
            )
            factors.append(
                [jnp.where(used, factor, pltpu.roll(factor, 96 - 32 * third, 1)) for third in range(3)]
            )
        arrived(rdv.at[1, 1:], DV_RECV + 1)
        arrived(rdv.at[0], DV_RECV)
        for group in range(2):
            slots = [dv.at[me] if group else rdv.at[0, 0]] + [rdv.at[group, step] for step in range(1, KV)]
            merged = []
            for third in range(3):
                rows = slice(16 * third, 16 * third + 16)
                sums = [
                    slot[rows].astype(F32) * factors[group][third][step : step + 1]
                    for step, slot in enumerate(slots)
                ]
                while len(sums) > 1:
                    sums = [a + b for a, b in zip(sums[::2], sums[1::2])]
                merged.append(sums[0])
            merged = _unpacked(jnp.concatenate(merged, axis=0)) + self_sum[group] * self_factor[group]
            attended = merged / denominator[group]
            difference = attended - lam_rows[group] * pltpu.roll(attended, BLOCK - 2 * PROP, 1)
            power = jnp.mean(difference * difference, axis=0, keepdims=True)
            normed = difference * lax.rsqrt(power + EPS)
            stacked = jnp.concatenate([normed, pltpu.roll(normed, BLOCK - PROP, 1)], axis=0)
            turned = jnp.transpose(stacked)[0:PROP]
            turned = turned * og[group, pl.ds(x, 1), :]
            ng[me, group] = turned.astype(BF16)
        for step in PARTNERS:
            send_ng(step)

        for z_step in Z_OUT:
            arrived(ng.at[pl.ds((z ^ z_step) * 4, 4 if z_step else 3)], NG_RECV + z_step)
            b = z ^ z_step
            projected = 0.0
            for group in range(2):
                rows = jnp.concatenate([ng[b * 4 + block, group] for block in range(4)], axis=1)
                projected = projected + _dot(rows, wo[group])
            rpart[z_step, 0] = projected.astype(BF16)
            for step in Y_STEPS:
                send_mx(z_step, step, 0)
            for step in Y_STEPS:
                send_mx(z_step, step, 1)
            send_mx(z_step, 0, 0)

    for z_step in Z_OUT:

        @pl.when(is_owner)
        def _(z_step=z_step):
            arrived(rpart.at[z_step, 1:], MX_RECV + z_step)

        @pl.when(is_other)
        def _(z_step=z_step):
            arrived(rpart.at[z_step], MX_RECV + z_step)

        mixed = rpart[z_step, 0].astype(F32)
        for step in range(1, 4):
            mixed = mixed + rpart[z_step, step].astype(F32)
        mixed_ref[z ^ z_step] = mixed.astype(BF16)

    arrived(kbuf, OUT)
    arrived(vbuf, OUT + 1)
    sent = ((pq, Q_SEND), (pkv, KV_SEND), (dv, DV_SEND), (ds, DS_SEND))

    @pl.when(is_owner)
    def _():
        for ref, index in sent + ((qg, QG_SEND + 1), (kvg, KVG_SEND + 1), (ng, NG_SEND)):
            arrived(ref.at[1:], index)
        arrived(qg, QG_SEND)
        arrived(kvg, KVG_SEND)
        arrived(rpart.at[0:7], MX_SEND)

    @pl.when(is_other)
    def _():
        for ref, index in sent:
            arrived(ref, index)
        arrived(wo.at[0], GIVE_SEND)
        arrived(og.at[0], GIVE_SEND + 1)
        arrived(lam.at[0], GIVE_SEND + 2)


def _main(*arrays):
    hbm = pl.BlockSpec(memory_space=pltpu.HBM)
    vmem = pl.BlockSpec(memory_space=pltpu.VMEM)
    dma = pltpu.SemaphoreType.DMA
    return pl.pallas_call(
        _main_kernel,
        out_shape=(
            jax.ShapeDtypeStruct((SEQS, PROP, 256), BF16),
            jax.ShapeDtypeStruct((SEQS, POS, 512), BF16),
            jax.ShapeDtypeStruct((SEQS, POS, 512), BF16),
        ),
        in_specs=[hbm] * 14,
        out_specs=(vmem, pl.BlockSpec(memory_space=pl.ANY), pl.BlockSpec(memory_space=pl.ANY)),
        scratch_shapes=[
            pltpu.VMEM((SEQS, POS, 512), BF16),
            pltpu.VMEM((SEQS, POS, 512), BF16),
            pltpu.VMEM((ROWS, 256), BF16),
            pltpu.VMEM((1, 256), F32),
            pltpu.VMEM((2, 4, BLOCK), F32),
            pltpu.VMEM((SEQS, PROP), jnp.int32),
            pltpu.VMEM((2, 1, TP), F32),
            pltpu.SMEM((SEQS,), jnp.int32),
            pltpu.SMEM((SEQS,), jnp.int32),
            pltpu.VMEM((3, 256, 512), BF16),
            pltpu.VMEM((2, 512, 256), BF16),
            pltpu.VMEM((SEQS, 512, POS), BF16),
            pltpu.VMEM((KV, PAD, BLOCK), BF16),
            pltpu.VMEM((2, KV, PAD, BLOCK), BF16),
            pltpu.VMEM((KV, 2 * PROP, BLOCK), BF16),
            pltpu.VMEM((2, KV, 2 * PROP, BLOCK), BF16),
            pltpu.VMEM((PROP, BLOCK), BF16),
            pltpu.VMEM((2 * PROP, BLOCK), BF16),
            pltpu.VMEM((KV, PROP, BLOCK), BF16),
            pltpu.VMEM((KV, 2 * PROP, BLOCK), BF16),
            pltpu.VMEM((KV, 48, BLOCK), BF16),
            pltpu.VMEM((2, KV, 48, BLOCK), BF16),
            pltpu.VMEM((KV, 2, BLOCK), F32),
            pltpu.VMEM((2, KV, 2, BLOCK), F32),
            pltpu.VMEM((KV, 2, PROP, BLOCK), BF16),
            pltpu.VMEM((8, 4, PROP, 256), BF16),
            pltpu.VMEM((8, BLOCK), jnp.int32),
            pltpu.VMEM((SEQS, 2, 2 * BLOCK, 2 * BLOCK), BF16),
            pltpu.VMEM((2, 2, POS, 2 * BLOCK), F32),
            pltpu.VMEM((2, 2, 1, 2 * BLOCK), F32),
            dma((SEMAPHORES,)),
            pltpu.SemaphoreType.REGULAR,
            pltpu.VMEM((2, 2, BLOCK), F32),
            pltpu.VMEM((2, HEAD, BLOCK), F32),
        ],
        compiler_params=pltpu.CompilerParams(
            collective_id=0, has_side_effects=True, vmem_limit_bytes=MAIN_VMEM
        ),
        name="attention",
    )(*(pltpu.with_memory_space_constraint(array, pltpu.HBM) for array in arrays))


def _copies_first():
    return (lax.axis_index("kv") < 4) & (lax.axis_index("tp") // 2 * 4 + lax.axis_index("kv") < 5)


def _copy_kernel(keys_in, values_in, keys_out, values_out, kbuf, vbuf, sem):
    @pl.when(_copies_first())
    def _():
        pairs = ((keys_in, kbuf, keys_out), (values_in, vbuf, values_out))
        fetches = [pltpu.make_async_copy(src, buf, sem.at[which]) for which, (src, buf, _) in enumerate(pairs)]
        puts = [pltpu.make_async_copy(buf, dst, sem.at[which]) for which, (_, buf, dst) in enumerate(pairs)]
        for copy in fetches:
            copy.start()
        for fetch, put in zip(fetches, puts):
            fetch.wait()
            put.start()
        for copy in puts:
            copy.wait()


def _copy(*arrays):
    hbm = pl.BlockSpec(memory_space=pltpu.HBM)
    return pl.pallas_call(
        _copy_kernel,
        out_shape=tuple(jax.ShapeDtypeStruct(array.shape, array.dtype) for array in arrays),
        in_specs=[hbm] * 2,
        out_specs=(hbm,) * 2,
        scratch_shapes=[
            pltpu.VMEM((SEQS, POS, 512), BF16),
            pltpu.VMEM((SEQS, POS, 512), BF16),
            pltpu.SemaphoreType.DMA((2,)),
        ],
        compiler_params=pltpu.CompilerParams(vmem_limit_bytes=MAIN_VMEM),
        name="copy_caches",
    )(*(pltpu.with_memory_space_constraint(array, pltpu.HBM) for array in arrays))


def _write_kernel(mixed_ref, keys_ref, values_ref, _keys, _values, mixed_hbm, keys_hbm, values_hbm, sem):
    mixed_copy = pltpu.make_async_copy(mixed_ref, mixed_hbm, sem.at[2])
    mixed_copy.start()

    @pl.when(jnp.logical_not(_copies_first()))
    def _():
        copies = [
            pltpu.make_async_copy(keys_ref, keys_hbm, sem.at[0]),
            pltpu.make_async_copy(values_ref, values_hbm, sem.at[1]),
        ]
        for copy in copies:
            copy.start()
        for copy in copies:
            copy.wait()

    mixed_copy.wait()


def _write(*arrays):
    hbm = pl.BlockSpec(memory_space=pltpu.HBM)
    anywhere = pl.BlockSpec(memory_space=pl.ANY)
    return pl.pallas_call(
        _write_kernel,
        out_shape=tuple(jax.ShapeDtypeStruct(array.shape, array.dtype) for array in arrays[:3]),
        in_specs=[anywhere] * 3 + [hbm] * 2,
        out_specs=(hbm,) * 3,
        input_output_aliases={3: 1, 4: 2},
        scratch_shapes=[pltpu.SemaphoreType.DMA((3,))],
        compiler_params=pltpu.CompilerParams(vmem_limit_bytes=WRITE_VMEM),
        name="write",
    )(*arrays)


def _local(
    tokens,
    norm_gain,
    w_query,
    w_key,
    w_value,
    w_output,
    cache_keys,
    cache_values,
    map_lambda,
    out_gain,
    parents,
    lengths,
    accepted,
):
    first_keys, first_values = _copy(cache_keys, cache_values)
    mixed, keys, values = _main(
        tokens,
        norm_gain.reshape(1, 256),
        w_query,
        w_key,
        w_value,
        w_output,
        cache_keys,
        cache_values,
        map_lambda.reshape(1, TP),
        out_gain.reshape(4, BLOCK),
        parents,
        lengths,
        accepted,
        first_keys,
    )
    mixed, new_keys, new_values = _write(mixed, keys, values, first_keys, first_values)
    return mixed.reshape(ROWS, 256), new_keys, new_values


def solution(mesh):
    return jax.shard_map(
        _local,
        mesh=mesh,
        in_specs=(
            P(None, "kv"),
            P("kv"),
            P("kv", "tp"),
            P("kv", "tp"),
            P("kv", "tp"),
            P("tp", "kv"),
            P(None, "kv", "tp"),
            P(None, "kv", "tp"),
            P("tp"),
            P("tp"),
            P(),
            P(),
            P(),
        ),
        out_specs=(P(None, "kv"), P(None, "kv", "tp"), P(None, "kv", "tp")),
        check_vma=False,
    )
```

```python
import functools

import jax
import jax.numpy as jnp
from jax import lax
from jax.experimental import pallas as pl
from jax.experimental.pallas import tpu as pltpu
from jax.sharding import PartitionSpec as P

D = 4096
HEAD = 64
QK = 32
SEQS = 4
PROP = 24
KV = 16
TP = 8
BLOCK = 128
PAD = 32
POS = 512
ROWS = 96
EPS = 1e-05
LOW = -1e30
LOG2E = 1.4426950408889634
WRITE_VMEM = 16 * 1024 * 1024
MAIN_VMEM = 40 * 1024 * 1024
SCALE2 = QK ** (-0.5) * LOG2E
F32 = jnp.float32
BF16 = jnp.bfloat16
NT = (((1,), (1,)), ((), ()))


def _distance(step):
    ring = (0, 1, 2, 1)
    return ring[step >> 2] + ring[step & 3]


LOADS = 13
Q_SEND = 0
KV_SEND = 1
QG_SEND = 2
KVG_SEND = 4
DV_SEND = 6
DS_SEND = 7
NG_SEND = 8
MX_SEND = 9
GIVE_SEND = 10
Q_RECV = 13
KV_RECV = 15
DV_RECV = 17
DS_RECV = 19
QG_RECV = 21
KVG_RECV = 25
NG_RECV = 26
MX_RECV = 30
GIVE_RECV = 34
SEMAPHORES = 37
OUT = Q_RECV
Z_ORDER = (0, 1, 2, 3)
Z_OUT = (0, 1, 3, 2)
Z_SEND = (0, 2, 1, 3)
Z_GROUPS = ((0,), (1,), (2, 3))
Y_STEPS = (2, 1, 3)
PARTNERS = sorted(range(1, KV), key=lambda step: -_distance(step))


def _dot(a, b):
    return jnp.dot(a, b, preferred_element_type=F32)


def _dot_nt(a, b):
    return lax.dot_general(a, b, NT, preferred_element_type=F32)


def _split_rows(row):
    high = row.astype(BF16).astype(F32)
    middle = (row - high).astype(BF16).astype(F32)
    low = row - high - middle
    index = lax.broadcasted_iota(jnp.int32, (PAD - PROP, BLOCK), 0)
    return jnp.where(index == 0, high, jnp.where(index == 1, middle, jnp.where(index == 2, low, 0.0)))


def _packed(block):
    rest = block[48:]
    moved = jnp.concatenate([pltpu.roll(rest, 96 - 32 * part, 1) for part in range(3)], axis=0)
    return jnp.where(lax.broadcasted_iota(jnp.int32, (48, BLOCK), 1) < 96, block[:48], moved)


def _unpacked(packed):
    lane = lax.broadcasted_iota(jnp.int32, (16, BLOCK), 1)
    parts = [pltpu.roll(packed[16 * part : 16 * part + 16], 32 * part + 32, 1) for part in range(3)]
    rest = jnp.where(lane < 32, parts[0], jnp.where(lane < 64, parts[1], parts[2]))
    return jnp.concatenate([packed, rest], axis=0)


def _expanded(chunk):
    lane = lax.broadcasted_iota(jnp.int32, (PROP, BLOCK), 1)
    parts = []
    for which in range(2):
        for head in range(2):
            low = head * HEAD + which * QK
            inside = (lane >= low) & (lane < low + QK)
            parts.append(jnp.where(inside, chunk, 0.0))
    parts.append(jnp.zeros((BLOCK - 4 * PROP, BLOCK), F32))
    return jnp.concatenate(parts, axis=0).astype(BF16)


def _main_kernel(
    tok_hbm,
    gain_hbm,
    wq_hbm,
    wk_hbm,
    wv_hbm,
    wo_hbm,
    ck_hbm,
    cv_hbm,
    lam_hbm,
    og_hbm,
    par_hbm,
    len_hbm,
    acc_hbm,
    _first_keys,
    mixed_ref,
    keys_out,
    values_out,
    kbuf,
    vbuf,
    tok,
    gain_ref,
    og,
    par_ref,
    lam,
    len_ref,
    acc_ref,
    wqkv,
    wo,
    vt,
    pq,
    rq,
    pkv,
    rkv,
    oq,
    okv,
    qg,
    kvg,
    dv,
    rdv,
    ds,
    rds,
    ng,
    rpart,
    par_pad,
    qe,
    sc,
    sm,
    sems,
    ready,
    go,
    own_factor,
    self_stats,
    self_sum,
):
    me = lax.axis_index("kv")
    tp = lax.axis_index("tp")
    z = me // 4
    x = lax.rem(me, 4)
    core = lax.rem(tp, 2)
    first = tp - core
    is_owner = core == 1
    is_other = core == 0

    def spot(kv_step, y_step, to):
        return {"kv": me ^ kv_step, "tp": (first ^ (2 * y_step)) + to}

    barrier = pltpu.get_barrier_semaphore()

    def greet(kv_step, y_step, to):
        pl.semaphore_signal(
            barrier, inc=1, device_id=spot(kv_step, y_step, to), device_id_type=pl.DeviceIdType.MESH
        )

    @pl.when(is_owner)
    def _():
        for step in PARTNERS:
            greet(step, 0, 0)
            greet(step, 0, 1)
        greet(0, 0, 0)
        for step in Y_STEPS:
            greet(0, step, 1)
            greet(0, step, 0)


    loads = [
        (tok_hbm, tok),
        (gain_hbm, gain_ref),
        (wq_hbm, wqkv.at[0]),
        (wk_hbm, wqkv.at[1]),
        (wv_hbm, wqkv.at[2]),
        (cv_hbm, vbuf),
        (ck_hbm, kbuf),
        (wo_hbm, wo.at[core]),
        (og_hbm, og.at[core]),
        (lam_hbm, lam.at[core]),
        (par_hbm, par_ref),
        (len_hbm, len_ref),
        (acc_hbm, acc_ref),
    ]
    loads = [pltpu.make_async_copy(src, dst, sems.at[index]) for index, (src, dst) in enumerate(loads)]
    for copy in loads:
        copy.start()

    def arrived(ref, index):
        pltpu.make_async_copy(ref, ref, sems.at[index]).wait()

    def remote(src, dst, send, recv, where):
        return pltpu.make_async_remote_copy(
            src_ref=src,
            dst_ref=dst,
            send_sem=sems.at[send],
            recv_sem=sems.at[recv],
            device_id=where,
            device_id_type=pl.DeviceIdType.MESH,
        )

    def send_q(step):
        remote(pq.at[me ^ step], rq.at[core, step], Q_SEND, Q_RECV + core, spot(step, 0, 1)).start()

    def send_kv(step):
        remote(pkv.at[me ^ step], rkv.at[core, step], KV_SEND, KV_RECV + core, spot(step, 0, 1)).start()

    def send_d(step):
        remote(ds.at[me ^ step], rds.at[core, step], DS_SEND, DS_RECV + core, spot(step, 0, 1)).start()
        remote(dv.at[me ^ step], rdv.at[core, step], DV_SEND, DV_RECV + core, spot(step, 0, 1)).start()

    def send_qg(step, to):
        src = qg.at[me] if to else oq
        remote(src, qg.at[me], QG_SEND + to, QG_RECV + (step >> 2), spot(step, 0, to)).start()

    def send_kvg(step, to):
        src = kvg.at[me] if to else okv
        remote(src, kvg.at[me], KVG_SEND + to, KVG_RECV, spot(step, 0, to)).start()

    def send_ng(step):
        remote(ng.at[me], ng.at[me], NG_SEND, NG_RECV + (step >> 2), spot(step, 0, 1)).start()

    def send_mx(z_step, y_step, to):
        src = rpart.at[z_step, 0]
        dst = rpart.at[z_step, y_step]
        remote(src, dst, MX_SEND, MX_RECV + z_step, spot(0, y_step, to)).start()

    def out_copy(which, b):
        buf, out = ((kbuf, keys_out), (vbuf, values_out))[which]
        return pltpu.make_async_copy(buf.at[b], out.at[b], sems.at[OUT + which])

    loads[0].wait()
    loads[1].wait()
    wide = tok[...].astype(F32)
    gained = (wide * gain_ref[...]).astype(BF16)
    square = jnp.sum(wide * wide, axis=1, keepdims=True)
    eye = lax.broadcasted_iota(jnp.int32, (PROP, BLOCK), 0) == lax.broadcasted_iota(jnp.int32, (PROP, BLOCK), 1)
    loads[2].wait()
    partial_q = _dot(gained, wqkv[0])
    for b in range(SEQS):
        column = square[b * PROP : (b + 1) * PROP]
        row = jnp.sum(jnp.where(eye, column, 0.0), axis=0, keepdims=True)
        tail = _split_rows(row)
        for block in range(4):
            chunk = partial_q[b * PROP : (b + 1) * PROP, block * BLOCK : (block + 1) * BLOCK]
            pq[b * 4 + block] = jnp.concatenate([chunk, tail], axis=0).astype(BF16)

    @pl.when(is_owner)
    def _():
        pl.semaphore_wait(barrier, KV - 1 + 3)

    @pl.when(is_other)
    def _():
        pl.semaphore_wait(barrier, KV + 3)

    for step in PARTNERS:
        send_q(step)

    @pl.when(is_other)
    def _():
        send_q(0)

        def tell(kv_step, y_step):
            pl.semaphore_signal(
                ready, inc=1, device_id=spot(kv_step, y_step, 1), device_id_type=pl.DeviceIdType.MESH
            )

        for step in PARTNERS + [0]:
            tell(step, 0)
        for step in Y_STEPS:
            tell(0, step)

    projected = []
    for which in range(2):
        loads[3 + which].wait()
        projected.append(_dot(gained, wqkv[1 + which]))
    for b in range(SEQS):
        for block in range(4):
            pkv[b * 4 + block] = jnp.concatenate(
                [
                    part_kv[b * PROP : (b + 1) * PROP, block * BLOCK : (block + 1) * BLOCK]
                    for part_kv in projected
                ],
                axis=0,
            ).astype(BF16)
    loads[5].wait()

    def transpose_values(b):
        for block in range(4):
            vt[b, block * BLOCK : (block + 1) * BLOCK, :] = jnp.transpose(
                vbuf[b, :, block * BLOCK : (block + 1) * BLOCK]
            )

    for order in range(SEQS):
        for half in range(2):
            for side in range(2):
                qe[order, half, side * BLOCK : (side + 1) * BLOCK, (1 - side) * BLOCK : (2 - side) * BLOCK] = (
                    jnp.zeros((BLOCK, BLOCK), BF16)
                )
    for b in range(SEQS):
        transpose_values(b)
    for index in (6, 7, 8, 9, 10, 11, 12):
        loads[index].wait()

    zero_tail = jnp.zeros((PAD - PROP, BLOCK), F32)
    lane = lax.broadcasted_iota(jnp.int32, (HEAD, BLOCK), 1)
    second_head = ((lane >= PROP) & (lane < 2 * PROP)) | (lane >= 3 * PROP)

    @pl.when(is_owner)
    def _():
        arrived(rq.at[1, 1:], Q_RECV + 1)
        arrived(rq.at[0], Q_RECV)
        for group in range(2):
            total = (pq[me] if group else rq[0, 0]).astype(F32)
            for step in range(1, KV):
                total = total + rq[group, step].astype(F32)
            square_row = jnp.sum(total[PROP:PAD], axis=0, keepdims=True)
            square_column = jnp.sum(jnp.where(eye, square_row, 0.0), axis=1, keepdims=True)
            factor = lax.rsqrt(square_column / D + EPS)
            own_factor[group] = jnp.broadcast_to(factor, (PROP, BLOCK))
            own_q = (total[0:PROP] * factor).astype(BF16)
            if group:
                qg[me] = own_q
            else:
                oq[...] = own_q
        pl.semaphore_wait(ready, KV + 3)
        for z_step in Z_SEND:
            for step in PARTNERS + [0]:
                if step >> 2 == z_step:
                    send_qg(step, 0)
                    if step:
                        send_qg(step, 1)
        pl.semaphore_signal(go, inc=1, device_id=spot(0, 0, 0), device_id_type=pl.DeviceIdType.MESH)
        for step in PARTNERS:
            send_kv(step)

    @pl.when(is_other)
    def _():
        pl.semaphore_wait(go, 1)
        for step in PARTNERS + [0]:
            send_kv(step)
        remote(wo.at[0], wo.at[0], GIVE_SEND, GIVE_RECV, spot(0, 0, 1)).start()
        remote(og.at[0], og.at[0], GIVE_SEND + 1, GIVE_RECV + 1, spot(0, 0, 1)).start()
        remote(lam.at[0], lam.at[0], GIVE_SEND + 2, GIVE_RECV + 2, spot(0, 0, 1)).start()


    def gathered(z_step):
        if z_step:
            arrived(qg.at[pl.ds((z ^ z_step) * 4, 4)], QG_RECV + z_step)
            return

        @pl.when(is_owner)
        def _():
            arrived(qg.at[0:3], QG_RECV)

        @pl.when(is_other)
        def _():
            arrived(qg.at[0:4], QG_RECV)

    def expand(order):
        b = z ^ Z_ORDER[order]
        for half in range(2):
            for side in range(2):
                chunk = qg[b * 4 + half * 2 + side].astype(F32)
                lanes = slice(side * BLOCK, (side + 1) * BLOCK)
                qe[order, half, lanes, lanes] = _expanded(chunk)

    def score(order):
        b = z ^ Z_ORDER[order]
        begin = len_ref[b] + acc_ref[b] - me * POS
        visible = lax.broadcasted_iota(jnp.int32, (POS, BLOCK), 0) < begin
        visible = jnp.concatenate([visible, visible], axis=1)
        for half in range(2):
            keys = kbuf[b, :, half * 2 * BLOCK : (half + 1) * 2 * BLOCK]
            scores = jnp.where(visible, _dot_nt(keys, qe[order, half]) * SCALE2, LOW)
            sc[order % 2, half] = scores
            sm[order % 2, half] = jnp.max(scores, axis=0, keepdims=True)

    def weigh(order):
        b = z ^ Z_ORDER[order]
        for half in range(2):
            largest = sm[order % 2, half]
            weight = jnp.exp2(sc[order % 2, half] - largest)
            weight_sum = jnp.sum(weight, axis=0, keepdims=True)
            weight = weight.astype(BF16)
            for side in range(2):
                block = half * 2 + side
                lanes = slice(side * BLOCK, (side + 1) * BLOCK)
                out = _dot(vt[b, block * BLOCK : (block + 1) * BLOCK, :], weight[:, lanes])
                owner = b * 4 + block
                dv[owner] = _packed(jnp.where(second_head, out[HEAD:], out[:HEAD])).astype(BF16)
                ds[owner] = jnp.concatenate([largest[:, lanes], weight_sum[:, lanes]], axis=0)

    def send(order):
        for x_step in (2, 1, 3, 0):
            step = Z_ORDER[order] << 2 | x_step
            if step:
                send_d(step)
        if Z_ORDER[order] == 0:

            @pl.when(is_other)
            def _():
                send_d(0)

    for group in Z_GROUPS:
        for order in group:
            gathered(Z_ORDER[order])
        for order in group:
            expand(order)
        score(group[0])
        for order in group:
            if order + 1 in group:
                score(order + 1)
            weigh(order)
            send(order)

    @pl.when(is_owner)
    def _():
        arrived(rkv.at[1, 1:], KV_RECV + 1)
        arrived(rkv.at[0], KV_RECV)
        for group in range(2):
            summed = (pkv[me] if group else rkv[0, 0]).astype(F32)
            for step in range(1, KV):
                summed = summed + rkv[group, step].astype(F32)
            rows = [summed[0:PROP] * own_factor[group], summed[PROP:] * own_factor[group]]
            rows = jnp.concatenate(rows, axis=0).astype(BF16)
            if group:
                kvg[me] = rows
            else:
                okv[...] = rows
        par_pad[...] = jnp.full((8, BLOCK), -1, jnp.int32)
        par_pad[0:SEQS, 0:PROP] = par_ref[...]
        parent_row = par_pad[pl.ds(z, 1), :]
        row_index = lax.broadcasted_iota(jnp.int32, (BLOCK, BLOCK), 0)
        lane_index = lax.broadcasted_iota(jnp.int32, (BLOCK, BLOCK), 1)
        reach = ((parent_row == row_index) & (lane_index < PROP)) | (row_index == lane_index)
        reach = jnp.where(reach, 1.0, 0.0).astype(BF16)
        for _ in range(5):
            reach = jnp.minimum(_dot(reach, reach), 1.0).astype(BF16)
        spread = (lax.rem(lane_index, PROP) == row_index) & (lane_index < 4 * PROP) & (row_index < PROP)
        lineage = _dot(reach, jnp.where(spread, 1.0, 0.0).astype(BF16))[0:PAD]
        linked = (lineage > 0.5) & (lax.broadcasted_iota(jnp.int32, (PAD, BLOCK), 0) < PROP)
        for group in range(2):
            own_expanded = _expanded((qg[me] if group else oq[...]).astype(F32))
            own_kv = (kvg[me] if group else okv[...]).astype(F32)
            own_k = jnp.concatenate([own_kv[0:PROP], zero_tail], axis=0).astype(BF16)
            own_v = jnp.concatenate([own_kv[PROP:], zero_tail], axis=0)
            self_scores = _dot_nt(own_k, own_expanded) * SCALE2
            self_scores = jnp.where(linked, self_scores, LOW)
            largest = jnp.max(self_scores, axis=0, keepdims=True)
            self_weight = jnp.where(linked, jnp.exp2(self_scores - largest), 0.0)
            self_stats[group, 0:1] = largest
            self_stats[group, 1:2] = jnp.sum(self_weight, axis=0, keepdims=True)
            self_out = _dot(jnp.transpose(own_v).astype(BF16), self_weight.astype(BF16))
            self_sum[group] = jnp.where(second_head, self_out[HEAD:], self_out[:HEAD])
        lane_row = lax.broadcasted_iota(jnp.int32, (1, BLOCK), 1)
        arrived(og.at[0], GIVE_RECV + 1)
        arrived(lam.at[0], GIVE_RECV + 2)
        arrived(wo.at[0], GIVE_RECV)
        lam_rows = []
        for group in range(2):
            index = lax.broadcasted_iota(jnp.int32, (1, TP), 1)
            pair = [
                jnp.sum(jnp.where(index == x * 2 + head, lam[group], 0.0), axis=1, keepdims=True)
                for head in range(2)
            ]
            lam_rows.append(jnp.where(lane_row < PROP, pair[0], pair[1]))

        arrived(rds.at[1, 1:], DS_RECV + 1)
        arrived(rds.at[0], DS_RECV)
        denominator = []
        self_factor = []
        factors = []
        used = lax.broadcasted_iota(jnp.int32, (KV, BLOCK), 1) < 96
        for group in range(2):
            slots = [ds.at[me] if group else rds.at[0, 0]] + [rds.at[group, step] for step in range(1, KV)]
            maxima = jnp.concatenate([slot[0:1] for slot in slots], axis=0)
            totals = jnp.concatenate([slot[1:2] for slot in slots], axis=0)
            top = jnp.maximum(jnp.max(maxima, axis=0, keepdims=True), self_stats[group, 0:1])
            self_factor.append(jnp.exp2(self_stats[group, 0:1] - top))
            factor = jnp.exp2(maxima - top)
            denominator.append(
                self_stats[group, 1:2] * self_factor[group] + jnp.sum(totals * factor, axis=0, keepdims=True)
            )
            factors.append(
                [jnp.where(used, factor, pltpu.roll(factor, 96 - 32 * third, 1)) for third in range(3)]
            )
        arrived(rdv.at[1, 1:], DV_RECV + 1)
        arrived(rdv.at[0], DV_RECV)
        for group in range(2):
            slots = [dv.at[me] if group else rdv.at[0, 0]] + [rdv.at[group, step] for step in range(1, KV)]
            merged = []
            for third in range(3):
                rows = slice(16 * third, 16 * third + 16)
                sums = [
                    slot[rows].astype(F32) * factors[group][third][step : step + 1]
                    for step, slot in enumerate(slots)
                ]
                while len(sums) > 1:
                    sums = [a + b for a, b in zip(sums[::2], sums[1::2])]
                merged.append(sums[0])
            merged = _unpacked(jnp.concatenate(merged, axis=0)) + self_sum[group] * self_factor[group]
            attended = merged / denominator[group]
            difference = attended - lam_rows[group] * pltpu.roll(attended, BLOCK - 2 * PROP, 1)
            power = jnp.mean(difference * difference, axis=0, keepdims=True)
            normed = difference * lax.rsqrt(power + EPS)
            stacked = jnp.concatenate([normed, pltpu.roll(normed, BLOCK - PROP, 1)], axis=0)
            turned = jnp.transpose(stacked)[0:PROP]
            turned = turned * og[group, pl.ds(x, 1), :]
            ng[me, group] = turned.astype(BF16)
        for step in PARTNERS:
            send_ng(step)
        for z_step in (2, 1, 3, 0):

            @pl.when((z ^ z_step) >= 2)
            def _(z_step=z_step):
                for step in PARTNERS + [0]:
                    if step >> 2 == z_step:
                        send_kvg(step, 0)
                        if step:
                            send_kvg(step, 1)


        for z_step in Z_OUT:
            arrived(ng.at[pl.ds((z ^ z_step) * 4, 4 if z_step else 3)], NG_RECV + z_step)
            b = z ^ z_step
            projected = 0.0
            for group in range(2):
                rows = jnp.concatenate([ng[b * 4 + block, group] for block in range(4)], axis=1)
                projected = projected + _dot(rows, wo[group])
            rpart[z_step, 0] = projected.astype(BF16)
            for step in Y_STEPS:
                send_mx(z_step, step, 1)
            for step in Y_STEPS:
                send_mx(z_step, step, 0)
            send_mx(z_step, 0, 0)

    @pl.when(is_owner & (z >= 2))
    def _():
        arrived(kvg.at[1:], KVG_RECV)

    @pl.when(is_other & (z >= 2))
    def _():
        arrived(kvg, KVG_RECV)

    @pl.when(z >= 2)
    def _():
        for b in range(SEQS):
            begin = len_ref[b] + acc_ref[b] - me * POS
            position = lax.broadcasted_iota(jnp.int32, (POS, BLOCK), 0) - begin
            written = (position >= 0) & (position < PROP)
            slot = lax.broadcasted_iota(jnp.int32, (POS, BLOCK), 1)
            for which, buf in enumerate((kbuf, vbuf)):
                offset = which * PROP
                placing = jnp.where(written & (position + offset == slot), 1.0, 0.0)
                placing = placing.astype(BF16)[:, 0 : 2 * PROP]
                for block in range(4):
                    lanes = slice(block * BLOCK, (block + 1) * BLOCK)
                    moved = _dot(placing, kvg[b * 4 + block])
                    buf[b, :, lanes] = jnp.where(written, moved, buf[b, :, lanes].astype(F32)).astype(BF16)
                out_copy(which, b).start()

    @pl.when(z < 2)
    def _():
        for b in range(SEQS):
            for which in range(2):
                out_copy(which, b).start()

    for z_step in Z_OUT:

        @pl.when(is_owner)
        def _(z_step=z_step):
            arrived(rpart.at[z_step, 1:], MX_RECV + z_step)

        @pl.when(is_other)
        def _(z_step=z_step):
            arrived(rpart.at[z_step], MX_RECV + z_step)

        mixed = rpart[z_step, 0].astype(F32)
        for step in range(1, 4):
            mixed = mixed + rpart[z_step, step].astype(F32)
        mixed_ref[z ^ z_step] = mixed.astype(BF16)

    arrived(kbuf, OUT)
    arrived(vbuf, OUT + 1)
    sent = ((pq, Q_SEND), (pkv, KV_SEND), (dv, DV_SEND), (ds, DS_SEND))

    @pl.when(is_owner)
    def _():
        for ref, index in sent + ((qg, QG_SEND + 1), (ng, NG_SEND)):
            arrived(ref.at[1:], index)
        arrived(qg, QG_SEND)
        arrived(kvg.at[0:8], KVG_SEND)
        arrived(rpart.at[0:7], MX_SEND)

    @pl.when(is_owner & (z < 2))
    def _():
        arrived(kvg.at[0:8], KVG_SEND + 1)

    @pl.when(is_owner & (z >= 2))
    def _():
        arrived(kvg.at[0:7], KVG_SEND + 1)

    @pl.when(is_other)
    def _():
        for ref, index in sent:
            arrived(ref, index)
        arrived(wo.at[0], GIVE_SEND)
        arrived(og.at[0], GIVE_SEND + 1)
        arrived(lam.at[0], GIVE_SEND + 2)


def _main(*arrays):
    hbm = pl.BlockSpec(memory_space=pltpu.HBM)
    vmem = pl.BlockSpec(memory_space=pltpu.VMEM)
    dma = pltpu.SemaphoreType.DMA
    return pl.pallas_call(
        _main_kernel,
        out_shape=(
            jax.ShapeDtypeStruct((SEQS, PROP, 256), BF16),
            jax.ShapeDtypeStruct((SEQS, POS, 512), BF16),
            jax.ShapeDtypeStruct((SEQS, POS, 512), BF16),
        ),
        in_specs=[hbm] * 14,
        out_specs=(vmem, pl.BlockSpec(memory_space=pl.ANY), pl.BlockSpec(memory_space=pl.ANY)),
        scratch_shapes=[
            pltpu.VMEM((SEQS, POS, 512), BF16),
            pltpu.VMEM((SEQS, POS, 512), BF16),
            pltpu.VMEM((ROWS, 256), BF16),
            pltpu.VMEM((1, 256), F32),
            pltpu.VMEM((2, 4, BLOCK), F32),
            pltpu.VMEM((SEQS, PROP), jnp.int32),
            pltpu.VMEM((2, 1, TP), F32),
            pltpu.SMEM((SEQS,), jnp.int32),
            pltpu.SMEM((SEQS,), jnp.int32),
            pltpu.VMEM((3, 256, 512), BF16),
            pltpu.VMEM((2, 512, 256), BF16),
            pltpu.VMEM((SEQS, 512, POS), BF16),
            pltpu.VMEM((KV, PAD, BLOCK), BF16),
            pltpu.VMEM((2, KV, PAD, BLOCK), BF16),
            pltpu.VMEM((KV, 2 * PROP, BLOCK), BF16),
            pltpu.VMEM((2, KV, 2 * PROP, BLOCK), BF16),
            pltpu.VMEM((PROP, BLOCK), BF16),
            pltpu.VMEM((2 * PROP, BLOCK), BF16),
            pltpu.VMEM((KV, PROP, BLOCK), BF16),
            pltpu.VMEM((KV, 2 * PROP, BLOCK), BF16),
            pltpu.VMEM((KV, 48, BLOCK), BF16),
            pltpu.VMEM((2, KV, 48, BLOCK), BF16),
            pltpu.VMEM((KV, 2, BLOCK), F32),
            pltpu.VMEM((2, KV, 2, BLOCK), F32),
            pltpu.VMEM((KV, 2, PROP, BLOCK), BF16),
            pltpu.VMEM((8, 4, PROP, 256), BF16),
            pltpu.VMEM((8, BLOCK), jnp.int32),
            pltpu.VMEM((SEQS, 2, 2 * BLOCK, 2 * BLOCK), BF16),
            pltpu.VMEM((2, 2, POS, 2 * BLOCK), F32),
            pltpu.VMEM((2, 2, 1, 2 * BLOCK), F32),
            dma((SEMAPHORES,)),
            pltpu.SemaphoreType.REGULAR,
            pltpu.SemaphoreType.REGULAR,
            pltpu.VMEM((2, PROP, BLOCK), F32),
            pltpu.VMEM((2, 2, BLOCK), F32),
            pltpu.VMEM((2, HEAD, BLOCK), F32),
        ],
        compiler_params=pltpu.CompilerParams(
            collective_id=0, has_side_effects=True, vmem_limit_bytes=MAIN_VMEM
        ),
        name="attention",
    )(*(pltpu.with_memory_space_constraint(array, pltpu.HBM) for array in arrays))


def _copies_first(which):
    kv = lax.axis_index("kv")
    y = lax.axis_index("tp") // 2
    return (kv < 4) & (kv + y * 4 < 6) if which else (kv + y) < 1


def _copy_kernel(keys_in, values_in, keys_out, values_out, kbuf, vbuf, sem):
    pairs = ((keys_in, kbuf, keys_out), (values_in, vbuf, values_out))
    fetches = [pltpu.make_async_copy(src, buf, sem.at[which]) for which, (src, buf, _) in enumerate(pairs)]
    puts = [pltpu.make_async_copy(buf, dst, sem.at[which]) for which, (_, buf, dst) in enumerate(pairs)]

    @pl.when(_copies_first(1))
    def _():
        fetches[1].start()

        @pl.when(_copies_first(0))
        def _():
            fetches[0].start()

        fetches[1].wait()
        puts[1].start()

        @pl.when(_copies_first(0))
        def _():
            fetches[0].wait()
            puts[0].start()
            puts[0].wait()

        puts[1].wait()


def _copy(*arrays):
    hbm = pl.BlockSpec(memory_space=pltpu.HBM)
    return pl.pallas_call(
        _copy_kernel,
        out_shape=tuple(jax.ShapeDtypeStruct(array.shape, array.dtype) for array in arrays),
        in_specs=[hbm] * 2,
        out_specs=(hbm,) * 2,
        scratch_shapes=[
            pltpu.VMEM((SEQS, POS, 512), BF16),
            pltpu.VMEM((SEQS, POS, 512), BF16),
            pltpu.SemaphoreType.DMA((2,)),
        ],
        compiler_params=pltpu.CompilerParams(vmem_limit_bytes=MAIN_VMEM),
        name="copy_caches",
    )(*(pltpu.with_memory_space_constraint(array, pltpu.HBM) for array in arrays))


def _write_kernel(mixed_ref, keys_ref, values_ref, _keys, _values, mixed_hbm, keys_hbm, values_hbm, sem):
    mixed_copy = pltpu.make_async_copy(mixed_ref, mixed_hbm, sem.at[2])
    mixed_copy.start()

    copies = [
        pltpu.make_async_copy(keys_ref, keys_hbm, sem.at[0]),
        pltpu.make_async_copy(values_ref, values_hbm, sem.at[1]),
    ]

    @pl.when(jnp.logical_not(_copies_first(0)))
    def _():
        copies[0].start()

        @pl.when(jnp.logical_not(_copies_first(1)))
        def _():
            copies[1].start()
            copies[1].wait()

        copies[0].wait()

    mixed_copy.wait()


def _write(*arrays):
    hbm = pl.BlockSpec(memory_space=pltpu.HBM)
    anywhere = pl.BlockSpec(memory_space=pl.ANY)
    return pl.pallas_call(
        _write_kernel,
        out_shape=tuple(jax.ShapeDtypeStruct(array.shape, array.dtype) for array in arrays[:3]),
        in_specs=[anywhere] * 3 + [hbm] * 2,
        out_specs=(hbm,) * 3,
        input_output_aliases={3: 1, 4: 2},
        scratch_shapes=[pltpu.SemaphoreType.DMA((3,))],
        compiler_params=pltpu.CompilerParams(vmem_limit_bytes=WRITE_VMEM),
        name="write",
    )(*arrays)


def _local(
    tokens,
    norm_gain,
    w_query,
    w_key,
    w_value,
    w_output,
    cache_keys,
    cache_values,
    map_lambda,
    out_gain,
    parents,
    lengths,
    accepted,
):
    first_keys, first_values = _copy(cache_keys, cache_values)
    mixed, keys, values = _main(
        tokens,
        norm_gain.reshape(1, 256),
        w_query,
        w_key,
        w_value,
        w_output,
        cache_keys,
        cache_values,
        map_lambda.reshape(1, TP),
        out_gain.reshape(4, BLOCK),
        parents,
        lengths,
        accepted,
        first_keys,
    )
    mixed, new_keys, new_values = _write(mixed, keys, values, first_keys, first_values)
    return mixed.reshape(ROWS, 256), new_keys, new_values


def solution(mesh):
    return jax.shard_map(
        _local,
        mesh=mesh,
        in_specs=(
            P(None, "kv"),
            P("kv"),
            P("kv", "tp"),
            P("kv", "tp"),
            P("kv", "tp"),
            P("tp", "kv"),
            P(None, "kv", "tp"),
            P(None, "kv", "tp"),
            P("tp"),
            P("tp"),
            P(),
            P(),
            P(),
        ),
        out_specs=(P(None, "kv"), P(None, "kv", "tp"), P(None, "kv", "tp")),
        check_vma=False,
    )
```

```python
import functools

import jax
import jax.numpy as jnp
from jax import lax
from jax.experimental import pallas as pl
from jax.experimental.pallas import tpu as pltpu
from jax.sharding import PartitionSpec as P

D = 4096
HEAD = 64
QK = 32
SEQS = 4
PROP = 24
KV = 16
TP = 8
BLOCK = 128
PAD = 32
POS = 512
ROWS = 96
EPS = 1e-05
LOW = -1e30
LOG2E = 1.4426950408889634
WRITE_VMEM = 16 * 1024 * 1024
MAIN_VMEM = 40 * 1024 * 1024
SCALE2 = QK ** (-0.5) * LOG2E
F32 = jnp.float32
BF16 = jnp.bfloat16
NT = (((1,), (1,)), ((), ()))


def _distance(step):
    ring = (0, 1, 2, 1)
    return ring[step >> 2] + ring[step & 3]


LOADS = 13
Q_SEND = 0
KV_SEND = 1
QG_SEND = 2
KVG_SEND = 4
DV_SEND = 6
DS_SEND = 7
NG_SEND = 8
MX_SEND = 9
GIVE_SEND = 10
Q_RECV = 13
KV_RECV = 14
DV_RECV = 15
DS_RECV = 16
QG_RECV = 17
KVG_RECV = 21
NG_RECV = 22
MX_RECV = 26
GIVE_RECV = 30
SEMAPHORES = 33
OUT = 8
Z_ORDER = (0, 1, 2, 3)
Z_OUT = (0, 1, 3, 2)
Z_SEND = (0, 1, 2, 3)
Z_GROUPS = ((0,), (1,), (2, 3))
Y_STEPS = (2, 1, 3)
PARTNERS = sorted(range(1, KV), key=lambda step: -_distance(step))


def _dot(a, b):
    return jnp.dot(a, b, preferred_element_type=F32)


def _dot_nt(a, b):
    return lax.dot_general(a, b, NT, preferred_element_type=F32)


def _split_rows(row):
    high = row.astype(BF16).astype(F32)
    middle = (row - high).astype(BF16).astype(F32)
    low = row - high - middle
    index = lax.broadcasted_iota(jnp.int32, (PAD - PROP, BLOCK), 0)
    return jnp.where(index == 0, high, jnp.where(index == 1, middle, jnp.where(index == 2, low, 0.0)))


def _packed(block):
    rest = block[48:]
    moved = jnp.concatenate([pltpu.roll(rest, 96 - 32 * part, 1) for part in range(3)], axis=0)
    return jnp.where(lax.broadcasted_iota(jnp.int32, (48, BLOCK), 1) < 96, block[:48], moved)


def _unpacked(packed):
    lane = lax.broadcasted_iota(jnp.int32, (16, BLOCK), 1)
    parts = [pltpu.roll(packed[16 * part : 16 * part + 16], 32 * part + 32, 1) for part in range(3)]
    rest = jnp.where(lane < 32, parts[0], jnp.where(lane < 64, parts[1], parts[2]))
    return jnp.concatenate([packed, rest], axis=0)


def _expanded(chunk):
    lane = lax.broadcasted_iota(jnp.int32, (PROP, BLOCK), 1)
    parts = []
    for which in range(2):
        for head in range(2):
            low = head * HEAD + which * QK
            inside = (lane >= low) & (lane < low + QK)
            parts.append(jnp.where(inside, chunk, 0.0))
    parts.append(jnp.zeros((BLOCK - 4 * PROP, BLOCK), F32))
    return jnp.concatenate(parts, axis=0).astype(BF16)


def _main_kernel(
    tok_hbm,
    gain_hbm,
    wq_hbm,
    wk_hbm,
    wv_hbm,
    wo_hbm,
    ck_hbm,
    cv_hbm,
    lam_hbm,
    og_hbm,
    par_hbm,
    len_hbm,
    acc_hbm,
    _first_keys,
    mixed_ref,
    keys_out,
    values_out,
    kbuf,
    vbuf,
    tok,
    gain_ref,
    og,
    par_ref,
    lam,
    len_ref,
    acc_ref,
    wqkv,
    wo,
    vt,
    pq,
    rq,
    pkv,
    rkv,
    oq,
    okv,
    qg,
    kvg,
    dv,
    rdv,
    ds,
    rds,
    ng,
    rpart,
    par_pad,
    qe,
    sc,
    sm,
    sems,
    ready,
    go,
    own_factor,
    self_stats,
    self_sum,
):
    me = lax.axis_index("kv")
    tp = lax.axis_index("tp")
    z = me // 4
    x = lax.rem(me, 4)
    core = lax.rem(tp, 2)
    first = tp - core
    is_owner = core == 1
    is_other = core == 0

    def spot(kv_step, y_step, to):
        return {"kv": me ^ kv_step, "tp": (first ^ (2 * y_step)) + to}

    barrier = pltpu.get_barrier_semaphore()

    def greet(kv_step, y_step, to):
        pl.semaphore_signal(
            barrier, inc=1, device_id=spot(kv_step, y_step, to), device_id_type=pl.DeviceIdType.MESH
        )

    @pl.when(is_owner)
    def _():
        for step in PARTNERS:
            greet(step, 0, 0)
            greet(step, 0, 1)
        greet(0, 0, 0)
        for step in Y_STEPS:
            greet(0, step, 1)
            greet(0, step, 0)


    loads = [
        (tok_hbm, tok),
        (gain_hbm, gain_ref),
        (wq_hbm, wqkv.at[0]),
        (wk_hbm, wqkv.at[1]),
        (wv_hbm, wqkv.at[2]),
        (cv_hbm, vbuf),
        (ck_hbm, kbuf),
        (wo_hbm, wo.at[core]),
        (og_hbm, og.at[core]),
        (lam_hbm, lam.at[core]),
        (par_hbm, par_ref),
        (len_hbm, len_ref),
        (acc_hbm, acc_ref),
    ]
    loads = [pltpu.make_async_copy(src, dst, sems.at[index]) for index, (src, dst) in enumerate(loads)]
    for copy in loads:
        copy.start()

    def arrived(ref, index):
        pltpu.make_async_copy(ref, ref, sems.at[index]).wait()

    def remote(src, dst, send, recv, where):
        return pltpu.make_async_remote_copy(
            src_ref=src,
            dst_ref=dst,
            send_sem=sems.at[send],
            recv_sem=sems.at[recv],
            device_id=where,
            device_id_type=pl.DeviceIdType.MESH,
        )

    def send_q(step):
        remote(pq.at[me ^ step], rq.at[core * KV + step], Q_SEND, Q_RECV, spot(step, 0, 1)).start()

    def send_kv(step):
        remote(pkv.at[me ^ step], rkv.at[core * KV + step], KV_SEND, KV_RECV, spot(step, 0, 1)).start()

    def send_d(step):
        remote(ds.at[me ^ step], rds.at[core * KV + step], DS_SEND, DS_RECV, spot(step, 0, 1)).start()
        remote(dv.at[me ^ step], rdv.at[core * KV + step], DV_SEND, DV_RECV, spot(step, 0, 1)).start()

    def send_qg(step, to):
        src = qg.at[me] if to else oq
        remote(src, qg.at[me], QG_SEND + to, QG_RECV + (step >> 2), spot(step, 0, to)).start()

    def send_kvg(step, to):
        src = kvg.at[me] if to else okv
        remote(src, kvg.at[me], KVG_SEND + to, KVG_RECV, spot(step, 0, to)).start()

    def send_ng(step):
        remote(ng.at[me], ng.at[me], NG_SEND, NG_RECV + (step >> 2), spot(step, 0, 1)).start()

    def send_mx(z_step, y_step, to):
        src = rpart.at[z_step, 0]
        dst = rpart.at[z_step, y_step]
        remote(src, dst, MX_SEND, MX_RECV + z_step, spot(0, y_step, to)).start()

    def out_copy(which, b):
        buf, out = ((kbuf, keys_out), (vbuf, values_out))[which]
        return pltpu.make_async_copy(buf.at[b], out.at[b], sems.at[OUT + 3 * core + which])

    loads[0].wait()
    loads[1].wait()
    wide = tok[...].astype(F32)
    gained = (wide * gain_ref[...]).astype(BF16)
    square = jnp.sum(wide * wide, axis=1, keepdims=True)
    eye = lax.broadcasted_iota(jnp.int32, (PROP, BLOCK), 0) == lax.broadcasted_iota(jnp.int32, (PROP, BLOCK), 1)
    loads[2].wait()
    partial_q = _dot(gained, wqkv[0])
    for b in range(SEQS):
        column = square[b * PROP : (b + 1) * PROP]
        row = jnp.sum(jnp.where(eye, column, 0.0), axis=0, keepdims=True)
        tail = _split_rows(row)
        for block in range(4):
            chunk = partial_q[b * PROP : (b + 1) * PROP, block * BLOCK : (block + 1) * BLOCK]
            pq[b * 4 + block] = jnp.concatenate([chunk, tail], axis=0).astype(BF16)

    @pl.when(is_owner)
    def _():
        pl.semaphore_wait(barrier, KV - 1 + 3)

    @pl.when(is_other)
    def _():
        pl.semaphore_wait(barrier, KV + 3)

    for step in PARTNERS:
        send_q(step)

    @pl.when(is_other)
    def _():
        send_q(0)

        def tell(kv_step, y_step):
            pl.semaphore_signal(
                ready, inc=1, device_id=spot(kv_step, y_step, 1), device_id_type=pl.DeviceIdType.MESH
            )

        for step in PARTNERS + [0]:
            tell(step, 0)
        for step in Y_STEPS:
            tell(0, step)

    projected = []
    for which in range(2):
        loads[3 + which].wait()
        projected.append(_dot(gained, wqkv[1 + which]))
    for b in range(SEQS):
        for block in range(4):
            pkv[b * 4 + block] = jnp.concatenate(
                [
                    part_kv[b * PROP : (b + 1) * PROP, block * BLOCK : (block + 1) * BLOCK]
                    for part_kv in projected
                ],
                axis=0,
            ).astype(BF16)
    loads[5].wait()

    def transpose_values(b):
        for block in range(4):
            vt[b, block * BLOCK : (block + 1) * BLOCK, :] = jnp.transpose(
                vbuf[b, :, block * BLOCK : (block + 1) * BLOCK]
            )

    for order in range(SEQS):
        for half in range(2):
            for side in range(2):
                qe[order, half, side * BLOCK : (side + 1) * BLOCK, (1 - side) * BLOCK : (2 - side) * BLOCK] = (
                    jnp.zeros((BLOCK, BLOCK), BF16)
                )
    for b in range(SEQS):
        transpose_values(b)
    for index in (6, 7, 8, 9, 10, 11, 12):
        loads[index].wait()

    zero_tail = jnp.zeros((PAD - PROP, BLOCK), F32)
    lane = lax.broadcasted_iota(jnp.int32, (HEAD, BLOCK), 1)
    second_head = ((lane >= PROP) & (lane < 2 * PROP)) | (lane >= 3 * PROP)

    @pl.when(is_owner)
    def _():
        arrived(rq.at[0:31], Q_RECV)
        for group in range(2):
            total = (pq[me] if group else rq[0]).astype(F32)
            for step in range(1, KV):
                total = total + rq[group * KV + step].astype(F32)
            square_row = jnp.sum(total[PROP:PAD], axis=0, keepdims=True)
            square_column = jnp.sum(jnp.where(eye, square_row, 0.0), axis=1, keepdims=True)
            factor = lax.rsqrt(square_column / D + EPS)
            own_factor[group] = jnp.broadcast_to(factor, (PROP, BLOCK))
            own_q = (total[0:PROP] * factor).astype(BF16)
            if group:
                qg[me] = own_q
            else:
                oq[...] = own_q
        pl.semaphore_wait(ready, KV + 3)
        for z_step in Z_SEND:
            for step in PARTNERS + [0]:
                if step >> 2 == z_step:
                    send_qg(step, 0)
                    if step:
                        send_qg(step, 1)
        pl.semaphore_signal(go, inc=1, device_id=spot(0, 0, 0), device_id_type=pl.DeviceIdType.MESH)
        for step in PARTNERS:
            send_kv(step)

    @pl.when(is_other)
    def _():
        pl.semaphore_wait(go, 1)
        for step in PARTNERS + [0]:
            send_kv(step)
        remote(wo.at[0], wo.at[0], GIVE_SEND, GIVE_RECV, spot(0, 0, 1)).start()
        remote(og.at[0], og.at[0], GIVE_SEND + 1, GIVE_RECV + 1, spot(0, 0, 1)).start()
        remote(lam.at[0], lam.at[0], GIVE_SEND + 2, GIVE_RECV + 2, spot(0, 0, 1)).start()


    def gathered(z_step):
        if z_step:
            arrived(qg.at[pl.ds((z ^ z_step) * 4, 4)], QG_RECV + z_step)
            return

        @pl.when(is_owner)
        def _():
            arrived(qg.at[0:3], QG_RECV)

        @pl.when(is_other)
        def _():
            arrived(qg.at[0:4], QG_RECV)

    def expand(order):
        b = z ^ Z_ORDER[order]
        for half in range(2):
            for side in range(2):
                chunk = qg[b * 4 + half * 2 + side].astype(F32)
                lanes = slice(side * BLOCK, (side + 1) * BLOCK)
                qe[order, half, lanes, lanes] = _expanded(chunk)

    def score(order):
        b = z ^ Z_ORDER[order]
        begin = len_ref[b] + acc_ref[b] - me * POS
        visible = lax.broadcasted_iota(jnp.int32, (POS, BLOCK), 0) < begin
        visible = jnp.concatenate([visible, visible], axis=1)
        for half in range(2):
            keys = kbuf[b, :, half * 2 * BLOCK : (half + 1) * 2 * BLOCK]
            scores = jnp.where(visible, _dot_nt(keys, qe[order, half]) * SCALE2, LOW)
            sc[order % 2, half] = scores
            sm[order % 2, half] = jnp.max(scores, axis=0, keepdims=True)

    def weigh(order):
        b = z ^ Z_ORDER[order]
        for half in range(2):
            largest = sm[order % 2, half]
            weight = jnp.exp2(sc[order % 2, half] - largest)
            weight_sum = jnp.sum(weight, axis=0, keepdims=True)
            weight = weight.astype(BF16)
            for side in range(2):
                block = half * 2 + side
                lanes = slice(side * BLOCK, (side + 1) * BLOCK)
                out = _dot(vt[b, block * BLOCK : (block + 1) * BLOCK, :], weight[:, lanes])
                owner = b * 4 + block
                dv[owner] = _packed(jnp.where(second_head, out[HEAD:], out[:HEAD])).astype(BF16)
                ds[owner] = jnp.concatenate([largest[:, lanes], weight_sum[:, lanes]], axis=0)

    def send(order):
        for x_step in (2, 1, 3, 0):
            step = Z_ORDER[order] << 2 | x_step
            if step:
                send_d(step)
        if Z_ORDER[order] == 0:

            @pl.when(is_other)
            def _():
                send_d(0)

    for group in Z_GROUPS:
        for order in group:
            gathered(Z_ORDER[order])
        for order in group:
            expand(order)
        score(group[0])
        for order in group:
            if order + 1 in group:
                score(order + 1)
            weigh(order)
            send(order)

    @pl.when(is_owner)
    def _():
        arrived(rkv.at[0:31], KV_RECV)
        for group in range(2):
            summed = (pkv[me] if group else rkv[0]).astype(F32)
            for step in range(1, KV):
                summed = summed + rkv[group * KV + step].astype(F32)
            rows = [summed[0:PROP] * own_factor[group], summed[PROP:] * own_factor[group]]
            rows = jnp.concatenate(rows, axis=0).astype(BF16)
            if group:
                kvg[me] = rows
            else:
                okv[...] = rows
        par_pad[...] = jnp.full((8, BLOCK), -1, jnp.int32)
        par_pad[0:SEQS, 0:PROP] = par_ref[...]
        parent_row = par_pad[pl.ds(z, 1), :]
        row_index = lax.broadcasted_iota(jnp.int32, (BLOCK, BLOCK), 0)
        lane_index = lax.broadcasted_iota(jnp.int32, (BLOCK, BLOCK), 1)
        reach = ((parent_row == row_index) & (lane_index < PROP)) | (row_index == lane_index)
        reach = jnp.where(reach, 1.0, 0.0).astype(BF16)
        for _ in range(5):
            reach = jnp.minimum(_dot(reach, reach), 1.0).astype(BF16)
        spread = (lax.rem(lane_index, PROP) == row_index) & (lane_index < 4 * PROP) & (row_index < PROP)
        lineage = _dot(reach, jnp.where(spread, 1.0, 0.0).astype(BF16))[0:PAD]
        linked = (lineage > 0.5) & (lax.broadcasted_iota(jnp.int32, (PAD, BLOCK), 0) < PROP)
        for group in range(2):
            own_expanded = _expanded((qg[me] if group else oq[...]).astype(F32))
            own_kv = (kvg[me] if group else okv[...]).astype(F32)
            own_k = jnp.concatenate([own_kv[0:PROP], zero_tail], axis=0).astype(BF16)
            own_v = jnp.concatenate([own_kv[PROP:], zero_tail], axis=0)
            self_scores = _dot_nt(own_k, own_expanded) * SCALE2
            self_scores = jnp.where(linked, self_scores, LOW)
            largest = jnp.max(self_scores, axis=0, keepdims=True)
            self_weight = jnp.where(linked, jnp.exp2(self_scores - largest), 0.0)
            self_stats[group, 0:1] = largest
            self_stats[group, 1:2] = jnp.sum(self_weight, axis=0, keepdims=True)
            self_out = _dot(jnp.transpose(own_v).astype(BF16), self_weight.astype(BF16))
            self_sum[group] = jnp.where(second_head, self_out[HEAD:], self_out[:HEAD])
        lane_row = lax.broadcasted_iota(jnp.int32, (1, BLOCK), 1)
        arrived(og.at[0], GIVE_RECV + 1)
        arrived(lam.at[0], GIVE_RECV + 2)
        arrived(wo.at[0], GIVE_RECV)
        lam_rows = []
        for group in range(2):
            index = lax.broadcasted_iota(jnp.int32, (1, TP), 1)
            pair = [
                jnp.sum(jnp.where(index == x * 2 + head, lam[group], 0.0), axis=1, keepdims=True)
                for head in range(2)
            ]
            lam_rows.append(jnp.where(lane_row < PROP, pair[0], pair[1]))

        arrived(rds.at[0:31], DS_RECV)
        self_factor = []
        factors = []
        used = lax.broadcasted_iota(jnp.int32, (KV, BLOCK), 1) < 96
        for group in range(2):
            slots = [ds.at[me] if group else rds.at[0]] + [rds.at[group * KV + step] for step in range(1, KV)]
            maxima = jnp.concatenate([slot[0:1] for slot in slots], axis=0)
            totals = jnp.concatenate([slot[1:2] for slot in slots], axis=0)
            top = jnp.maximum(jnp.max(maxima, axis=0, keepdims=True), self_stats[group, 0:1])
            own = jnp.exp2(self_stats[group, 0:1] - top)
            factor = jnp.exp2(maxima - top)
            denominator = self_stats[group, 1:2] * own + jnp.sum(totals * factor, axis=0, keepdims=True)
            inverse = 1.0 / denominator
            factor = factor * inverse
            self_factor.append(own * inverse)
            factors.append(
                [jnp.where(used, factor, pltpu.roll(factor, 96 - 32 * third, 1)) for third in range(3)]
            )
        arrived(rdv.at[0:31], DV_RECV)
        for group in range(2):
            slots = [dv.at[me] if group else rdv.at[0]] + [rdv.at[group * KV + step] for step in range(1, KV)]
            merged = []
            for third in range(3):
                rows = slice(16 * third, 16 * third + 16)
                sums = [
                    slot[rows].astype(F32) * factors[group][third][step : step + 1]
                    for step, slot in enumerate(slots)
                ]
                while len(sums) > 1:
                    sums = [a + b for a, b in zip(sums[::2], sums[1::2])]
                merged.append(sums[0])
            attended = _unpacked(jnp.concatenate(merged, axis=0)) + self_sum[group] * self_factor[group]
            difference = attended - lam_rows[group] * pltpu.roll(attended, BLOCK - 2 * PROP, 1)
            power = jnp.mean(difference * difference, axis=0, keepdims=True)
            normed = difference * lax.rsqrt(power + EPS)
            stacked = jnp.concatenate([normed, pltpu.roll(normed, BLOCK - PROP, 1)], axis=0)
            turned = jnp.transpose(stacked)[0:PROP]
            turned = turned * og[group, pl.ds(x, 1), :]
            ng[me, group] = turned.astype(BF16)
        for step in PARTNERS:
            send_ng(step)
        for z_step in (2, 1, 3, 0):

            @pl.when((z ^ z_step) >= 2)
            def _(z_step=z_step):
                for step in PARTNERS + [0]:
                    if step >> 2 == z_step:
                        send_kvg(step, 0)
                        if step:
                            send_kvg(step, 1)


        for z_step in Z_OUT:
            arrived(ng.at[pl.ds((z ^ z_step) * 4, 4 if z_step else 3)], NG_RECV + z_step)
            b = z ^ z_step
            projected = 0.0
            for group in range(2):
                rows = jnp.concatenate([ng[b * 4 + block, group] for block in range(4)], axis=1)
                projected = projected + _dot(rows, wo[group])
            rpart[z_step, 0] = projected.astype(BF16)
            for step in Y_STEPS:
                send_mx(z_step, step, 1)
            for step in Y_STEPS:
                send_mx(z_step, step, 0)
            send_mx(z_step, 0, 0)

    @pl.when(is_owner & (z >= 2))
    def _():
        arrived(kvg.at[1:], KVG_RECV)

    @pl.when(is_other & (z >= 2))
    def _():
        arrived(kvg, KVG_RECV)

    @pl.when(z >= 2)
    def _():
        for b in range(SEQS):
            begin = len_ref[b] + acc_ref[b] - me * POS
            position = lax.broadcasted_iota(jnp.int32, (POS, BLOCK), 0) - begin
            written = (position >= 0) & (position < PROP)
            slot = lax.broadcasted_iota(jnp.int32, (POS, BLOCK), 1)
            for which, buf in enumerate((kbuf, vbuf)):
                offset = which * PROP
                placing = jnp.where(written & (position + offset == slot), 1.0, 0.0)
                placing = placing.astype(BF16)[:, 0 : 2 * PROP]
                for block in range(4):
                    lanes = slice(block * BLOCK, (block + 1) * BLOCK)
                    moved = _dot(placing, kvg[b * 4 + block])
                    buf[b, :, lanes] = jnp.where(written, moved, buf[b, :, lanes].astype(F32)).astype(BF16)
                out_copy(which, b).start()

    @pl.when(z < 2)
    def _():
        for b in range(SEQS):
            for which in range(2):
                out_copy(which, b).start()

    for z_step in Z_OUT:

        @pl.when(is_owner)
        def _(z_step=z_step):
            arrived(rpart.at[z_step, 1:], MX_RECV + z_step)

        @pl.when(is_other)
        def _(z_step=z_step):
            arrived(rpart.at[z_step], MX_RECV + z_step)

        mixed = rpart[z_step, 0].astype(F32)
        for step in range(1, 4):
            mixed = mixed + rpart[z_step, step].astype(F32)
        mixed_ref[z ^ z_step] = mixed.astype(BF16)

    arrived(kbuf, OUT + 3 * core)
    arrived(vbuf, OUT + 3 * core + 1)
    sent = ((pq, Q_SEND), (pkv, KV_SEND), (dv, DV_SEND), (ds, DS_SEND))

    @pl.when(is_owner)
    def _():
        for ref, index in sent + ((qg, QG_SEND + 1), (ng, NG_SEND)):
            arrived(ref.at[1:], index)
        arrived(qg, QG_SEND)
        arrived(kvg.at[0:8], KVG_SEND)
        arrived(rpart.at[0:7], MX_SEND)

    @pl.when(is_owner & (z < 2))
    def _():
        arrived(kvg.at[0:8], KVG_SEND + 1)

    @pl.when(is_owner & (z >= 2))
    def _():
        arrived(kvg.at[0:7], KVG_SEND + 1)

    @pl.when(is_other)
    def _():
        for ref, index in sent:
            arrived(ref, index)
        arrived(wo.at[0], GIVE_SEND)
        arrived(og.at[0], GIVE_SEND + 1)
        arrived(lam.at[0], GIVE_SEND + 2)


def _main(*arrays):
    hbm = pl.BlockSpec(memory_space=pltpu.HBM)
    vmem = pl.BlockSpec(memory_space=pltpu.VMEM)
    dma = pltpu.SemaphoreType.DMA
    return pl.pallas_call(
        _main_kernel,
        out_shape=(
            jax.ShapeDtypeStruct((SEQS, PROP, 256), BF16),
            jax.ShapeDtypeStruct((SEQS, POS, 512), BF16),
            jax.ShapeDtypeStruct((SEQS, POS, 512), BF16),
        ),
        in_specs=[hbm] * 14,
        out_specs=(vmem, pl.BlockSpec(memory_space=pl.ANY), pl.BlockSpec(memory_space=pl.ANY)),
        scratch_shapes=[
            pltpu.VMEM((SEQS, POS, 512), BF16),
            pltpu.VMEM((SEQS, POS, 512), BF16),
            pltpu.VMEM((ROWS, 256), BF16),
            pltpu.VMEM((1, 256), F32),
            pltpu.VMEM((2, 4, BLOCK), F32),
            pltpu.VMEM((SEQS, PROP), jnp.int32),
            pltpu.VMEM((2, 1, TP), F32),
            pltpu.SMEM((SEQS,), jnp.int32),
            pltpu.SMEM((SEQS,), jnp.int32),
            pltpu.VMEM((3, 256, 512), BF16),
            pltpu.VMEM((2, 512, 256), BF16),
            pltpu.VMEM((SEQS, 512, POS), BF16),
            pltpu.VMEM((KV, PAD, BLOCK), BF16),
            pltpu.VMEM((2 * KV, PAD, BLOCK), BF16),
            pltpu.VMEM((KV, 2 * PROP, BLOCK), BF16),
            pltpu.VMEM((2 * KV, 2 * PROP, BLOCK), BF16),
            pltpu.VMEM((PROP, BLOCK), BF16),
            pltpu.VMEM((2 * PROP, BLOCK), BF16),
            pltpu.VMEM((KV, PROP, BLOCK), BF16),
            pltpu.VMEM((KV, 2 * PROP, BLOCK), BF16),
            pltpu.VMEM((KV, 48, BLOCK), BF16),
            pltpu.VMEM((2 * KV, 48, BLOCK), BF16),
            pltpu.VMEM((KV, 2, BLOCK), F32),
            pltpu.VMEM((2 * KV, 2, BLOCK), F32),
            pltpu.VMEM((KV, 2, PROP, BLOCK), BF16),
            pltpu.VMEM((8, 4, PROP, 256), BF16),
            pltpu.VMEM((8, BLOCK), jnp.int32),
            pltpu.VMEM((SEQS, 2, 2 * BLOCK, 2 * BLOCK), BF16),
            pltpu.VMEM((2, 2, POS, 2 * BLOCK), F32),
            pltpu.VMEM((2, 2, 1, 2 * BLOCK), F32),
            dma((SEMAPHORES,)),
            pltpu.SemaphoreType.REGULAR,
            pltpu.SemaphoreType.REGULAR,
            pltpu.VMEM((2, PROP, BLOCK), F32),
            pltpu.VMEM((2, 2, BLOCK), F32),
            pltpu.VMEM((2, HEAD, BLOCK), F32),
        ],
        compiler_params=pltpu.CompilerParams(
            collective_id=0, has_side_effects=True, vmem_limit_bytes=MAIN_VMEM
        ),
        name="attention",
    )(*(pltpu.with_memory_space_constraint(array, pltpu.HBM) for array in arrays))


def _copies_first(which):
    kv = lax.axis_index("kv")
    y = lax.axis_index("tp") // 2
    return (kv < 4) & (kv + y * 4 < 6) if which else (kv + y) < 1


def _copy_kernel(keys_in, values_in, keys_out, values_out, kbuf, vbuf, sem):
    pairs = ((keys_in, kbuf, keys_out), (values_in, vbuf, values_out))
    fetches = [pltpu.make_async_copy(src, buf, sem.at[which]) for which, (src, buf, _) in enumerate(pairs)]
    puts = [pltpu.make_async_copy(buf, dst, sem.at[which]) for which, (_, buf, dst) in enumerate(pairs)]

    @pl.when(_copies_first(1))
    def _():
        fetches[1].start()

        @pl.when(_copies_first(0))
        def _():
            fetches[0].start()

        fetches[1].wait()
        puts[1].start()

        @pl.when(_copies_first(0))
        def _():
            fetches[0].wait()
            puts[0].start()
            puts[0].wait()

        puts[1].wait()


def _copy(*arrays):
    hbm = pl.BlockSpec(memory_space=pltpu.HBM)
    return pl.pallas_call(
        _copy_kernel,
        out_shape=tuple(jax.ShapeDtypeStruct(array.shape, array.dtype) for array in arrays),
        in_specs=[hbm] * 2,
        out_specs=(hbm,) * 2,
        scratch_shapes=[
            pltpu.VMEM((SEQS, POS, 512), BF16),
            pltpu.VMEM((SEQS, POS, 512), BF16),
            pltpu.SemaphoreType.DMA((2,)),
        ],
        compiler_params=pltpu.CompilerParams(vmem_limit_bytes=MAIN_VMEM),
        name="copy_caches",
    )(*(pltpu.with_memory_space_constraint(array, pltpu.HBM) for array in arrays))


def _write_kernel(mixed_ref, keys_ref, values_ref, _keys, _values, mixed_hbm, keys_hbm, values_hbm, sem):
    mixed_copy = pltpu.make_async_copy(mixed_ref, mixed_hbm, sem.at[2])
    mixed_copy.start()

    copies = [
        pltpu.make_async_copy(keys_ref, keys_hbm, sem.at[0]),
        pltpu.make_async_copy(values_ref, values_hbm, sem.at[1]),
    ]

    @pl.when(jnp.logical_not(_copies_first(0)))
    def _():
        copies[0].start()

        @pl.when(jnp.logical_not(_copies_first(1)))
        def _():
            copies[1].start()
            copies[1].wait()

        copies[0].wait()

    mixed_copy.wait()


def _write(*arrays):
    hbm = pl.BlockSpec(memory_space=pltpu.HBM)
    anywhere = pl.BlockSpec(memory_space=pl.ANY)
    return pl.pallas_call(
        _write_kernel,
        out_shape=tuple(jax.ShapeDtypeStruct(array.shape, array.dtype) for array in arrays[:3]),
        in_specs=[anywhere] * 3 + [hbm] * 2,
        out_specs=(hbm,) * 3,
        input_output_aliases={3: 1, 4: 2},
        scratch_shapes=[pltpu.SemaphoreType.DMA((3,))],
        compiler_params=pltpu.CompilerParams(vmem_limit_bytes=WRITE_VMEM),
        name="write",
    )(*arrays)


def _local(
    tokens,
    norm_gain,
    w_query,
    w_key,
    w_value,
    w_output,
    cache_keys,
    cache_values,
    map_lambda,
    out_gain,
    parents,
    lengths,
    accepted,
):
    first_keys, first_values = _copy(cache_keys, cache_values)
    mixed, keys, values = _main(
        tokens,
        norm_gain.reshape(1, 256),
        w_query,
        w_key,
        w_value,
        w_output,
        cache_keys,
        cache_values,
        map_lambda.reshape(1, TP),
        out_gain.reshape(4, BLOCK),
        parents,
        lengths,
        accepted,
        first_keys,
    )
    mixed, new_keys, new_values = _write(mixed, keys, values, first_keys, first_values)
    return mixed.reshape(ROWS, 256), new_keys, new_values


def solution(mesh):
    return jax.shard_map(
        _local,
        mesh=mesh,
        in_specs=(
            P(None, "kv"),
            P("kv"),
            P("kv", "tp"),
            P("kv", "tp"),
            P("kv", "tp"),
            P("tp", "kv"),
            P(None, "kv", "tp"),
            P(None, "kv", "tp"),
            P("tp"),
            P("tp"),
            P(),
            P(),
            P(),
        ),
        out_specs=(P(None, "kv"), P(None, "kv", "tp"), P(None, "kv", "tp")),
        check_vma=False,
    )
```

```python
import functools

import jax
import jax.numpy as jnp
from jax import lax
from jax.experimental import pallas as pl
from jax.experimental.pallas import tpu as pltpu
from jax.sharding import PartitionSpec as P

D = 4096
HEAD = 64
QK = 32
SEQS = 4
PROP = 24
KV = 16
TP = 8
BLOCK = 128
PAD = 32
POS = 512
ROWS = 96
EPS = 1e-05
LOW = -1e30
LOG2E = 1.4426950408889634
WRITE_VMEM = 16 * 1024 * 1024
MAIN_VMEM = 40 * 1024 * 1024
SCALE2 = QK ** (-0.5) * LOG2E
F32 = jnp.float32
BF16 = jnp.bfloat16
NT = (((1,), (1,)), ((), ()))


def _distance(step):
    ring = (0, 1, 2, 1)
    return ring[step >> 2] + ring[step & 3]


LOADS = 13
Q_SEND = 0
KV_SEND = 1
QG_SEND = 2
KVG_SEND = 4
DV_SEND = 6
DS_SEND = 7
NG_SEND = 8
MX_SEND = 9
GIVE_SEND = 10
Q_RECV = 13
KV_RECV = 14
DV_RECV = 15
DS_RECV = 16
QG_RECV = 17
KVG_RECV = 21
NG_RECV = 22
MX_RECV = 26
GIVE_RECV = 30
SEMAPHORES = 33
OUT = 8
Z_ORDER = (0, 1, 2, 3)
Z_OUT = (0, 1, 3, 2)
Z_OUT_GROUPS = ((0,), (1,), (3, 2))
Z_SEND = (0, 1, 2, 3)
Z_GROUPS = ((0,), (1,), (2, 3))
Y_STEPS = (2, 1, 3)
PARTNERS = sorted(range(1, KV), key=lambda step: -_distance(step))


def _dot(a, b):
    return jnp.dot(a, b, preferred_element_type=F32)


def _dot_nt(a, b):
    return lax.dot_general(a, b, NT, preferred_element_type=F32)


def _split_rows(row):
    high = row.astype(BF16).astype(F32)
    middle = (row - high).astype(BF16).astype(F32)
    low = row - high - middle
    index = lax.broadcasted_iota(jnp.int32, (PAD - PROP, BLOCK), 0)
    return jnp.where(index == 0, high, jnp.where(index == 1, middle, jnp.where(index == 2, low, 0.0)))


def _packed(block):
    rest = block[48:]
    moved = jnp.concatenate([pltpu.roll(rest, 96 - 32 * part, 1) for part in range(3)], axis=0)
    return jnp.where(lax.broadcasted_iota(jnp.int32, (48, BLOCK), 1) < 96, block[:48], moved)


def _unpacked(packed):
    lane = lax.broadcasted_iota(jnp.int32, (16, BLOCK), 1)
    parts = [pltpu.roll(packed[16 * part : 16 * part + 16], 32 * part + 32, 1) for part in range(3)]
    rest = jnp.where(lane < 32, parts[0], jnp.where(lane < 64, parts[1], parts[2]))
    return jnp.concatenate([packed, rest], axis=0)


def _expanded(chunk):
    lane = lax.broadcasted_iota(jnp.int32, (PROP, BLOCK), 1)
    parts = []
    for which in range(2):
        for head in range(2):
            low = head * HEAD + which * QK
            inside = (lane >= low) & (lane < low + QK)
            parts.append(jnp.where(inside, chunk, 0.0))
    parts.append(jnp.zeros((BLOCK - 4 * PROP, BLOCK), F32))
    return jnp.concatenate(parts, axis=0).astype(BF16)


def _main_kernel(
    tok_hbm,
    gain_hbm,
    wq_hbm,
    wk_hbm,
    wv_hbm,
    wo_hbm,
    ck_hbm,
    cv_hbm,
    lam_hbm,
    og_hbm,
    par_hbm,
    len_hbm,
    acc_hbm,
    _first_keys,
    mixed_ref,
    keys_out,
    values_out,
    kbuf,
    vbuf,
    tok,
    gain_ref,
    og,
    par_ref,
    lam,
    len_ref,
    acc_ref,
    wqkv,
    wo,
    vt,
    pq,
    rq,
    pkv,
    rkv,
    oq,
    okv,
    qg,
    kvg,
    dv,
    rdv,
    ds,
    rds,
    ng,
    rpart,
    par_pad,
    qe,
    sc,
    sm,
    sems,
    ready,
    go,
    own_factor,
    self_stats,
    self_sum,
):
    me = lax.axis_index("kv")
    tp = lax.axis_index("tp")
    z = me // 4
    x = lax.rem(me, 4)
    core = lax.rem(tp, 2)
    first = tp - core
    is_owner = core == 1
    is_other = core == 0

    def spot(kv_step, y_step, to):
        return {"kv": me ^ kv_step, "tp": (first ^ (2 * y_step)) + to}

    barrier = pltpu.get_barrier_semaphore()

    def greet(kv_step, y_step, to):
        pl.semaphore_signal(
            barrier, inc=1, device_id=spot(kv_step, y_step, to), device_id_type=pl.DeviceIdType.MESH
        )

    @pl.when(is_owner)
    def _():
        for step in PARTNERS:
            greet(step, 0, 0)
            greet(step, 0, 1)
        greet(0, 0, 0)
        for step in Y_STEPS:
            greet(0, step, 1)
            greet(0, step, 0)


    loads = [
        (tok_hbm, tok),
        (gain_hbm, gain_ref),
        (wq_hbm, wqkv.at[0]),
        (wk_hbm, wqkv.at[1]),
        (wv_hbm, wqkv.at[2]),
        (cv_hbm, vbuf),
        (ck_hbm, kbuf),
        (wo_hbm, wo.at[core]),
        (og_hbm, og.at[core]),
        (lam_hbm, lam.at[core]),
        (par_hbm, par_ref),
        (len_hbm, len_ref),
        (acc_hbm, acc_ref),
    ]
    loads = [pltpu.make_async_copy(src, dst, sems.at[index]) for index, (src, dst) in enumerate(loads)]
    for copy in loads:
        copy.start()

    def arrived(ref, index):
        pltpu.make_async_copy(ref, ref, sems.at[index]).wait()

    def remote(src, dst, send, recv, where):
        return pltpu.make_async_remote_copy(
            src_ref=src,
            dst_ref=dst,
            send_sem=sems.at[send],
            recv_sem=sems.at[recv],
            device_id=where,
            device_id_type=pl.DeviceIdType.MESH,
        )

    def send_q(step):
        remote(pq.at[me ^ step], rq.at[core * KV + step], Q_SEND, Q_RECV, spot(step, 0, 1)).start()

    def send_kv(step):
        remote(pkv.at[me ^ step], rkv.at[core * KV + step], KV_SEND, KV_RECV, spot(step, 0, 1)).start()

    def send_d(step):
        remote(ds.at[me ^ step], rds.at[core * KV + step], DS_SEND, DS_RECV, spot(step, 0, 1)).start()
        remote(dv.at[me ^ step], rdv.at[core * KV + step], DV_SEND, DV_RECV, spot(step, 0, 1)).start()

    def send_qg(step, to):
        src = qg.at[me] if to else oq
        remote(src, qg.at[me], QG_SEND + to, QG_RECV + (step >> 2), spot(step, 0, to)).start()

    def send_kvg(step, to):
        src = kvg.at[me] if to else okv
        remote(src, kvg.at[me], KVG_SEND + to, KVG_RECV, spot(step, 0, to)).start()

    def send_ng(step):
        remote(ng.at[me], ng.at[me], NG_SEND, NG_RECV + (step >> 2), spot(step, 0, 1)).start()

    def send_mx(z_step, y_step, to):
        src = rpart.at[z_step, 0]
        dst = rpart.at[z_step, y_step]
        remote(src, dst, MX_SEND, MX_RECV + z_step, spot(0, y_step, to)).start()

    def out_copy(which, b):
        buf, out = ((kbuf, keys_out), (vbuf, values_out))[which]
        return pltpu.make_async_copy(buf.at[b], out.at[b], sems.at[OUT + 3 * core + which])

    loads[0].wait()
    loads[1].wait()
    wide = tok[...].astype(F32)
    gained = (wide * gain_ref[...]).astype(BF16)
    square = jnp.sum(wide * wide, axis=1, keepdims=True)
    eye = lax.broadcasted_iota(jnp.int32, (PROP, BLOCK), 0) == lax.broadcasted_iota(jnp.int32, (PROP, BLOCK), 1)
    loads[2].wait()
    partial_q = _dot(gained, wqkv[0])
    for b in range(SEQS):
        column = square[b * PROP : (b + 1) * PROP]
        row = jnp.sum(jnp.where(eye, column, 0.0), axis=0, keepdims=True)
        tail = _split_rows(row)
        for block in range(4):
            chunk = partial_q[b * PROP : (b + 1) * PROP, block * BLOCK : (block + 1) * BLOCK]
            pq[b * 4 + block] = jnp.concatenate([chunk, tail], axis=0).astype(BF16)

    @pl.when(is_owner)
    def _():
        pl.semaphore_wait(barrier, KV - 1 + 3)

    @pl.when(is_other)
    def _():
        pl.semaphore_wait(barrier, KV + 3)

    for step in PARTNERS:
        send_q(step)

    @pl.when(is_other)
    def _():
        send_q(0)

        def tell(kv_step, y_step):
            pl.semaphore_signal(
                ready, inc=1, device_id=spot(kv_step, y_step, 1), device_id_type=pl.DeviceIdType.MESH
            )

        for step in PARTNERS + [0]:
            tell(step, 0)
        for step in Y_STEPS:
            tell(0, step)

    projected = []
    for which in range(2):
        loads[3 + which].wait()
        projected.append(_dot(gained, wqkv[1 + which]))
    for b in range(SEQS):
        for block in range(4):
            pkv[b * 4 + block] = jnp.concatenate(
                [
                    part_kv[b * PROP : (b + 1) * PROP, block * BLOCK : (block + 1) * BLOCK]
                    for part_kv in projected
                ],
                axis=0,
            ).astype(BF16)
    loads[5].wait()

    def transpose_values(b):
        for block in range(4):
            vt[b, block * BLOCK : (block + 1) * BLOCK, :] = jnp.transpose(
                vbuf[b, :, block * BLOCK : (block + 1) * BLOCK]
            )

    for order in range(SEQS):
        for half in range(2):
            for side in range(2):
                qe[order, half, side * BLOCK : (side + 1) * BLOCK, (1 - side) * BLOCK : (2 - side) * BLOCK] = (
                    jnp.zeros((BLOCK, BLOCK), BF16)
                )
    for b in range(SEQS):
        transpose_values(b)
    for index in (6, 7, 8, 9, 10, 11, 12):
        loads[index].wait()

    zero_tail = jnp.zeros((PAD - PROP, BLOCK), F32)
    lane = lax.broadcasted_iota(jnp.int32, (HEAD, BLOCK), 1)
    second_head = ((lane >= PROP) & (lane < 2 * PROP)) | (lane >= 3 * PROP)

    @pl.when(is_owner)
    def _():
        arrived(rq.at[0:31], Q_RECV)
        for group in range(2):
            total = (pq[me] if group else rq[0]).astype(F32)
            for step in range(1, KV):
                total = total + rq[group * KV + step].astype(F32)
            square_row = jnp.sum(total[PROP:PAD], axis=0, keepdims=True)
            square_column = jnp.sum(jnp.where(eye, square_row, 0.0), axis=1, keepdims=True)
            factor = lax.rsqrt(square_column / D + EPS)
            own_factor[group] = jnp.broadcast_to(factor, (PROP, BLOCK))
            own_q = (total[0:PROP] * factor).astype(BF16)
            if group:
                qg[me] = own_q
            else:
                oq[...] = own_q
        pl.semaphore_wait(ready, KV + 3)
        for z_step in Z_SEND:
            for step in PARTNERS + [0]:
                if step >> 2 == z_step:
                    send_qg(step, 0)
                    if step:
                        send_qg(step, 1)
        pl.semaphore_signal(go, inc=1, device_id=spot(0, 0, 0), device_id_type=pl.DeviceIdType.MESH)
        for step in PARTNERS:
            send_kv(step)

    @pl.when(is_other)
    def _():
        pl.semaphore_wait(go, 1)
        for step in PARTNERS + [0]:
            send_kv(step)
        remote(wo.at[0], wo.at[0], GIVE_SEND, GIVE_RECV, spot(0, 0, 1)).start()
        remote(og.at[0], og.at[0], GIVE_SEND + 1, GIVE_RECV + 1, spot(0, 0, 1)).start()
        remote(lam.at[0], lam.at[0], GIVE_SEND + 2, GIVE_RECV + 2, spot(0, 0, 1)).start()


    def gathered(z_step):
        if z_step:
            arrived(qg.at[pl.ds((z ^ z_step) * 4, 4)], QG_RECV + z_step)
            return

        @pl.when(is_owner)
        def _():
            arrived(qg.at[0:3], QG_RECV)

        @pl.when(is_other)
        def _():
            arrived(qg.at[0:4], QG_RECV)

    def expand(order):
        b = z ^ Z_ORDER[order]
        for half in range(2):
            for side in range(2):
                chunk = qg[b * 4 + half * 2 + side].astype(F32)
                lanes = slice(side * BLOCK, (side + 1) * BLOCK)
                qe[order, half, lanes, lanes] = _expanded(chunk)

    def score(order):
        b = z ^ Z_ORDER[order]
        begin = len_ref[b] + acc_ref[b] - me * POS
        visible = lax.broadcasted_iota(jnp.int32, (POS, BLOCK), 0) < begin
        visible = jnp.concatenate([visible, visible], axis=1)
        for half in range(2):
            keys = kbuf[b, :, half * 2 * BLOCK : (half + 1) * 2 * BLOCK]
            scores = jnp.where(visible, _dot_nt(keys, qe[order, half]) * SCALE2, LOW)
            sc[order % 2, half] = scores
            sm[order % 2, half] = jnp.max(scores, axis=0, keepdims=True)

    def weigh(order):
        b = z ^ Z_ORDER[order]
        for half in range(2):
            largest = sm[order % 2, half]
            weight = jnp.exp2(sc[order % 2, half] - largest)
            weight_sum = jnp.sum(weight, axis=0, keepdims=True)
            weight = weight.astype(BF16)
            for side in range(2):
                block = half * 2 + side
                lanes = slice(side * BLOCK, (side + 1) * BLOCK)
                out = _dot(vt[b, block * BLOCK : (block + 1) * BLOCK, :], weight[:, lanes])
                owner = b * 4 + block
                dv[owner] = _packed(jnp.where(second_head, out[HEAD:], out[:HEAD])).astype(BF16)
                ds[owner] = jnp.concatenate([largest[:, lanes], weight_sum[:, lanes]], axis=0)

    def send(order):
        for x_step in (2, 1, 3, 0):
            step = Z_ORDER[order] << 2 | x_step
            if step:
                send_d(step)
        if Z_ORDER[order] == 0:

            @pl.when(is_other)
            def _():
                send_d(0)

    for group in Z_GROUPS:
        for order in group:
            gathered(Z_ORDER[order])
        for order in group:
            expand(order)
        score(group[0])
        for order in group:
            if order + 1 in group:
                score(order + 1)
            weigh(order)
            send(order)

    @pl.when(is_owner)
    def _():
        arrived(rkv.at[0:31], KV_RECV)
        for group in range(2):
            summed = (pkv[me] if group else rkv[0]).astype(F32)
            for step in range(1, KV):
                summed = summed + rkv[group * KV + step].astype(F32)
            rows = [summed[0:PROP] * own_factor[group], summed[PROP:] * own_factor[group]]
            rows = jnp.concatenate(rows, axis=0).astype(BF16)
            if group:
                kvg[me] = rows
            else:
                okv[...] = rows
        par_pad[...] = jnp.full((8, BLOCK), -1, jnp.int32)
        par_pad[0:SEQS, 0:PROP] = par_ref[...]
        parent_row = par_pad[pl.ds(z, 1), :]
        row_index = lax.broadcasted_iota(jnp.int32, (BLOCK, BLOCK), 0)
        lane_index = lax.broadcasted_iota(jnp.int32, (BLOCK, BLOCK), 1)
        reach = ((parent_row == row_index) & (lane_index < PROP)) | (row_index == lane_index)
        reach = jnp.where(reach, 1.0, 0.0).astype(BF16)
        for _ in range(5):
            reach = jnp.minimum(_dot(reach, reach), 1.0).astype(BF16)
        spread = (lax.rem(lane_index, PROP) == row_index) & (lane_index < 4 * PROP) & (row_index < PROP)
        lineage = _dot(reach, jnp.where(spread, 1.0, 0.0).astype(BF16))[0:PAD]
        linked = (lineage > 0.5) & (lax.broadcasted_iota(jnp.int32, (PAD, BLOCK), 0) < PROP)
        for group in range(2):
            own_expanded = _expanded((qg[me] if group else oq[...]).astype(F32))
            own_kv = (kvg[me] if group else okv[...]).astype(F32)
            own_k = jnp.concatenate([own_kv[0:PROP], zero_tail], axis=0).astype(BF16)
            own_v = jnp.concatenate([own_kv[PROP:], zero_tail], axis=0)
            self_scores = _dot_nt(own_k, own_expanded) * SCALE2
            self_scores = jnp.where(linked, self_scores, LOW)
            largest = jnp.max(self_scores, axis=0, keepdims=True)
            self_weight = jnp.where(linked, jnp.exp2(self_scores - largest), 0.0)
            self_stats[group, 0:1] = largest
            self_stats[group, 1:2] = jnp.sum(self_weight, axis=0, keepdims=True)
            self_out = _dot(jnp.transpose(own_v).astype(BF16), self_weight.astype(BF16))
            self_sum[group] = jnp.where(second_head, self_out[HEAD:], self_out[:HEAD])
        lane_row = lax.broadcasted_iota(jnp.int32, (1, BLOCK), 1)
        arrived(og.at[0], GIVE_RECV + 1)
        arrived(lam.at[0], GIVE_RECV + 2)
        arrived(wo.at[0], GIVE_RECV)
        lam_rows = []
        for group in range(2):
            index = lax.broadcasted_iota(jnp.int32, (1, TP), 1)
            pair = [
                jnp.sum(jnp.where(index == x * 2 + head, lam[group], 0.0), axis=1, keepdims=True)
                for head in range(2)
            ]
            lam_rows.append(jnp.where(lane_row < PROP, pair[0], pair[1]))

        arrived(rds.at[0:31], DS_RECV)
        self_factor = []
        factors = []
        used = lax.broadcasted_iota(jnp.int32, (KV, BLOCK), 1) < 96
        for group in range(2):
            slots = [ds.at[me] if group else rds.at[0]] + [rds.at[group * KV + step] for step in range(1, KV)]
            maxima = jnp.concatenate([slot[0:1] for slot in slots], axis=0)
            totals = jnp.concatenate([slot[1:2] for slot in slots], axis=0)
            top = jnp.maximum(jnp.max(maxima, axis=0, keepdims=True), self_stats[group, 0:1])
            own = jnp.exp2(self_stats[group, 0:1] - top)
            factor = jnp.exp2(maxima - top)
            denominator = self_stats[group, 1:2] * own + jnp.sum(totals * factor, axis=0, keepdims=True)
            inverse = 1.0 / denominator
            factor = factor * inverse
            self_factor.append(own * inverse)
            factors.append(
                [jnp.where(used, factor, pltpu.roll(factor, 96 - 32 * third, 1)) for third in range(3)]
            )
        arrived(rdv.at[0:31], DV_RECV)
        for group in range(2):
            slots = [dv.at[me] if group else rdv.at[0]] + [rdv.at[group * KV + step] for step in range(1, KV)]
            merged = []
            for third in range(3):
                rows = slice(16 * third, 16 * third + 16)
                sums = [
                    slot[rows].astype(F32) * factors[group][third][step : step + 1]
                    for step, slot in enumerate(slots)
                ]
                while len(sums) > 1:
                    sums = [a + b for a, b in zip(sums[::2], sums[1::2])]
                merged.append(sums[0])
            attended = _unpacked(jnp.concatenate(merged, axis=0)) + self_sum[group] * self_factor[group]
            difference = attended - lam_rows[group] * pltpu.roll(attended, BLOCK - 2 * PROP, 1)
            power = jnp.mean(difference * difference, axis=0, keepdims=True)
            normed = difference * lax.rsqrt(power + EPS)
            stacked = jnp.concatenate([normed, pltpu.roll(normed, BLOCK - PROP, 1)], axis=0)
            turned = jnp.transpose(stacked)[0:PROP]
            turned = turned * og[group, pl.ds(x, 1), :]
            ng[me, group] = turned.astype(BF16)
        for step in PARTNERS:
            send_ng(step)
        for z_step in (2, 1, 3, 0):

            @pl.when((z ^ z_step) >= 2)
            def _(z_step=z_step):
                for step in PARTNERS + [0]:
                    if step >> 2 == z_step:
                        send_kvg(step, 0)
                        if step:
                            send_kvg(step, 1)


        for group in Z_OUT_GROUPS:
            for z_step in group:
                arrived(ng.at[pl.ds((z ^ z_step) * 4, 4 if z_step else 3)], NG_RECV + z_step)
            sums = []
            for z_step in group:
                rows = [
                    jnp.concatenate([ng[(z ^ z_step) * 4 + block, half] for block in range(4)], axis=1)
                    for half in range(2)
                ]
                sums.append((_dot(rows[0], wo[0]) + _dot(rows[1], wo[1])).astype(BF16))
            for z_step, piece in zip(group, sums):
                rpart[z_step, 0] = piece
            for to in (1, 0):
                for z_step in group:
                    for step in Y_STEPS:
                        send_mx(z_step, step, to)
            for z_step in group:
                send_mx(z_step, 0, 0)

    @pl.when(is_owner & (z >= 2))
    def _():
        arrived(kvg.at[1:], KVG_RECV)

    @pl.when(is_other & (z >= 2))
    def _():
        arrived(kvg, KVG_RECV)

    @pl.when(z >= 2)
    def _():
        for b in range(SEQS):
            begin = len_ref[b] + acc_ref[b] - me * POS
            position = lax.broadcasted_iota(jnp.int32, (POS, BLOCK), 0) - begin
            written = (position >= 0) & (position < PROP)
            slot = lax.broadcasted_iota(jnp.int32, (POS, BLOCK), 1)
            for which, buf in enumerate((kbuf, vbuf)):
                offset = which * PROP
                placing = jnp.where(written & (position + offset == slot), 1.0, 0.0)
                placing = placing.astype(BF16)[:, 0 : 2 * PROP]
                for block in range(4):
                    lanes = slice(block * BLOCK, (block + 1) * BLOCK)
                    moved = _dot(placing, kvg[b * 4 + block])
                    buf[b, :, lanes] = jnp.where(written, moved, buf[b, :, lanes].astype(F32)).astype(BF16)
                out_copy(which, b).start()

    @pl.when(z < 2)
    def _():
        for b in range(SEQS):
            for which in range(2):
                out_copy(which, b).start()

    for z_step in Z_OUT:

        @pl.when(is_owner)
        def _(z_step=z_step):
            arrived(rpart.at[z_step, 1:], MX_RECV + z_step)

        @pl.when(is_other)
        def _(z_step=z_step):
            arrived(rpart.at[z_step], MX_RECV + z_step)

        mixed = rpart[z_step, 0].astype(F32)
        for step in range(1, 4):
            mixed = mixed + rpart[z_step, step].astype(F32)
        mixed_ref[z ^ z_step] = mixed.astype(BF16)

    arrived(kbuf, OUT + 3 * core)
    arrived(vbuf, OUT + 3 * core + 1)
    sent = ((pq, Q_SEND), (pkv, KV_SEND), (dv, DV_SEND), (ds, DS_SEND))

    @pl.when(is_owner)
    def _():
        for ref, index in sent + ((qg, QG_SEND + 1), (ng, NG_SEND)):
            arrived(ref.at[1:], index)
        arrived(qg, QG_SEND)
        arrived(kvg.at[0:8], KVG_SEND)
        arrived(rpart.at[0:7], MX_SEND)

    @pl.when(is_owner & (z < 2))
    def _():
        arrived(kvg.at[0:8], KVG_SEND + 1)

    @pl.when(is_owner & (z >= 2))
    def _():
        arrived(kvg.at[0:7], KVG_SEND + 1)

    @pl.when(is_other)
    def _():
        for ref, index in sent:
            arrived(ref, index)
        arrived(wo.at[0], GIVE_SEND)
        arrived(og.at[0], GIVE_SEND + 1)
        arrived(lam.at[0], GIVE_SEND + 2)


def _main(*arrays):
    hbm = pl.BlockSpec(memory_space=pltpu.HBM)
    vmem = pl.BlockSpec(memory_space=pltpu.VMEM)
    dma = pltpu.SemaphoreType.DMA
    return pl.pallas_call(
        _main_kernel,
        out_shape=(
            jax.ShapeDtypeStruct((SEQS, PROP, 256), BF16),
            jax.ShapeDtypeStruct((SEQS, POS, 512), BF16),
            jax.ShapeDtypeStruct((SEQS, POS, 512), BF16),
        ),
        in_specs=[hbm] * 14,
        out_specs=(vmem, pl.BlockSpec(memory_space=pl.ANY), pl.BlockSpec(memory_space=pl.ANY)),
        scratch_shapes=[
            pltpu.VMEM((SEQS, POS, 512), BF16),
            pltpu.VMEM((SEQS, POS, 512), BF16),
            pltpu.VMEM((ROWS, 256), BF16),
            pltpu.VMEM((1, 256), F32),
            pltpu.VMEM((2, 4, BLOCK), F32),
            pltpu.VMEM((SEQS, PROP), jnp.int32),
            pltpu.VMEM((2, 1, TP), F32),
            pltpu.SMEM((SEQS,), jnp.int32),
            pltpu.SMEM((SEQS,), jnp.int32),
            pltpu.VMEM((3, 256, 512), BF16),
            pltpu.VMEM((2, 512, 256), BF16),
            pltpu.VMEM((SEQS, 512, POS), BF16),
            pltpu.VMEM((KV, PAD, BLOCK), BF16),
            pltpu.VMEM((2 * KV, PAD, BLOCK), BF16),
            pltpu.VMEM((KV, 2 * PROP, BLOCK), BF16),
            pltpu.VMEM((2 * KV, 2 * PROP, BLOCK), BF16),
            pltpu.VMEM((PROP, BLOCK), BF16),
            pltpu.VMEM((2 * PROP, BLOCK), BF16),
            pltpu.VMEM((KV, PROP, BLOCK), BF16),
            pltpu.VMEM((KV, 2 * PROP, BLOCK), BF16),
            pltpu.VMEM((KV, 48, BLOCK), BF16),
            pltpu.VMEM((2 * KV, 48, BLOCK), BF16),
            pltpu.VMEM((KV, 2, BLOCK), F32),
            pltpu.VMEM((2 * KV, 2, BLOCK), F32),
            pltpu.VMEM((KV, 2, PROP, BLOCK), BF16),
            pltpu.VMEM((8, 4, PROP, 256), BF16),
            pltpu.VMEM((8, BLOCK), jnp.int32),
            pltpu.VMEM((SEQS, 2, 2 * BLOCK, 2 * BLOCK), BF16),
            pltpu.VMEM((2, 2, POS, 2 * BLOCK), F32),
            pltpu.VMEM((2, 2, 1, 2 * BLOCK), F32),
            dma((SEMAPHORES,)),
            pltpu.SemaphoreType.REGULAR,
            pltpu.SemaphoreType.REGULAR,
            pltpu.VMEM((2, PROP, BLOCK), F32),
            pltpu.VMEM((2, 2, BLOCK), F32),
            pltpu.VMEM((2, HEAD, BLOCK), F32),
        ],
        compiler_params=pltpu.CompilerParams(
            collective_id=0, has_side_effects=True, vmem_limit_bytes=MAIN_VMEM
        ),
        name="attention",
    )(*(pltpu.with_memory_space_constraint(array, pltpu.HBM) for array in arrays))


def _copies_first(which):
    kv = lax.axis_index("kv")
    y = lax.axis_index("tp") // 2
    return (kv < 5) & (kv + y * 4 < 6) if which else (kv + y) < 1


def _copy_kernel(keys_in, values_in, keys_out, values_out, kbuf, vbuf, sem):
    pairs = ((keys_in, kbuf, keys_out), (values_in, vbuf, values_out))
    fetches = [pltpu.make_async_copy(src, buf, sem.at[which]) for which, (src, buf, _) in enumerate(pairs)]
    puts = [pltpu.make_async_copy(buf, dst, sem.at[which]) for which, (_, buf, dst) in enumerate(pairs)]

    @pl.when(_copies_first(1))
    def _():
        fetches[1].start()

        @pl.when(_copies_first(0))
        def _():
            fetches[0].start()

        fetches[1].wait()
        puts[1].start()

        @pl.when(_copies_first(0))
        def _():
            fetches[0].wait()
            puts[0].start()
            puts[0].wait()

        puts[1].wait()


def _copy(*arrays):
    hbm = pl.BlockSpec(memory_space=pltpu.HBM)
    return pl.pallas_call(
        _copy_kernel,
        out_shape=tuple(jax.ShapeDtypeStruct(array.shape, array.dtype) for array in arrays),
        in_specs=[hbm] * 2,
        out_specs=(hbm,) * 2,
        scratch_shapes=[
            pltpu.VMEM((SEQS, POS, 512), BF16),
            pltpu.VMEM((SEQS, POS, 512), BF16),
            pltpu.SemaphoreType.DMA((2,)),
        ],
        compiler_params=pltpu.CompilerParams(vmem_limit_bytes=MAIN_VMEM),
        name="copy_caches",
    )(*(pltpu.with_memory_space_constraint(array, pltpu.HBM) for array in arrays))


def _write_kernel(mixed_ref, keys_ref, values_ref, _keys, _values, mixed_hbm, keys_hbm, values_hbm, sem):
    mixed_copy = pltpu.make_async_copy(mixed_ref, mixed_hbm, sem.at[2])
    mixed_copy.start()

    copies = [
        pltpu.make_async_copy(keys_ref, keys_hbm, sem.at[0]),
        pltpu.make_async_copy(values_ref, values_hbm, sem.at[1]),
    ]

    @pl.when(jnp.logical_not(_copies_first(0)))
    def _():
        copies[0].start()

        @pl.when(jnp.logical_not(_copies_first(1)))
        def _():
            copies[1].start()
            copies[1].wait()

        copies[0].wait()

    mixed_copy.wait()


def _write(*arrays):
    hbm = pl.BlockSpec(memory_space=pltpu.HBM)
    anywhere = pl.BlockSpec(memory_space=pl.ANY)
    return pl.pallas_call(
        _write_kernel,
        out_shape=tuple(jax.ShapeDtypeStruct(array.shape, array.dtype) for array in arrays[:3]),
        in_specs=[anywhere] * 3 + [hbm] * 2,
        out_specs=(hbm,) * 3,
        input_output_aliases={3: 1, 4: 2},
        scratch_shapes=[pltpu.SemaphoreType.DMA((3,))],
        compiler_params=pltpu.CompilerParams(vmem_limit_bytes=WRITE_VMEM),
        name="write",
    )(*arrays)


def _local(
    tokens,
    norm_gain,
    w_query,
    w_key,
    w_value,
    w_output,
    cache_keys,
    cache_values,
    map_lambda,
    out_gain,
    parents,
    lengths,
    accepted,
):
    first_keys, first_values = _copy(cache_keys, cache_values)
    mixed, keys, values = _main(
        tokens,
        norm_gain.reshape(1, 256),
        w_query,
        w_key,
        w_value,
        w_output,
        cache_keys,
        cache_values,
        map_lambda.reshape(1, TP),
        out_gain.reshape(4, BLOCK),
        parents,
        lengths,
        accepted,
        first_keys,
    )
    mixed, new_keys, new_values = _write(mixed, keys, values, first_keys, first_values)
    return mixed.reshape(ROWS, 256), new_keys, new_values


def solution(mesh):
    return jax.shard_map(
        _local,
        mesh=mesh,
        in_specs=(
            P(None, "kv"),
            P("kv"),
            P("kv", "tp"),
            P("kv", "tp"),
            P("kv", "tp"),
            P("tp", "kv"),
            P(None, "kv", "tp"),
            P(None, "kv", "tp"),
            P("tp"),
            P("tp"),
            P(),
            P(),
            P(),
        ),
        out_specs=(P(None, "kv"), P(None, "kv", "tp"), P(None, "kv", "tp")),
        check_vma=False,
    )
```

```python
import functools

import jax
import jax.numpy as jnp
from jax import lax
from jax.experimental import pallas as pl
from jax.experimental.pallas import tpu as pltpu
from jax.sharding import PartitionSpec as P

D = 4096
HEAD = 64
QK = 32
SEQS = 4
PROP = 24
KV = 16
TP = 8
BLOCK = 128
PAD = 32
POS = 512
ROWS = 96
EPS = 1e-05
LOW = -1e30
LOG2E = 1.4426950408889634
WRITE_VMEM = 16 * 1024 * 1024
MAIN_VMEM = 40 * 1024 * 1024
SCALE2 = QK ** (-0.5) * LOG2E
F32 = jnp.float32
BF16 = jnp.bfloat16
NT = (((1,), (1,)), ((), ()))


def _distance(step):
    ring = (0, 1, 2, 1)
    return ring[step >> 2] + ring[step & 3]


LOADS = 13
Q_SEND = 0
KV_SEND = 1
QG_SEND = 2
KVG_SEND = 4
DV_SEND = 6
DS_SEND = 7
NG_SEND = 8
MX_SEND = 9
GIVE_SEND = 10
Q_RECV = 13
KV_RECV = 14
DV_RECV = 15
DS_RECV = 16
QG_RECV = 17
KVG_RECV = 21
NG_RECV = 22
MX_RECV = 26
GIVE_RECV = 30
SEMAPHORES = 33
OUT = 8
Z_ORDER = (0, 1, 2, 3)
Z_OUT = (0, 1, 3, 2)
Z_OUT_GROUPS = ((0,), (1,), (3, 2))
Z_SEND = (0, 1, 2, 3)
Z_GROUPS = ((0,), (1,), (2, 3))
Y_STEPS = (3, 2, 1)
PARTNERS = sorted(range(1, KV), key=lambda step: -_distance(step))


def _dot(a, b):
    return jnp.dot(a, b, preferred_element_type=F32)


def _dot_nt(a, b):
    return lax.dot_general(a, b, NT, preferred_element_type=F32)


def _split_rows(row):
    high = row.astype(BF16).astype(F32)
    middle = (row - high).astype(BF16).astype(F32)
    low = row - high - middle
    index = lax.broadcasted_iota(jnp.int32, (PAD - PROP, BLOCK), 0)
    return jnp.where(index == 0, high, jnp.where(index == 1, middle, jnp.where(index == 2, low, 0.0)))


def _packed(block):
    rest = block[48:]
    moved = jnp.concatenate([pltpu.roll(rest, 96 - 32 * part, 1) for part in range(3)], axis=0)
    return jnp.where(lax.broadcasted_iota(jnp.int32, (48, BLOCK), 1) < 96, block[:48], moved)


def _unpacked(packed):
    lane = lax.broadcasted_iota(jnp.int32, (16, BLOCK), 1)
    parts = [pltpu.roll(packed[16 * part : 16 * part + 16], 32 * part + 32, 1) for part in range(3)]
    rest = jnp.where(lane < 32, parts[0], jnp.where(lane < 64, parts[1], parts[2]))
    return jnp.concatenate([packed, rest], axis=0)


def _expanded(chunk):
    lane = lax.broadcasted_iota(jnp.int32, (PROP, BLOCK), 1)
    parts = []
    for which in range(2):
        for head in range(2):
            low = head * HEAD + which * QK
            inside = (lane >= low) & (lane < low + QK)
            parts.append(jnp.where(inside, chunk, 0.0))
    parts.append(jnp.zeros((BLOCK - 4 * PROP, BLOCK), F32))
    return jnp.concatenate(parts, axis=0).astype(BF16)


def _main_kernel(
    tok_hbm,
    gain_hbm,
    wq_hbm,
    wk_hbm,
    wv_hbm,
    wo_hbm,
    ck_hbm,
    cv_hbm,
    lam_hbm,
    og_hbm,
    par_hbm,
    len_hbm,
    acc_hbm,
    _first_keys,
    mixed_ref,
    keys_out,
    values_out,
    kbuf,
    vbuf,
    tok,
    gain_ref,
    og,
    par_ref,
    lam,
    len_ref,
    acc_ref,
    wqkv,
    wo,
    vt,
    pq,
    rq,
    pkv,
    rkv,
    oq,
    okv,
    qg,
    kvg,
    dv,
    rdv,
    ds,
    rds,
    ng,
    rpart,
    par_pad,
    qe,
    sc,
    sm,
    sems,
    ready,
    go,
    own_factor,
    self_stats,
    self_sum,
):
    me = lax.axis_index("kv")
    tp = lax.axis_index("tp")
    z = me // 4
    x = lax.rem(me, 4)
    core = lax.rem(tp, 2)
    first = tp - core
    is_owner = core == 1
    is_other = core == 0

    def spot(kv_step, y_step, to):
        return {"kv": me ^ kv_step, "tp": (first ^ (2 * y_step)) + to}

    barrier = pltpu.get_barrier_semaphore()

    def greet(kv_step, y_step, to):
        pl.semaphore_signal(
            barrier, inc=1, device_id=spot(kv_step, y_step, to), device_id_type=pl.DeviceIdType.MESH
        )

    @pl.when(is_owner)
    def _():
        for step in PARTNERS:
            greet(step, 0, 0)
            greet(step, 0, 1)
        greet(0, 0, 0)
        for step in Y_STEPS:
            greet(0, step, 1)
            greet(0, step, 0)


    loads = [
        (tok_hbm, tok),
        (gain_hbm, gain_ref),
        (wq_hbm, wqkv.at[0]),
        (wk_hbm, wqkv.at[1]),
        (wv_hbm, wqkv.at[2]),
        (cv_hbm, vbuf),
        (ck_hbm, kbuf),
        (wo_hbm, wo.at[core]),
        (og_hbm, og.at[core]),
        (lam_hbm, lam.at[core]),
        (par_hbm, par_ref),
        (len_hbm, len_ref),
        (acc_hbm, acc_ref),
    ]
    loads = [pltpu.make_async_copy(src, dst, sems.at[index]) for index, (src, dst) in enumerate(loads)]
    for copy in loads:
        copy.start()

    def arrived(ref, index):
        pltpu.make_async_copy(ref, ref, sems.at[index]).wait()

    def remote(src, dst, send, recv, where):
        return pltpu.make_async_remote_copy(
            src_ref=src,
            dst_ref=dst,
            send_sem=sems.at[send],
            recv_sem=sems.at[recv],
            device_id=where,
            device_id_type=pl.DeviceIdType.MESH,
        )

    def send_q(step):
        remote(pq.at[me ^ step], rq.at[core * KV + step], Q_SEND, Q_RECV, spot(step, 0, 1)).start()

    def send_kv(step):
        remote(pkv.at[me ^ step], rkv.at[core * KV + step], KV_SEND, KV_RECV, spot(step, 0, 1)).start()

    def send_d(step):
        remote(ds.at[me ^ step], rds.at[core * KV + step], DS_SEND, DS_RECV, spot(step, 0, 1)).start()
        remote(dv.at[me ^ step], rdv.at[core * KV + step], DV_SEND, DV_RECV, spot(step, 0, 1)).start()

    def send_qg(step, to):
        src = qg.at[me] if to else oq
        remote(src, qg.at[me], QG_SEND + to, QG_RECV + (step >> 2), spot(step, 0, to)).start()

    def send_kvg(step, to):
        src = kvg.at[me] if to else okv
        remote(src, kvg.at[me], KVG_SEND + to, KVG_RECV, spot(step, 0, to)).start()

    def send_ng(step):
        remote(ng.at[me], ng.at[me], NG_SEND, NG_RECV + (step >> 2), spot(step, 0, 1)).start()

    def send_mx(z_step, y_step, to):
        src = rpart.at[z_step, 0]
        dst = rpart.at[z_step, y_step]
        remote(src, dst, MX_SEND, MX_RECV + z_step, spot(0, y_step, to)).start()

    def out_copy(which, b):
        buf, out = ((kbuf, keys_out), (vbuf, values_out))[which]
        return pltpu.make_async_copy(buf.at[b], out.at[b], sems.at[OUT + 3 * core + which])

    loads[0].wait()
    loads[1].wait()
    wide = tok[...].astype(F32)
    gained = (wide * gain_ref[...]).astype(BF16)
    square = jnp.sum(wide * wide, axis=1, keepdims=True)
    eye = lax.broadcasted_iota(jnp.int32, (PROP, BLOCK), 0) == lax.broadcasted_iota(jnp.int32, (PROP, BLOCK), 1)
    loads[2].wait()
    partial_q = _dot(gained, wqkv[0])
    for b in range(SEQS):
        column = square[b * PROP : (b + 1) * PROP]
        row = jnp.sum(jnp.where(eye, column, 0.0), axis=0, keepdims=True)
        tail = _split_rows(row)
        for block in range(4):
            chunk = partial_q[b * PROP : (b + 1) * PROP, block * BLOCK : (block + 1) * BLOCK]
            pq[b * 4 + block] = jnp.concatenate([chunk, tail], axis=0).astype(BF16)

    @pl.when(is_owner)
    def _():
        pl.semaphore_wait(barrier, KV - 1 + 3)

    @pl.when(is_other)
    def _():
        pl.semaphore_wait(barrier, KV + 3)

    for step in PARTNERS:
        send_q(step)

    @pl.when(is_other)
    def _():
        send_q(0)

        def tell(kv_step, y_step):
            pl.semaphore_signal(
                ready, inc=1, device_id=spot(kv_step, y_step, 1), device_id_type=pl.DeviceIdType.MESH
            )

        for step in PARTNERS + [0]:
            tell(step, 0)
        for step in Y_STEPS:
            tell(0, step)

    projected = []
    for which in range(2):
        loads[3 + which].wait()
        projected.append(_dot(gained, wqkv[1 + which]))
    for b in range(SEQS):
        for block in range(4):
            pkv[b * 4 + block] = jnp.concatenate(
                [
                    part_kv[b * PROP : (b + 1) * PROP, block * BLOCK : (block + 1) * BLOCK]
                    for part_kv in projected
                ],
                axis=0,
            ).astype(BF16)
    loads[5].wait()

    def transpose_values(b):
        for block in range(4):
            vt[b, block * BLOCK : (block + 1) * BLOCK, :] = jnp.transpose(
                vbuf[b, :, block * BLOCK : (block + 1) * BLOCK]
            )

    for order in range(SEQS):
        for half in range(2):
            for side in range(2):
                qe[order, half, side * BLOCK : (side + 1) * BLOCK, (1 - side) * BLOCK : (2 - side) * BLOCK] = (
                    jnp.zeros((BLOCK, BLOCK), BF16)
                )
    for b in range(SEQS):
        transpose_values(b)
    for index in (6, 7, 8, 9, 10, 11, 12):
        loads[index].wait()

    zero_tail = jnp.zeros((PAD - PROP, BLOCK), F32)
    lane = lax.broadcasted_iota(jnp.int32, (HEAD, BLOCK), 1)
    second_head = ((lane >= PROP) & (lane < 2 * PROP)) | (lane >= 3 * PROP)

    @pl.when(is_owner)
    def _():
        arrived(rq.at[0:31], Q_RECV)
        for group in range(2):
            total = (pq[me] if group else rq[0]).astype(F32)
            for step in range(1, KV):
                total = total + rq[group * KV + step].astype(F32)
            square_row = jnp.sum(total[PROP:PAD], axis=0, keepdims=True)
            square_column = jnp.sum(jnp.where(eye, square_row, 0.0), axis=1, keepdims=True)
            factor = lax.rsqrt(square_column / D + EPS)
            own_factor[group] = jnp.broadcast_to(factor, (PROP, BLOCK))
            own_q = (total[0:PROP] * factor).astype(BF16)
            if group:
                qg[me] = own_q
            else:
                oq[...] = own_q
        pl.semaphore_wait(ready, KV + 3)
        for z_step in Z_SEND:
            for step in PARTNERS + [0]:
                if step >> 2 == z_step:
                    send_qg(step, 0)
                    if step:
                        send_qg(step, 1)
        pl.semaphore_signal(go, inc=1, device_id=spot(0, 0, 0), device_id_type=pl.DeviceIdType.MESH)
        for step in PARTNERS:
            send_kv(step)

    @pl.when(is_other)
    def _():
        pl.semaphore_wait(go, 1)
        for step in PARTNERS + [0]:
            send_kv(step)
        remote(wo.at[0], wo.at[0], GIVE_SEND, GIVE_RECV, spot(0, 0, 1)).start()
        remote(og.at[0], og.at[0], GIVE_SEND + 1, GIVE_RECV + 1, spot(0, 0, 1)).start()
        remote(lam.at[0], lam.at[0], GIVE_SEND + 2, GIVE_RECV + 2, spot(0, 0, 1)).start()


    def gathered(z_step):
        if z_step:
            arrived(qg.at[pl.ds((z ^ z_step) * 4, 4)], QG_RECV + z_step)
            return

        @pl.when(is_owner)
        def _():
            arrived(qg.at[0:3], QG_RECV)

        @pl.when(is_other)
        def _():
            arrived(qg.at[0:4], QG_RECV)

    def expand(order):
        b = z ^ Z_ORDER[order]
        for half in range(2):
            for side in range(2):
                chunk = qg[b * 4 + half * 2 + side].astype(F32)
                lanes = slice(side * BLOCK, (side + 1) * BLOCK)
                qe[order, half, lanes, lanes] = _expanded(chunk)

    def score(order):
        b = z ^ Z_ORDER[order]
        begin = len_ref[b] + acc_ref[b] - me * POS
        visible = lax.broadcasted_iota(jnp.int32, (POS, BLOCK), 0) < begin
        visible = jnp.concatenate([visible, visible], axis=1)
        for half in range(2):
            keys = kbuf[b, :, half * 2 * BLOCK : (half + 1) * 2 * BLOCK]
            scores = jnp.where(visible, _dot_nt(keys, qe[order, half]) * SCALE2, LOW)
            sc[order % 2, half] = scores
            sm[order % 2, half] = jnp.max(scores, axis=0, keepdims=True)

    def weigh(order):
        b = z ^ Z_ORDER[order]
        for half in range(2):
            largest = sm[order % 2, half]
            weight = jnp.exp2(sc[order % 2, half] - largest)
            weight_sum = jnp.sum(weight, axis=0, keepdims=True)
            weight = weight.astype(BF16)
            for side in range(2):
                block = half * 2 + side
                lanes = slice(side * BLOCK, (side + 1) * BLOCK)
                out = _dot(vt[b, block * BLOCK : (block + 1) * BLOCK, :], weight[:, lanes])
                owner = b * 4 + block
                dv[owner] = _packed(jnp.where(second_head, out[HEAD:], out[:HEAD])).astype(BF16)
                ds[owner] = jnp.concatenate([largest[:, lanes], weight_sum[:, lanes]], axis=0)

    def send(order):
        for x_step in (2, 1, 3, 0):
            step = Z_ORDER[order] << 2 | x_step
            if step:
                send_d(step)
        if Z_ORDER[order] == 0:

            @pl.when(is_other)
            def _():
                send_d(0)

    for group in Z_GROUPS:
        for order in group:
            gathered(Z_ORDER[order])
        for order in group:
            expand(order)
        score(group[0])
        for order in group:
            if order + 1 in group:
                score(order + 1)
            weigh(order)
            send(order)

    @pl.when(is_owner)
    def _():
        arrived(rkv.at[0:31], KV_RECV)
        for group in range(2):
            summed = (pkv[me] if group else rkv[0]).astype(F32)
            for step in range(1, KV):
                summed = summed + rkv[group * KV + step].astype(F32)
            rows = [summed[0:PROP] * own_factor[group], summed[PROP:] * own_factor[group]]
            rows = jnp.concatenate(rows, axis=0).astype(BF16)
            if group:
                kvg[me] = rows
            else:
                okv[...] = rows
        par_pad[...] = jnp.full((8, BLOCK), -1, jnp.int32)
        par_pad[0:SEQS, 0:PROP] = par_ref[...]
        parent_row = par_pad[pl.ds(z, 1), :]
        row_index = lax.broadcasted_iota(jnp.int32, (BLOCK, BLOCK), 0)
        lane_index = lax.broadcasted_iota(jnp.int32, (BLOCK, BLOCK), 1)
        reach = ((parent_row == row_index) & (lane_index < PROP)) | (row_index == lane_index)
        reach = jnp.where(reach, 1.0, 0.0).astype(BF16)
        for _ in range(5):
            reach = jnp.minimum(_dot(reach, reach), 1.0).astype(BF16)
        spread = (lax.rem(lane_index, PROP) == row_index) & (lane_index < 4 * PROP) & (row_index < PROP)
        lineage = _dot(reach, jnp.where(spread, 1.0, 0.0).astype(BF16))[0:PAD]
        linked = (lineage > 0.5) & (lax.broadcasted_iota(jnp.int32, (PAD, BLOCK), 0) < PROP)
        for group in range(2):
            own_expanded = _expanded((qg[me] if group else oq[...]).astype(F32))
            own_kv = (kvg[me] if group else okv[...]).astype(F32)
            own_k = jnp.concatenate([own_kv[0:PROP], zero_tail], axis=0).astype(BF16)
            own_v = jnp.concatenate([own_kv[PROP:], zero_tail], axis=0)
            self_scores = _dot_nt(own_k, own_expanded) * SCALE2
            self_scores = jnp.where(linked, self_scores, LOW)
            largest = jnp.max(self_scores, axis=0, keepdims=True)
            self_weight = jnp.where(linked, jnp.exp2(self_scores - largest), 0.0)
            self_stats[group, 0:1] = largest
            self_stats[group, 1:2] = jnp.sum(self_weight, axis=0, keepdims=True)
            self_out = _dot(jnp.transpose(own_v).astype(BF16), self_weight.astype(BF16))
            self_sum[group] = jnp.where(second_head, self_out[HEAD:], self_out[:HEAD])
        lane_row = lax.broadcasted_iota(jnp.int32, (1, BLOCK), 1)
        arrived(og.at[0], GIVE_RECV + 1)
        arrived(lam.at[0], GIVE_RECV + 2)
        arrived(wo.at[0], GIVE_RECV)
        lam_rows = []
        for group in range(2):
            index = lax.broadcasted_iota(jnp.int32, (1, TP), 1)
            pair = [
                jnp.sum(jnp.where(index == x * 2 + head, lam[group], 0.0), axis=1, keepdims=True)
                for head in range(2)
            ]
            lam_rows.append(jnp.where(lane_row < PROP, pair[0], pair[1]))

        arrived(rds.at[0:31], DS_RECV)
        self_factor = []
        factors = []
        used = lax.broadcasted_iota(jnp.int32, (KV, BLOCK), 1) < 96
        for group in range(2):
            slots = [ds.at[me] if group else rds.at[0]] + [rds.at[group * KV + step] for step in range(1, KV)]
            maxima = jnp.concatenate([slot[0:1] for slot in slots], axis=0)
            totals = jnp.concatenate([slot[1:2] for slot in slots], axis=0)
            top = jnp.maximum(jnp.max(maxima, axis=0, keepdims=True), self_stats[group, 0:1])
            own = jnp.exp2(self_stats[group, 0:1] - top)
            factor = jnp.exp2(maxima - top)
            denominator = self_stats[group, 1:2] * own + jnp.sum(totals * factor, axis=0, keepdims=True)
            inverse = 1.0 / denominator
            factor = factor * inverse
            self_factor.append(own * inverse)
            factors.append(
                [jnp.where(used, factor, pltpu.roll(factor, 96 - 32 * third, 1)) for third in range(3)]
            )
        arrived(rdv.at[0:31], DV_RECV)
        for group in range(2):
            slots = [dv.at[me] if group else rdv.at[0]] + [rdv.at[group * KV + step] for step in range(1, KV)]
            merged = []
            for third in range(3):
                rows = slice(16 * third, 16 * third + 16)
                sums = [
                    slot[rows].astype(F32) * factors[group][third][step : step + 1]
                    for step, slot in enumerate(slots)
                ]
                while len(sums) > 1:
                    sums = [a + b for a, b in zip(sums[::2], sums[1::2])]
                merged.append(sums[0])
            attended = _unpacked(jnp.concatenate(merged, axis=0)) + self_sum[group] * self_factor[group]
            difference = attended - lam_rows[group] * pltpu.roll(attended, BLOCK - 2 * PROP, 1)
            power = jnp.mean(difference * difference, axis=0, keepdims=True)
            normed = difference * lax.rsqrt(power + EPS)
            stacked = jnp.concatenate([normed, pltpu.roll(normed, BLOCK - PROP, 1)], axis=0)
            turned = jnp.transpose(stacked)[0:PROP]
            turned = turned * og[group, pl.ds(x, 1), :]
            ng[me, group] = turned.astype(BF16)
        for step in PARTNERS:
            send_ng(step)
        for z_step in (2, 1, 3, 0):

            @pl.when((z ^ z_step) >= 2)
            def _(z_step=z_step):
                for step in PARTNERS + [0]:
                    if step >> 2 == z_step:
                        send_kvg(step, 0)
                        if step:
                            send_kvg(step, 1)


        for group in Z_OUT_GROUPS:
            for z_step in group:
                arrived(ng.at[pl.ds((z ^ z_step) * 4, 4 if z_step else 3)], NG_RECV + z_step)
            sums = []
            for z_step in group:
                rows = [
                    jnp.concatenate([ng[(z ^ z_step) * 4 + block, half] for block in range(4)], axis=1)
                    for half in range(2)
                ]
                sums.append((_dot(rows[0], wo[0]) + _dot(rows[1], wo[1])).astype(BF16))
            for z_step, piece in zip(group, sums):
                rpart[z_step, 0] = piece
            for to in (1, 0):
                for z_step in group:
                    for step in Y_STEPS:
                        send_mx(z_step, step, to)
            for z_step in group:
                send_mx(z_step, 0, 0)

    @pl.when(is_owner & (z >= 2))
    def _():
        arrived(kvg.at[1:], KVG_RECV)

    @pl.when(is_other & (z >= 2))
    def _():
        arrived(kvg, KVG_RECV)

    @pl.when(z >= 2)
    def _():
        for b in range(SEQS):
            begin = len_ref[b] + acc_ref[b] - me * POS
            position = lax.broadcasted_iota(jnp.int32, (POS, BLOCK), 0) - begin
            written = (position >= 0) & (position < PROP)
            slot = lax.broadcasted_iota(jnp.int32, (POS, BLOCK), 1)
            for which, buf in enumerate((kbuf, vbuf)):
                offset = which * PROP
                placing = jnp.where(written & (position + offset == slot), 1.0, 0.0)
                placing = placing.astype(BF16)[:, 0 : 2 * PROP]
                for block in range(4):
                    lanes = slice(block * BLOCK, (block + 1) * BLOCK)
                    moved = _dot(placing, kvg[b * 4 + block])
                    buf[b, :, lanes] = jnp.where(written, moved, buf[b, :, lanes].astype(F32)).astype(BF16)
                out_copy(which, b).start()

    @pl.when(z < 2)
    def _():
        for b in range(SEQS):
            for which in range(2):
                out_copy(which, b).start()

    for z_step in Z_OUT:

        @pl.when(is_owner)
        def _(z_step=z_step):
            arrived(rpart.at[z_step, 1:], MX_RECV + z_step)

        @pl.when(is_other)
        def _(z_step=z_step):
            arrived(rpart.at[z_step], MX_RECV + z_step)

        mixed = rpart[z_step, 0].astype(F32)
        for step in range(1, 4):
            mixed = mixed + rpart[z_step, step].astype(F32)
        mixed_ref[z ^ z_step] = mixed.astype(BF16)

    arrived(kbuf, OUT + 3 * core)
    arrived(vbuf, OUT + 3 * core + 1)
    sent = ((pq, Q_SEND), (pkv, KV_SEND), (dv, DV_SEND), (ds, DS_SEND))

    @pl.when(is_owner)
    def _():
        for ref, index in sent + ((qg, QG_SEND + 1), (ng, NG_SEND)):
            arrived(ref.at[1:], index)
        arrived(qg, QG_SEND)
        arrived(kvg.at[0:8], KVG_SEND)
        arrived(rpart.at[0:7], MX_SEND)

    @pl.when(is_owner & (z < 2))
    def _():
        arrived(kvg.at[0:8], KVG_SEND + 1)

    @pl.when(is_owner & (z >= 2))
    def _():
        arrived(kvg.at[0:7], KVG_SEND + 1)

    @pl.when(is_other)
    def _():
        for ref, index in sent:
            arrived(ref, index)
        arrived(wo.at[0], GIVE_SEND)
        arrived(og.at[0], GIVE_SEND + 1)
        arrived(lam.at[0], GIVE_SEND + 2)


def _main(*arrays):
    hbm = pl.BlockSpec(memory_space=pltpu.HBM)
    vmem = pl.BlockSpec(memory_space=pltpu.VMEM)
    dma = pltpu.SemaphoreType.DMA
    return pl.pallas_call(
        _main_kernel,
        out_shape=(
            jax.ShapeDtypeStruct((SEQS, PROP, 256), BF16),
            jax.ShapeDtypeStruct((SEQS, POS, 512), BF16),
            jax.ShapeDtypeStruct((SEQS, POS, 512), BF16),
        ),
        in_specs=[hbm] * 14,
        out_specs=(vmem, pl.BlockSpec(memory_space=pl.ANY), pl.BlockSpec(memory_space=pl.ANY)),
        scratch_shapes=[
            pltpu.VMEM((SEQS, POS, 512), BF16),
            pltpu.VMEM((SEQS, POS, 512), BF16),
            pltpu.VMEM((ROWS, 256), BF16),
            pltpu.VMEM((1, 256), F32),
            pltpu.VMEM((2, 4, BLOCK), F32),
            pltpu.VMEM((SEQS, PROP), jnp.int32),
            pltpu.VMEM((2, 1, TP), F32),
            pltpu.SMEM((SEQS,), jnp.int32),
            pltpu.SMEM((SEQS,), jnp.int32),
            pltpu.VMEM((3, 256, 512), BF16),
            pltpu.VMEM((2, 512, 256), BF16),
            pltpu.VMEM((SEQS, 512, POS), BF16),
            pltpu.VMEM((KV, PAD, BLOCK), BF16),
            pltpu.VMEM((2 * KV, PAD, BLOCK), BF16),
            pltpu.VMEM((KV, 2 * PROP, BLOCK), BF16),
            pltpu.VMEM((2 * KV, 2 * PROP, BLOCK), BF16),
            pltpu.VMEM((PROP, BLOCK), BF16),
            pltpu.VMEM((2 * PROP, BLOCK), BF16),
            pltpu.VMEM((KV, PROP, BLOCK), BF16),
            pltpu.VMEM((KV, 2 * PROP, BLOCK), BF16),
            pltpu.VMEM((KV, 48, BLOCK), BF16),
            pltpu.VMEM((2 * KV, 48, BLOCK), BF16),
            pltpu.VMEM((KV, 2, BLOCK), F32),
            pltpu.VMEM((2 * KV, 2, BLOCK), F32),
            pltpu.VMEM((KV, 2, PROP, BLOCK), BF16),
            pltpu.VMEM((8, 4, PROP, 256), BF16),
            pltpu.VMEM((8, BLOCK), jnp.int32),
            pltpu.VMEM((SEQS, 2, 2 * BLOCK, 2 * BLOCK), BF16),
            pltpu.VMEM((2, 2, POS, 2 * BLOCK), F32),
            pltpu.VMEM((2, 2, 1, 2 * BLOCK), F32),
            dma((SEMAPHORES,)),
            pltpu.SemaphoreType.REGULAR,
            pltpu.SemaphoreType.REGULAR,
            pltpu.VMEM((2, PROP, BLOCK), F32),
            pltpu.VMEM((2, 2, BLOCK), F32),
            pltpu.VMEM((2, HEAD, BLOCK), F32),
        ],
        compiler_params=pltpu.CompilerParams(
            collective_id=0, has_side_effects=True, vmem_limit_bytes=MAIN_VMEM
        ),
        name="attention",
    )(*(pltpu.with_memory_space_constraint(array, pltpu.HBM) for array in arrays))


def _copies_first(which):
    kv = lax.axis_index("kv")
    y = lax.axis_index("tp") // 2
    return (kv < 5) & (kv + y * 4 < 6) if which else (kv + y) < 1


def _copy_kernel(keys_in, values_in, keys_out, values_out, kbuf, vbuf, sem):
    pairs = ((keys_in, kbuf, keys_out), (values_in, vbuf, values_out))
    fetches = [pltpu.make_async_copy(src, buf, sem.at[which]) for which, (src, buf, _) in enumerate(pairs)]
    puts = [pltpu.make_async_copy(buf, dst, sem.at[which]) for which, (_, buf, dst) in enumerate(pairs)]

    @pl.when(_copies_first(1))
    def _():
        fetches[1].start()

        @pl.when(_copies_first(0))
        def _():
            fetches[0].start()

        fetches[1].wait()
        puts[1].start()

        @pl.when(_copies_first(0))
        def _():
            fetches[0].wait()
            puts[0].start()
            puts[0].wait()

        puts[1].wait()


def _copy(*arrays):
    hbm = pl.BlockSpec(memory_space=pltpu.HBM)
    return pl.pallas_call(
        _copy_kernel,
        out_shape=tuple(jax.ShapeDtypeStruct(array.shape, array.dtype) for array in arrays),
        in_specs=[hbm] * 2,
        out_specs=(hbm,) * 2,
        scratch_shapes=[
            pltpu.VMEM((SEQS, POS, 512), BF16),
            pltpu.VMEM((SEQS, POS, 512), BF16),
            pltpu.SemaphoreType.DMA((2,)),
        ],
        compiler_params=pltpu.CompilerParams(vmem_limit_bytes=MAIN_VMEM),
        name="copy_caches",
    )(*(pltpu.with_memory_space_constraint(array, pltpu.HBM) for array in arrays))


def _write_kernel(mixed_ref, keys_ref, values_ref, _keys, _values, mixed_hbm, keys_hbm, values_hbm, sem):
    mixed_copy = pltpu.make_async_copy(mixed_ref, mixed_hbm, sem.at[2])
    mixed_copy.start()

    copies = [
        pltpu.make_async_copy(keys_ref, keys_hbm, sem.at[0]),
        pltpu.make_async_copy(values_ref, values_hbm, sem.at[1]),
    ]

    @pl.when(jnp.logical_not(_copies_first(0)))
    def _():
        copies[0].start()

        @pl.when(jnp.logical_not(_copies_first(1)))
        def _():
            copies[1].start()
            copies[1].wait()

        copies[0].wait()

    mixed_copy.wait()


def _write(*arrays):
    hbm = pl.BlockSpec(memory_space=pltpu.HBM)
    anywhere = pl.BlockSpec(memory_space=pl.ANY)
    return pl.pallas_call(
        _write_kernel,
        out_shape=tuple(jax.ShapeDtypeStruct(array.shape, array.dtype) for array in arrays[:3]),
        in_specs=[anywhere] * 3 + [hbm] * 2,
        out_specs=(hbm,) * 3,
        input_output_aliases={3: 1, 4: 2},
        scratch_shapes=[pltpu.SemaphoreType.DMA((3,))],
        compiler_params=pltpu.CompilerParams(vmem_limit_bytes=WRITE_VMEM),
        name="write",
    )(*arrays)


def _local(
    tokens,
    norm_gain,
    w_query,
    w_key,
    w_value,
    w_output,
    cache_keys,
    cache_values,
    map_lambda,
    out_gain,
    parents,
    lengths,
    accepted,
):
    first_keys, first_values = _copy(cache_keys, cache_values)
    mixed, keys, values = _main(
        tokens,
        norm_gain.reshape(1, 256),
        w_query,
        w_key,
        w_value,
        w_output,
        cache_keys,
        cache_values,
        map_lambda.reshape(1, TP),
        out_gain.reshape(4, BLOCK),
        parents,
        lengths,
        accepted,
        first_keys,
    )
    mixed, new_keys, new_values = _write(mixed, keys, values, first_keys, first_values)
    return mixed.reshape(ROWS, 256), new_keys, new_values


def solution(mesh):
    return jax.shard_map(
        _local,
        mesh=mesh,
        in_specs=(
            P(None, "kv"),
            P("kv"),
            P("kv", "tp"),
            P("kv", "tp"),
            P("kv", "tp"),
            P("tp", "kv"),
            P(None, "kv", "tp"),
            P(None, "kv", "tp"),
            P("tp"),
            P("tp"),
            P(),
            P(),
            P(),
        ),
        out_specs=(P(None, "kv"), P(None, "kv", "tp"), P(None, "kv", "tp")),
        check_vma=False,
    )
```

```python
import functools

import jax
import jax.numpy as jnp
from jax import lax
from jax.experimental import pallas as pl
from jax.experimental.pallas import tpu as pltpu
from jax.sharding import PartitionSpec as P

D = 4096
HEAD = 64
QK = 32
SEQS = 4
PROP = 24
KV = 16
TP = 8
BLOCK = 128
PAD = 32
POS = 512
ROWS = 96
EPS = 1e-05
LOW = -1e30
LOG2E = 1.4426950408889634
WRITE_VMEM = 16 * 1024 * 1024
MAIN_VMEM = 40 * 1024 * 1024
SCALE2 = QK ** (-0.5) * LOG2E
F32 = jnp.float32
BF16 = jnp.bfloat16
NT = (((1,), (1,)), ((), ()))


def _distance(step):
    ring = (0, 1, 2, 1)
    return ring[step >> 2] + ring[step & 3]


LOADS = 13
Q_SEND = 0
KV_SEND = 1
QG_SEND = 2
KVG_SEND = 4
DV_SEND = 6
DS_SEND = 7
NG_SEND = 8
MX_SEND = 9
GIVE_SEND = 10
Q_RECV = 13
KV_RECV = 14
DV_RECV = 15
DS_RECV = 16
QG_RECV = 17
KVG_RECV = 21
NG_RECV = QG_RECV
MX_RECV = 22
GIVE_RECV = 26
SEMAPHORES = 29
OUT = 8
Z_ORDER = (0, 1, 2, 3)
Z_OUT = (0, 1, 3, 2)
Z_OUT_GROUPS = ((0,), (1,), (3, 2))
Z_SEND = (0, 1, 2, 3)
Z_GROUPS = ((0,), (1,), (2, 3))
Y_STEPS = (3, 2, 1)
PARTNERS = sorted(range(1, KV), key=lambda step: -_distance(step))


def _dot(a, b):
    return jnp.dot(a, b, preferred_element_type=F32)


def _dot_nt(a, b):
    return lax.dot_general(a, b, NT, preferred_element_type=F32)


def _split_rows(row):
    high = row.astype(BF16).astype(F32)
    middle = (row - high).astype(BF16).astype(F32)
    low = row - high - middle
    index = lax.broadcasted_iota(jnp.int32, (PAD - PROP, BLOCK), 0)
    return jnp.where(index == 0, high, jnp.where(index == 1, middle, jnp.where(index == 2, low, 0.0)))


def _packed(block):
    rest = block[48:]
    moved = jnp.concatenate([pltpu.roll(rest, 96 - 32 * part, 1) for part in range(3)], axis=0)
    return jnp.where(lax.broadcasted_iota(jnp.int32, (48, BLOCK), 1) < 96, block[:48], moved)


def _unpacked(packed):
    lane = lax.broadcasted_iota(jnp.int32, (16, BLOCK), 1)
    parts = [pltpu.roll(packed[16 * part : 16 * part + 16], 32 * part + 32, 1) for part in range(3)]
    rest = jnp.where(lane < 32, parts[0], jnp.where(lane < 64, parts[1], parts[2]))
    return jnp.concatenate([packed, rest], axis=0)


def _expanded(chunk):
    lane = lax.broadcasted_iota(jnp.int32, (PROP, BLOCK), 1)
    parts = []
    for which in range(2):
        for head in range(2):
            low = head * HEAD + which * QK
            inside = (lane >= low) & (lane < low + QK)
            parts.append(jnp.where(inside, chunk, 0.0))
    parts.append(jnp.zeros((BLOCK - 4 * PROP, BLOCK), F32))
    return jnp.concatenate(parts, axis=0).astype(BF16)


def _main_kernel(
    tok_hbm,
    gain_hbm,
    wq_hbm,
    wk_hbm,
    wv_hbm,
    wo_hbm,
    ck_hbm,
    cv_hbm,
    lam_hbm,
    og_hbm,
    par_hbm,
    len_hbm,
    acc_hbm,
    _first_keys,
    mixed_ref,
    keys_out,
    values_out,
    kbuf,
    vbuf,
    tok,
    gain_ref,
    og,
    par_ref,
    lam,
    len_ref,
    acc_ref,
    wqkv,
    wo,
    vt,
    pq,
    rq,
    pkv,
    rkv,
    oq,
    okv,
    qg,
    kvg,
    dv,
    rdv,
    ds,
    rds,
    ng,
    rpart,
    par_pad,
    qe,
    sc,
    sm,
    sems,
    ready,
    go,
    own_factor,
    self_stats,
    self_sum,
):
    me = lax.axis_index("kv")
    tp = lax.axis_index("tp")
    z = me // 4
    x = lax.rem(me, 4)
    core = lax.rem(tp, 2)
    first = tp - core
    is_owner = core == 1
    is_other = core == 0

    def spot(kv_step, y_step, to):
        return {"kv": me ^ kv_step, "tp": (first ^ (2 * y_step)) + to}

    barrier = pltpu.get_barrier_semaphore()

    def greet(kv_step, y_step, to):
        pl.semaphore_signal(
            barrier, inc=1, device_id=spot(kv_step, y_step, to), device_id_type=pl.DeviceIdType.MESH
        )

    @pl.when(is_owner)
    def _():
        for step in PARTNERS:
            greet(step, 0, 0)
            greet(step, 0, 1)
        greet(0, 0, 0)
        for step in Y_STEPS:
            greet(0, step, 1)
            greet(0, step, 0)


    loads = [
        (tok_hbm, tok),
        (gain_hbm, gain_ref),
        (wq_hbm, wqkv.at[0]),
        (wk_hbm, wqkv.at[1]),
        (wv_hbm, wqkv.at[2]),
        (cv_hbm, vbuf),
        (ck_hbm, kbuf),
        (wo_hbm, wo.at[core]),
        (og_hbm, og.at[core]),
        (lam_hbm, lam.at[core]),
        (par_hbm, par_ref),
        (len_hbm, len_ref),
        (acc_hbm, acc_ref),
    ]
    loads = [pltpu.make_async_copy(src, dst, sems.at[index]) for index, (src, dst) in enumerate(loads)]
    for copy in loads:
        copy.start()

    def arrived(ref, index):
        pltpu.make_async_copy(ref, ref, sems.at[index]).wait()

    def remote(src, dst, send, recv, where):
        return pltpu.make_async_remote_copy(
            src_ref=src,
            dst_ref=dst,
            send_sem=sems.at[send],
            recv_sem=sems.at[recv],
            device_id=where,
            device_id_type=pl.DeviceIdType.MESH,
        )

    def send_q(step):
        remote(pq.at[me ^ step], rq.at[core * KV + step], Q_SEND, Q_RECV, spot(step, 0, 1)).start()

    def send_kv(step):
        remote(pkv.at[me ^ step], rkv.at[core * KV + step], KV_SEND, KV_RECV, spot(step, 0, 1)).start()

    def send_d(step):
        remote(ds.at[me ^ step], rds.at[core * KV + step], DS_SEND, DS_RECV, spot(step, 0, 1)).start()
        remote(dv.at[me ^ step], rdv.at[core * KV + step], DV_SEND, DV_RECV, spot(step, 0, 1)).start()

    def send_qg(step, to):
        src = qg.at[me] if to else oq
        remote(src, qg.at[me], QG_SEND + to, QG_RECV + (step >> 2), spot(step, 0, to)).start()

    def send_kvg(step, to):
        src = kvg.at[me] if to else okv
        remote(src, kvg.at[me], KVG_SEND + to, KVG_RECV, spot(step, 0, to)).start()

    def send_ng(step):
        remote(ng.at[me], ng.at[me], NG_SEND, NG_RECV + (step >> 2), spot(step, 0, 1)).start()

    def send_mx(z_step, y_step, to):
        src = rpart.at[z_step, 0]
        dst = rpart.at[z_step, y_step]
        remote(src, dst, MX_SEND, MX_RECV + z_step, spot(0, y_step, to)).start()

    def out_copy(which, b):
        buf, out = ((kbuf, keys_out), (vbuf, values_out))[which]
        return pltpu.make_async_copy(buf.at[b], out.at[b], sems.at[OUT + 3 * core + which])

    loads[0].wait()
    loads[1].wait()
    wide = tok[...].astype(F32)
    gained = (wide * gain_ref[...]).astype(BF16)
    square = jnp.sum(wide * wide, axis=1, keepdims=True)
    eye = lax.broadcasted_iota(jnp.int32, (PROP, BLOCK), 0) == lax.broadcasted_iota(jnp.int32, (PROP, BLOCK), 1)
    loads[2].wait()
    partial_q = _dot(gained, wqkv[0])
    for b in range(SEQS):
        column = square[b * PROP : (b + 1) * PROP]
        row = jnp.sum(jnp.where(eye, column, 0.0), axis=0, keepdims=True)
        tail = _split_rows(row)
        for block in range(4):
            chunk = partial_q[b * PROP : (b + 1) * PROP, block * BLOCK : (block + 1) * BLOCK]
            pq[b * 4 + block] = jnp.concatenate([chunk, tail], axis=0).astype(BF16)

    @pl.when(is_owner)
    def _():
        pl.semaphore_wait(barrier, KV - 1 + 3)

    @pl.when(is_other)
    def _():
        pl.semaphore_wait(barrier, KV + 3)

    for step in PARTNERS:
        send_q(step)

    @pl.when(is_other)
    def _():
        send_q(0)

        def tell(kv_step, y_step):
            pl.semaphore_signal(
                ready, inc=1, device_id=spot(kv_step, y_step, 1), device_id_type=pl.DeviceIdType.MESH
            )

        for step in PARTNERS + [0]:
            tell(step, 0)
        for step in Y_STEPS:
            tell(0, step)

    projected = []
    for which in range(2):
        loads[3 + which].wait()
        projected.append(_dot(gained, wqkv[1 + which]))
    for b in range(SEQS):
        for block in range(4):
            pkv[b * 4 + block] = jnp.concatenate(
                [
                    part_kv[b * PROP : (b + 1) * PROP, block * BLOCK : (block + 1) * BLOCK]
                    for part_kv in projected
                ],
                axis=0,
            ).astype(BF16)
    loads[5].wait()

    def transpose_values(b):
        for block in range(4):
            vt[b, block * BLOCK : (block + 1) * BLOCK, :] = jnp.transpose(
                vbuf[b, :, block * BLOCK : (block + 1) * BLOCK]
            )

    for order in range(SEQS):
        for half in range(2):
            for side in range(2):
                qe[order, half, side * BLOCK : (side + 1) * BLOCK, (1 - side) * BLOCK : (2 - side) * BLOCK] = (
                    jnp.zeros((BLOCK, BLOCK), BF16)
                )
    for b in range(SEQS):
        transpose_values(b)
    for index in (6, 7, 8, 9, 10, 11, 12):
        loads[index].wait()

    zero_tail = jnp.zeros((PAD - PROP, BLOCK), F32)
    lane = lax.broadcasted_iota(jnp.int32, (HEAD, BLOCK), 1)
    second_head = ((lane >= PROP) & (lane < 2 * PROP)) | (lane >= 3 * PROP)

    @pl.when(is_owner)
    def _():
        arrived(rq.at[0:31], Q_RECV)
        for group in range(2):
            total = (pq[me] if group else rq[0]).astype(F32)
            for step in range(1, KV):
                total = total + rq[group * KV + step].astype(F32)
            square_row = jnp.sum(total[PROP:PAD], axis=0, keepdims=True)
            square_column = jnp.sum(jnp.where(eye, square_row, 0.0), axis=1, keepdims=True)
            factor = lax.rsqrt(square_column / D + EPS)
            own_factor[group] = jnp.broadcast_to(factor, (PROP, BLOCK))
            own_q = (total[0:PROP] * factor).astype(BF16)
            if group:
                qg[me] = own_q
            else:
                oq[...] = own_q
        pl.semaphore_wait(ready, KV + 3)
        for z_step in Z_SEND:
            for step in PARTNERS + [0]:
                if step >> 2 == z_step:
                    send_qg(step, 0)
                    if step:
                        send_qg(step, 1)
        pl.semaphore_signal(go, inc=1, device_id=spot(0, 0, 0), device_id_type=pl.DeviceIdType.MESH)
        for step in PARTNERS:
            send_kv(step)

    @pl.when(is_other)
    def _():
        pl.semaphore_wait(go, 1)
        for step in PARTNERS + [0]:
            send_kv(step)
        remote(wo.at[0], wo.at[0], GIVE_SEND, GIVE_RECV, spot(0, 0, 1)).start()
        remote(og.at[0], og.at[0], GIVE_SEND + 1, GIVE_RECV + 1, spot(0, 0, 1)).start()
        remote(lam.at[0], lam.at[0], GIVE_SEND + 2, GIVE_RECV + 2, spot(0, 0, 1)).start()


    def gathered(z_step):
        if z_step:
            arrived(qg.at[pl.ds((z ^ z_step) * 4, 4)], QG_RECV + z_step)
            return

        @pl.when(is_owner)
        def _():
            arrived(qg.at[0:3], QG_RECV)

        @pl.when(is_other)
        def _():
            arrived(qg.at[0:4], QG_RECV)

    def expand(order):
        b = z ^ Z_ORDER[order]
        for half in range(2):
            for side in range(2):
                chunk = qg[b * 4 + half * 2 + side].astype(F32)
                lanes = slice(side * BLOCK, (side + 1) * BLOCK)
                qe[order, half, lanes, lanes] = _expanded(chunk)

    def score(order):
        b = z ^ Z_ORDER[order]
        begin = len_ref[b] + acc_ref[b] - me * POS
        visible = lax.broadcasted_iota(jnp.int32, (POS, BLOCK), 0) < begin
        visible = jnp.concatenate([visible, visible], axis=1)
        for half in range(2):
            keys = kbuf[b, :, half * 2 * BLOCK : (half + 1) * 2 * BLOCK]
            scores = jnp.where(visible, _dot_nt(keys, qe[order, half]) * SCALE2, LOW)
            sc[order % 2, half] = scores
            sm[order % 2, half] = jnp.max(scores, axis=0, keepdims=True)

    def weigh(order):
        b = z ^ Z_ORDER[order]
        for half in range(2):
            largest = sm[order % 2, half]
            weight = jnp.exp2(sc[order % 2, half] - largest)
            weight_sum = jnp.sum(weight, axis=0, keepdims=True)
            weight = weight.astype(BF16)
            for side in range(2):
                block = half * 2 + side
                lanes = slice(side * BLOCK, (side + 1) * BLOCK)
                out = _dot(vt[b, block * BLOCK : (block + 1) * BLOCK, :], weight[:, lanes])
                owner = b * 4 + block
                dv[owner] = _packed(jnp.where(second_head, out[HEAD:], out[:HEAD])).astype(BF16)
                ds[owner] = jnp.concatenate([largest[:, lanes], weight_sum[:, lanes]], axis=0)

    def send(order):
        for x_step in (2, 1, 3, 0):
            step = Z_ORDER[order] << 2 | x_step
            if step:
                send_d(step)
        if Z_ORDER[order] == 0:

            @pl.when(is_other)
            def _():
                send_d(0)

    for group in Z_GROUPS:
        for order in group:
            gathered(Z_ORDER[order])
        for order in group:
            expand(order)
        score(group[0])
        for order in group:
            if order + 1 in group:
                score(order + 1)
            weigh(order)
            send(order)

    @pl.when(is_owner)
    def _():
        arrived(rkv.at[0:31], KV_RECV)
        for group in range(2):
            summed = (pkv[me] if group else rkv[0]).astype(F32)
            for step in range(1, KV):
                summed = summed + rkv[group * KV + step].astype(F32)
            rows = [summed[0:PROP] * own_factor[group], summed[PROP:] * own_factor[group]]
            rows = jnp.concatenate(rows, axis=0).astype(BF16)
            if group:
                kvg[me] = rows
            else:
                okv[...] = rows
        par_pad[...] = jnp.full((8, BLOCK), -1, jnp.int32)
        par_pad[0:SEQS, 0:PROP] = par_ref[...]
        parent_row = par_pad[pl.ds(z, 1), :]
        row_index = lax.broadcasted_iota(jnp.int32, (BLOCK, BLOCK), 0)
        lane_index = lax.broadcasted_iota(jnp.int32, (BLOCK, BLOCK), 1)
        reach = ((parent_row == row_index) & (lane_index < PROP)) | (row_index == lane_index)
        reach = jnp.where(reach, 1.0, 0.0).astype(BF16)
        for _ in range(5):
            reach = jnp.minimum(_dot(reach, reach), 1.0).astype(BF16)
        spread = (lax.rem(lane_index, PROP) == row_index) & (lane_index < 4 * PROP) & (row_index < PROP)
        lineage = _dot(reach, jnp.where(spread, 1.0, 0.0).astype(BF16))[0:PAD]
        linked = (lineage > 0.5) & (lax.broadcasted_iota(jnp.int32, (PAD, BLOCK), 0) < PROP)
        for group in range(2):
            own_expanded = _expanded((qg[me] if group else oq[...]).astype(F32))
            own_kv = (kvg[me] if group else okv[...]).astype(F32)
            own_k = jnp.concatenate([own_kv[0:PROP], zero_tail], axis=0).astype(BF16)
            own_v = jnp.concatenate([own_kv[PROP:], zero_tail], axis=0)
            self_scores = _dot_nt(own_k, own_expanded) * SCALE2
            self_scores = jnp.where(linked, self_scores, LOW)
            largest = jnp.max(self_scores, axis=0, keepdims=True)
            self_weight = jnp.where(linked, jnp.exp2(self_scores - largest), 0.0)
            self_stats[group, 0:1] = largest
            self_stats[group, 1:2] = jnp.sum(self_weight, axis=0, keepdims=True)
            self_out = _dot(jnp.transpose(own_v).astype(BF16), self_weight.astype(BF16))
            self_sum[group] = jnp.where(second_head, self_out[HEAD:], self_out[:HEAD])
        lane_row = lax.broadcasted_iota(jnp.int32, (1, BLOCK), 1)
        arrived(og.at[0], GIVE_RECV + 1)
        arrived(lam.at[0], GIVE_RECV + 2)
        arrived(wo.at[0], GIVE_RECV)
        lam_rows = []
        for group in range(2):
            index = lax.broadcasted_iota(jnp.int32, (1, TP), 1)
            pair = [
                jnp.sum(jnp.where(index == x * 2 + head, lam[group], 0.0), axis=1, keepdims=True)
                for head in range(2)
            ]
            lam_rows.append(jnp.where(lane_row < PROP, pair[0], pair[1]))

        arrived(rds.at[0:31], DS_RECV)
        self_factor = []
        factors = []
        used = lax.broadcasted_iota(jnp.int32, (KV, BLOCK), 1) < 96
        for group in range(2):
            slots = [ds.at[me] if group else rds.at[0]] + [rds.at[group * KV + step] for step in range(1, KV)]
            maxima = jnp.concatenate([slot[0:1] for slot in slots], axis=0)
            totals = jnp.concatenate([slot[1:2] for slot in slots], axis=0)
            top = jnp.maximum(jnp.max(maxima, axis=0, keepdims=True), self_stats[group, 0:1])
            own = jnp.exp2(self_stats[group, 0:1] - top)
            factor = jnp.exp2(maxima - top)
            denominator = self_stats[group, 1:2] * own + jnp.sum(totals * factor, axis=0, keepdims=True)
            inverse = 1.0 / denominator
            factor = factor * inverse
            self_factor.append(own * inverse)
            factors.append(
                [jnp.where(used, factor, pltpu.roll(factor, 96 - 32 * third, 1)) for third in range(3)]
            )
        arrived(rdv.at[0:31], DV_RECV)
        for group in range(2):
            slots = [dv.at[me] if group else rdv.at[0]] + [rdv.at[group * KV + step] for step in range(1, KV)]
            merged = []
            for third in range(3):
                rows = slice(16 * third, 16 * third + 16)
                sums = [
                    slot[rows].astype(F32) * factors[group][third][step : step + 1]
                    for step, slot in enumerate(slots)
                ]
                while len(sums) > 1:
                    sums = [a + b for a, b in zip(sums[::2], sums[1::2])]
                merged.append(sums[0])
            attended = _unpacked(jnp.concatenate(merged, axis=0)) + self_sum[group] * self_factor[group]
            difference = attended - lam_rows[group] * pltpu.roll(attended, BLOCK - 2 * PROP, 1)
            power = jnp.mean(difference * difference, axis=0, keepdims=True)
            normed = difference * lax.rsqrt(power + EPS)
            stacked = jnp.concatenate([normed, pltpu.roll(normed, BLOCK - PROP, 1)], axis=0)
            turned = jnp.transpose(stacked)[0:PROP]
            turned = turned * og[group, pl.ds(x, 1), :]
            ng[me, group] = turned.astype(BF16)
        for step in PARTNERS:
            send_ng(step)
        for z_step in (2, 1, 3, 0):

            @pl.when((z ^ z_step) >= 2)
            def _(z_step=z_step):
                for step in PARTNERS + [0]:
                    if step >> 2 == z_step:
                        send_kvg(step, 0)
                        if step:
                            send_kvg(step, 1)


        for group in Z_OUT_GROUPS:
            for z_step in group:
                arrived(ng.at[pl.ds((z ^ z_step) * 4, 4 if z_step else 3)], NG_RECV + z_step)
            sums = []
            for z_step in group:
                rows = [
                    jnp.concatenate([ng[(z ^ z_step) * 4 + block, half] for block in range(4)], axis=1)
                    for half in range(2)
                ]
                sums.append((_dot(rows[0], wo[0]) + _dot(rows[1], wo[1])).astype(BF16))
            for z_step, piece in zip(group, sums):
                rpart[z_step, 0] = piece
            for to in (1, 0):
                for z_step in group:
                    for step in Y_STEPS:
                        send_mx(z_step, step, to)
            for z_step in group:
                send_mx(z_step, 0, 0)

    @pl.when(is_owner & (z >= 2))
    def _():
        arrived(kvg.at[1:], KVG_RECV)

    @pl.when(is_other & (z >= 2))
    def _():
        arrived(kvg, KVG_RECV)

    @pl.when(z >= 2)
    def _():
        for b in range(SEQS):
            begin = len_ref[b] + acc_ref[b] - me * POS
            position = lax.broadcasted_iota(jnp.int32, (POS, BLOCK), 0) - begin
            written = (position >= 0) & (position < PROP)
            slot = lax.broadcasted_iota(jnp.int32, (POS, BLOCK), 1)
            for which, buf in enumerate((kbuf, vbuf)):
                offset = which * PROP
                placing = jnp.where(written & (position + offset == slot), 1.0, 0.0)
                placing = placing.astype(BF16)[:, 0 : 2 * PROP]
                for block in range(4):
                    lanes = slice(block * BLOCK, (block + 1) * BLOCK)
                    moved = _dot(placing, kvg[b * 4 + block])
                    buf[b, :, lanes] = jnp.where(written, moved, buf[b, :, lanes].astype(F32)).astype(BF16)
                out_copy(which, b).start()

    @pl.when(z < 2)
    def _():
        for b in range(SEQS):
            for which in range(2):
                out_copy(which, b).start()

    for z_step in Z_OUT:

        @pl.when(is_owner)
        def _(z_step=z_step):
            arrived(rpart.at[z_step, 1:], MX_RECV + z_step)

        @pl.when(is_other)
        def _(z_step=z_step):
            arrived(rpart.at[z_step], MX_RECV + z_step)

        mixed = rpart[z_step, 0].astype(F32)
        for step in range(1, 4):
            mixed = mixed + rpart[z_step, step].astype(F32)
        mixed_ref[z ^ z_step] = mixed.astype(BF16)

    arrived(kbuf, OUT + 3 * core)
    arrived(vbuf, OUT + 3 * core + 1)
    sent = ((pq, Q_SEND), (pkv, KV_SEND), (dv, DV_SEND), (ds, DS_SEND))

    @pl.when(is_owner)
    def _():
        for ref, index in sent + ((qg, QG_SEND + 1), (ng, NG_SEND)):
            arrived(ref.at[1:], index)
        arrived(qg, QG_SEND)
        arrived(kvg.at[0:8], KVG_SEND)
        arrived(rpart.at[0:7], MX_SEND)

    @pl.when(is_owner & (z < 2))
    def _():
        arrived(kvg.at[0:8], KVG_SEND + 1)

    @pl.when(is_owner & (z >= 2))
    def _():
        arrived(kvg.at[0:7], KVG_SEND + 1)

    @pl.when(is_other)
    def _():
        for ref, index in sent:
            arrived(ref, index)
        arrived(wo.at[0], GIVE_SEND)
        arrived(og.at[0], GIVE_SEND + 1)
        arrived(lam.at[0], GIVE_SEND + 2)


def _main(*arrays):
    hbm = pl.BlockSpec(memory_space=pltpu.HBM)
    vmem = pl.BlockSpec(memory_space=pltpu.VMEM)
    dma = pltpu.SemaphoreType.DMA
    return pl.pallas_call(
        _main_kernel,
        out_shape=(
            jax.ShapeDtypeStruct((SEQS, PROP, 256), BF16),
            jax.ShapeDtypeStruct((SEQS, POS, 512), BF16),
            jax.ShapeDtypeStruct((SEQS, POS, 512), BF16),
        ),
        in_specs=[hbm] * 14,
        out_specs=(vmem, pl.BlockSpec(memory_space=pl.ANY), pl.BlockSpec(memory_space=pl.ANY)),
        scratch_shapes=[
            pltpu.VMEM((SEQS, POS, 512), BF16),
            pltpu.VMEM((SEQS, POS, 512), BF16),
            pltpu.VMEM((ROWS, 256), BF16),
            pltpu.VMEM((1, 256), F32),
            pltpu.VMEM((2, 4, BLOCK), F32),
            pltpu.VMEM((SEQS, PROP), jnp.int32),
            pltpu.VMEM((2, 1, TP), F32),
            pltpu.SMEM((SEQS,), jnp.int32),
            pltpu.SMEM((SEQS,), jnp.int32),
            pltpu.VMEM((3, 256, 512), BF16),
            pltpu.VMEM((2, 512, 256), BF16),
            pltpu.VMEM((SEQS, 512, POS), BF16),
            pltpu.VMEM((KV, PAD, BLOCK), BF16),
            pltpu.VMEM((2 * KV, PAD, BLOCK), BF16),
            pltpu.VMEM((KV, 2 * PROP, BLOCK), BF16),
            pltpu.VMEM((2 * KV, 2 * PROP, BLOCK), BF16),
            pltpu.VMEM((PROP, BLOCK), BF16),
            pltpu.VMEM((2 * PROP, BLOCK), BF16),
            pltpu.VMEM((KV, PROP, BLOCK), BF16),
            pltpu.VMEM((KV, 2 * PROP, BLOCK), BF16),
            pltpu.VMEM((KV, 48, BLOCK), BF16),
            pltpu.VMEM((2 * KV, 48, BLOCK), BF16),
            pltpu.VMEM((KV, 2, BLOCK), F32),
            pltpu.VMEM((2 * KV, 2, BLOCK), F32),
            pltpu.VMEM((KV, 2, PROP, BLOCK), BF16),
            pltpu.VMEM((8, 4, PROP, 256), BF16),
            pltpu.VMEM((8, BLOCK), jnp.int32),
            pltpu.VMEM((SEQS, 2, 2 * BLOCK, 2 * BLOCK), BF16),
            pltpu.VMEM((2, 2, POS, 2 * BLOCK), F32),
            pltpu.VMEM((2, 2, 1, 2 * BLOCK), F32),
            dma((SEMAPHORES,)),
            pltpu.SemaphoreType.REGULAR,
            pltpu.SemaphoreType.REGULAR,
            pltpu.VMEM((2, PROP, BLOCK), F32),
            pltpu.VMEM((2, 2, BLOCK), F32),
            pltpu.VMEM((2, HEAD, BLOCK), F32),
        ],
        compiler_params=pltpu.CompilerParams(
            collective_id=0, has_side_effects=True, vmem_limit_bytes=MAIN_VMEM
        ),
        name="attention",
    )(*(pltpu.with_memory_space_constraint(array, pltpu.HBM) for array in arrays))


def _copies_first(which):
    kv = lax.axis_index("kv")
    y = lax.axis_index("tp") // 2
    return (kv < 5) & (kv + y * 4 < 6) if which else (kv + y) < 1


def _copy_kernel(keys_in, values_in, keys_out, values_out, kbuf, vbuf, sem):
    pairs = ((keys_in, kbuf, keys_out), (values_in, vbuf, values_out))
    fetches = [pltpu.make_async_copy(src, buf, sem.at[which]) for which, (src, buf, _) in enumerate(pairs)]
    puts = [pltpu.make_async_copy(buf, dst, sem.at[which]) for which, (_, buf, dst) in enumerate(pairs)]

    @pl.when(_copies_first(1))
    def _():
        fetches[1].start()

        @pl.when(_copies_first(0))
        def _():
            fetches[0].start()

        fetches[1].wait()
        puts[1].start()

        @pl.when(_copies_first(0))
        def _():
            fetches[0].wait()
            puts[0].start()
            puts[0].wait()

        puts[1].wait()


def _copy(*arrays):
    hbm = pl.BlockSpec(memory_space=pltpu.HBM)
    return pl.pallas_call(
        _copy_kernel,
        out_shape=tuple(jax.ShapeDtypeStruct(array.shape, array.dtype) for array in arrays),
        in_specs=[hbm] * 2,
        out_specs=(hbm,) * 2,
        scratch_shapes=[
            pltpu.VMEM((SEQS, POS, 512), BF16),
            pltpu.VMEM((SEQS, POS, 512), BF16),
            pltpu.SemaphoreType.DMA((2,)),
        ],
        compiler_params=pltpu.CompilerParams(vmem_limit_bytes=MAIN_VMEM),
        name="copy_caches",
    )(*(pltpu.with_memory_space_constraint(array, pltpu.HBM) for array in arrays))


def _write_kernel(mixed_ref, keys_ref, values_ref, _keys, _values, mixed_hbm, keys_hbm, values_hbm, sem):
    mixed_copy = pltpu.make_async_copy(mixed_ref, mixed_hbm, sem.at[2])
    mixed_copy.start()

    copies = [
        pltpu.make_async_copy(keys_ref, keys_hbm, sem.at[0]),
        pltpu.make_async_copy(values_ref, values_hbm, sem.at[1]),
    ]

    @pl.when(jnp.logical_not(_copies_first(0)))
    def _():
        copies[0].start()

        @pl.when(jnp.logical_not(_copies_first(1)))
        def _():
            copies[1].start()
            copies[1].wait()

        copies[0].wait()

    mixed_copy.wait()


def _write(*arrays):
    hbm = pl.BlockSpec(memory_space=pltpu.HBM)
    anywhere = pl.BlockSpec(memory_space=pl.ANY)
    return pl.pallas_call(
        _write_kernel,
        out_shape=tuple(jax.ShapeDtypeStruct(array.shape, array.dtype) for array in arrays[:3]),
        in_specs=[anywhere] * 3 + [hbm] * 2,
        out_specs=(hbm,) * 3,
        input_output_aliases={3: 1, 4: 2},
        scratch_shapes=[pltpu.SemaphoreType.DMA((3,))],
        compiler_params=pltpu.CompilerParams(vmem_limit_bytes=WRITE_VMEM),
        name="write",
    )(*arrays)


def _local(
    tokens,
    norm_gain,
    w_query,
    w_key,
    w_value,
    w_output,
    cache_keys,
    cache_values,
    map_lambda,
    out_gain,
    parents,
    lengths,
    accepted,
):
    first_keys, first_values = _copy(cache_keys, cache_values)
    mixed, keys, values = _main(
        tokens,
        norm_gain.reshape(1, 256),
        w_query,
        w_key,
        w_value,
        w_output,
        cache_keys,
        cache_values,
        map_lambda.reshape(1, TP),
        out_gain.reshape(4, BLOCK),
        parents,
        lengths,
        accepted,
        first_keys,
    )
    mixed, new_keys, new_values = _write(mixed, keys, values, first_keys, first_values)
    return mixed.reshape(ROWS, 256), new_keys, new_values


def solution(mesh):
    return jax.shard_map(
        _local,
        mesh=mesh,
        in_specs=(
            P(None, "kv"),
            P("kv"),
            P("kv", "tp"),
            P("kv", "tp"),
            P("kv", "tp"),
            P("tp", "kv"),
            P(None, "kv", "tp"),
            P(None, "kv", "tp"),
            P("tp"),
            P("tp"),
            P(),
            P(),
            P(),
        ),
        out_specs=(P(None, "kv"), P(None, "kv", "tp"), P(None, "kv", "tp")),
        check_vma=False,
    )
```
